32 devices in a mesh: sp: 8 (over z, y), tp: 4 (over x, core).
Axes of the slice: x: 2, y: 2, z: 4, core: 2. Of those that a mesh axis runs over, the one named last changes fastest.
Arguments:
- queries: bfloat16 [4096, 512], P('sp', 'tp'), may hold values from -6 to 6
- key_matrix: bfloat16 [4096, 512], P('sp', 'tp'), may hold values from -6 to 6
- value_matrix: bfloat16 [4096, 1024], P('sp', 'tp'), may hold values from -6 to 6
- channel_decay_input: bfloat16 [4096, 512], P('sp', 'tp')
- head_decay_offset: float32 [4096, 8], P('sp', 'tp'), may hold values from -1 to 0
- output_gate_input: bfloat16 [4096, 1024], P('sp', 'tp'), may hold values from -6 to 6
- head_norm_gain: float32 [128], replicated, may hold values from 0.1 to 1.9
- residual: bfloat16 [4096, 2048], P(('sp', 'tp')), may hold values from -6 to 6
- mixer_output_weight: bfloat16 [1024, 2048], replicated, may hold values from -0.1875 to 0.1875
- expert_norm_gain: float32 [2048], replicated, may hold values from 0.1 to 1.9
- routes: int32 [4096, 4], P(('sp', 'tp')), may hold values from 0 to 63, all different within a row; in each aligned block of 128 rows (0 to 127, 128 to 255, ...) at most 16 rows name the same one
- chosen_router_scores: float32 [4096, 4], P(('sp', 'tp')), may hold values from 0.1 to 1
- routed_gate_weight: bfloat16 [64, 2048, 512], P(('sp', 'tp')), may hold values from -0.125 to 0.125
- routed_up_weight: bfloat16 [64, 2048, 512], P(('sp', 'tp')), may hold values from -0.125 to 0.125
- routed_down_weight: bfloat16 [64, 512, 2048], P(('sp', 'tp')), may hold values from -0.25 to 0.25
- common_gate_weight: bfloat16 [2048, 512], replicated, may hold values from -0.125 to 0.125
- common_up_weight: bfloat16 [2048, 512], replicated, may hold values from -0.125 to 0.125
- common_down_weight: bfloat16 [512, 2048], replicated, may hold values from -0.25 to 0.25
Outputs:
- layer_out: bfloat16 [4096, 2048], P(('sp', 'tp'))
The draws below stay inside these ranges and needn't reach their ends.
Inputs may be any that keep to these rules, and one draw needn't show every extreme that they name: `routes`: each row names 4 different experts. In each aligned block of 128 rows (the rows of one device) no expert is named by more than 16 rows, a bound that some block reaches.
All inputs are finite; a program needn't handle non-finite values.
Results may differ from the reference program's by a relative error of at most 0.017.
Values may be sent and summed in bfloat16 or wider, within the bound.
No kernel may reach another device: no remote copies, remote signals or barrier semaphores. Data moves between devices by JAX's collectives and lax.ppermute only.
A program may use at most 128 MiB of HBM per device.

```python
import math
import jax
import jax.numpy as jnp
import numpy as np
from jax import lax

D = 2048
HEADS = 8
KEY_CHANNELS = 64
VDIM = 128
BLOCK = 64
FFE = 512
SFF = 512
TOP_K = 4
TOK_DEV = 128
KW = 512
VW = 1024
TOK_SP = 512
TOKENS = 4096
EXPERTS = 64
CAP = 16


def draw_channel_decay_input(key, part):
    head_key = jax.random.fold_in(key, 11)
    channel_key = jax.random.fold_in(key, 12)
    shift_key = jax.random.fold_in(key, 13)
    jitter_key = jax.random.fold_in(key, 14)
    slow_heads = jax.random.bernoulli(head_key, 0.5, (HEADS,))
    jitter = jnp.clip(0.5 * jax.random.normal(jitter_key, (TOKENS, HEADS * KEY_CHANNELS), jnp.float32), -1.5, 1.5)
    head_base = jnp.where(slow_heads, math.log(TOKENS) - 1.5, 0.5).astype(jnp.float32)
    channel = jax.random.uniform(channel_key, (HEADS, KEY_CHANNELS), jnp.float32, -0.5, 0.5)
    column = (head_base[:, None] + channel).reshape(HEADS * KEY_CHANNELS)
    shifts = jax.random.uniform(shift_key, (TOKENS // TOK_SP,), jnp.float32, 0.0, math.log(4.0))
    rows_shift = jnp.repeat(shifts, TOK_SP)
    return (column[None, :] + jitter - rows_shift[:, None]).astype(jnp.bfloat16)


def draw_head_decay_offset(key, part):
    place_key = jax.random.fold_in(key, 21)
    size_key = jax.random.fold_in(key, 22)
    places = jax.random.randint(place_key, (3, HEADS), 0, TOKENS)
    drops = jax.random.uniform(size_key, (3, HEADS), jnp.float32, math.log(0.5), math.log(0.8))
    positions = jnp.arange(TOKENS, dtype=jnp.int32)
    landed = positions[:, None, None] == places[None, :, :]
    return jnp.sum(jnp.where(landed, drops[None, :, :], 0.0), axis=1).astype(jnp.float32)


def level_of(own_key, shape, shards, low, high):
    def one(position, blocks):
        heights = jax.random.uniform(jax.random.fold_in(jax.random.fold_in(own_key, 6), position), (blocks,), jnp.float32, low / len(shards), high / len(shards))
        return jnp.repeat(jnp.exp(heights), shape[position] // blocks).reshape((-1,) + (1,) * (len(shape) - position - 1))

    loudness = one(*shards[0])
    for cut in shards[1:]:
        loudness = loudness * one(*cut)
    return loudness


def routed_block(stream_key, own, number, rows, number_of, top, reach, skew):
    order = jax.random.permutation(stream_key, number_of)
    heavy_load, ordinary = portions_of(number_of, rows * top, reach, skew, True), portions_of(number_of, rows * top, reach, skew, False)
    places = jnp.arange(number_of)

    def named(sizes, offset_by):
        used = int((sizes > 0).sum())
        fixed = max(1, used // 4)
        passed = fixed + (places - fixed + offset_by * (used - fixed)) % max(1, number_of - fixed)
        return jnp.zeros((number_of,), jnp.int32).at[order[jnp.where(places < fixed, places, passed)]].set(jnp.asarray(sizes, jnp.int32))

    sizes = jnp.where(number % 4 == 0, named(heavy_load, number // 4), named(ordinary, number - number // 4 - 1))
    mixed = jax.random.permutation(jax.random.fold_in(own, 3), number_of)
    giver, taker = mixed[0:number_of // 2 * 2:2], mixed[1:number_of // 2 * 2:2]
    margin = jnp.minimum(sizes[giver] - 1, reach - sizes[taker]) // 2
    margin = jnp.where((giver == order[0]) | (taker == order[0]) | (sizes[taker] == 0), 0, jnp.maximum(margin, 0))
    passed = jax.random.randint(jax.random.fold_in(own, 4), (number_of // 2,), 0, 1 << 20) % (margin + 1)
    sizes = sizes.at[giver].add(-passed).at[taker].add(passed)
    items = jnp.searchsorted(jnp.cumsum(sizes), jnp.arange(rows * top), side="right").astype(jnp.int32)
    listing = items.reshape(top, rows).T
    listing = listing[jax.random.permutation(jax.random.fold_in(own, 1), rows)]
    offset_by = jax.random.randint(jax.random.fold_in(own, 2), (rows, 1), 0, top)
    return jnp.take_along_axis(listing, (jnp.arange(top)[None, :] + offset_by) % top, axis=1)


def portions_of(amount, total, reach, skew, full):
    portions = [(1 << 20) // math.isqrt(grade ** skew) + 1 for grade in range(1, amount + 1)]
    largest = reach if full else min(reach, max(-(-total // amount), total * portions[0] // sum(portions)))
    least = 1 if total - largest >= amount - 1 else 0
    given, surplus = [largest] + [least] * (amount - 1), total - largest - least * (amount - 1)
    while surplus > 0:
        movable = [i for i in range(1, amount) if given[i] < largest] or [i for i in range(1, amount) if given[i] < reach]
        mass, budget = sum([portions[i] for i in movable]), surplus
        for i in movable:
            extra = min(reach - given[i], max(1, budget * portions[i] // mass), surplus)
            given[i] = given[i] + extra
            surplus = surplus - extra
    return np.array(given)


def scatter_about(own_key, shape, deviation, reach, cuts=(), held_as=jnp.bfloat16):
    values = jax.random.normal(own_key, shape, jnp.float32) * deviation
    if len(cuts) > 0:
        values = level_of(own_key, shape, cuts, -0.22, 0.18) * values
    return jnp.clip(values, min=-reach, max=reach).astype(held_as)


def setup_inputs(seed: int = 0) -> dict:
    arg_keys = jax.random.split(jax.random.key(seed), 19)
    queries = scatter_about(arg_keys[0], (TOKENS, KW), 1.0, 6.0, ((0, 8), (1, 4)))
    key_matrix = scatter_about(arg_keys[1], (TOKENS, KW), 1.0, 6.0, ((0, 8), (1, 4)))
    value_matrix = scatter_about(arg_keys[2], (TOKENS, VW), 1.0, 6.0, ((0, 8), (1, 4)))
    channel_decay_input = draw_channel_decay_input(jax.random.fold_in(arg_keys[18], 71), 0)
    head_decay_offset = draw_head_decay_offset(jax.random.fold_in(arg_keys[18], 71), 0)
    output_gate_input = scatter_about(arg_keys[5], (TOKENS, VW), 1.0, 6.0, ((0, 8), (1, 4)))
    head_norm_gain = jnp.clip(1.0 + 0.18 * jax.random.normal(arg_keys[6], (VDIM,), jnp.float32), 0.1, 1.9)
    residual = scatter_about(arg_keys[7], (TOKENS, D), 1.0, 6.0, ((0, 32),))
    mixer_output_weight = scatter_about(arg_keys[8], (VW, D), VW ** -0.5, 0.1875)
    expert_norm_gain = jnp.clip(1.0 + 0.18 * jax.random.normal(arg_keys[9], (D,), jnp.float32), 0.1, 1.9)
    routes_keys = jax.random.split(jax.random.fold_in(arg_keys[10], 1), TOKENS // TOK_DEV)
    routes_turns = jax.random.permutation(jax.random.fold_in(arg_keys[10], 3), TOKENS // TOK_DEV)
    routes = jax.vmap(lambda own, number: routed_block(jax.random.fold_in(arg_keys[10], 2), own, number, TOK_DEV, EXPERTS, TOP_K, CAP, 2))(routes_keys, routes_turns).reshape((TOKENS, TOP_K))
    chosen_router_scores = jnp.clip(jnp.exp(math.log(1.0) - 2.3025851 * jax.random.uniform(arg_keys[11], (TOKENS, TOP_K), jnp.float32) ** level_of(arg_keys[11], (TOKENS, TOP_K), ((0, 32),), -0.2, 0.2)), 0.1, 1.0)
    routed_gate_weight = scatter_about(arg_keys[12], (EXPERTS, D, FFE), D ** -0.5, 0.125, ((0, 32),))
    routed_up_weight = scatter_about(arg_keys[13], (EXPERTS, D, FFE), D ** -0.5, 0.125, ((0, 32),))
    routed_down_weight = scatter_about(arg_keys[14], (EXPERTS, FFE, D), FFE ** -0.5, 0.25, ((0, 32),))
    common_gate_weight = scatter_about(arg_keys[15], (D, SFF), D ** -0.5, 0.125)
    common_up_weight = scatter_about(arg_keys[16], (D, SFF), D ** -0.5, 0.125)
    common_down_weight = scatter_about(arg_keys[17], (SFF, D), SFF ** -0.5, 0.25)
    return dict(queries=queries, key_matrix=key_matrix, value_matrix=value_matrix, channel_decay_input=channel_decay_input, head_decay_offset=head_decay_offset, output_gate_input=output_gate_input, head_norm_gain=head_norm_gain, residual=residual, mixer_output_weight=mixer_output_weight, expert_norm_gain=expert_norm_gain, routes=routes, chosen_router_scores=chosen_router_scores, routed_gate_weight=routed_gate_weight, routed_up_weight=routed_up_weight, routed_down_weight=routed_down_weight, common_gate_weight=common_gate_weight, common_up_weight=common_up_weight, common_down_weight=common_down_weight)


eps_norm = 1e-06
decay_running = 16.0
routed_scale = 2.5

def split_heads(values, columns):
    blocks = values.shape[0] // BLOCK
    return values.astype(jnp.float32).reshape(blocks, BLOCK, HEADS, columns).transpose(2, 0, 1, 3)

def recurrent_mixer(queries, key_matrix, value_matrix, channel_decay_input, head_decay_offset, output_gate_input, head_norm_gain):
    decay_spike_columns = jnp.repeat(head_decay_offset, KEY_CHANNELS, axis=1)
    decay_logarithm = jax.nn.log_sigmoid(channel_decay_input.astype(jnp.float32)) / decay_running + decay_spike_columns
    within = jnp.cumsum(split_heads(decay_logarithm, KEY_CHANNELS), axis=2)
    block_end = within[:, :, -1:, :]
    q_heads = split_heads(queries, KEY_CHANNELS) * KEY_CHANNELS ** (-0.5)
    k_heads = split_heads(key_matrix, KEY_CHANNELS)
    v_heads = split_heads(value_matrix, VDIM)
    q_decay = q_heads * jnp.exp(within)
    k_grow = k_heads * jnp.exp(-within)
    k_tail = k_heads * jnp.exp(block_end - within)
    causal = jnp.tril(jnp.ones((BLOCK, BLOCK), dtype=bool))
    scores = jnp.where(causal, jnp.einsum('hnid,hnjd->hnij', q_decay, k_grow), 0.0)
    output = jnp.einsum('hnij,hnje->hnie', scores, v_heads)
    block_state = jnp.einsum('hncd,hnce->nhde', k_tail, v_heads)
    block_decay = jnp.moveaxis(jnp.exp(block_end[:, :, 0, :]), 1, 0)

    def advance(carried, block_inputs):
        added_state, factor = block_inputs
        return (factor[..., None] * carried + added_state, carried)
    start_state = jnp.zeros((HEADS, KEY_CHANNELS, VDIM), jnp.float32)
    _, entering = lax.scan(advance, start_state, (block_state, block_decay))
    output = output + jnp.einsum('hncd,nhde->hnce', q_decay, entering)
    output = output.transpose(1, 2, 0, 3).reshape(-1, HEADS, VDIM)
    inv_rms = lax.rsqrt(lax.optimization_barrier(jnp.mean(output * output, axis=-1, keepdims=True)) + eps_norm)
    normed = (output * inv_rms * head_norm_gain).reshape(-1, HEADS * VDIM)
    return (normed * jax.nn.silu(output_gate_input.astype(jnp.float32))).astype(jnp.bfloat16)

def expert_block(picked_rows, gate_weight, up_weight, down_weight):
    gate_pre = jnp.dot(picked_rows, gate_weight, preferred_element_type=jnp.float32)
    up_pre = jnp.dot(picked_rows, up_weight, preferred_element_type=jnp.float32)
    hidden = (jax.nn.silu(gate_pre) * up_pre).astype(jnp.bfloat16)
    return jnp.dot(hidden, down_weight, preferred_element_type=jnp.float32)

def reference(queries, key_matrix, value_matrix, channel_decay_input, head_decay_offset, output_gate_input, head_norm_gain, residual, mixer_output_weight, expert_norm_gain, routes, chosen_router_scores, routed_gate_weight, routed_up_weight, routed_down_weight, common_gate_weight, common_up_weight, common_down_weight):
    gated_output = recurrent_mixer(queries, key_matrix, value_matrix, channel_decay_input, head_decay_offset, output_gate_input, head_norm_gain)
    middle = (residual.astype(jnp.float32) + jnp.dot(gated_output, mixer_output_weight, preferred_element_type=jnp.float32)).astype(jnp.bfloat16)
    middle_wide = middle.astype(jnp.float32)
    inv_rms = lax.rsqrt(lax.optimization_barrier(jnp.mean(middle_wide * middle_wide, axis=-1, keepdims=True)) + eps_norm)
    normed = (middle_wide * inv_rms * expert_norm_gain).astype(jnp.bfloat16)
    weights = routed_scale * chosen_router_scores / lax.optimization_barrier(jnp.sum(chosen_router_scores, axis=-1, keepdims=True))
    flat_expert = routes.reshape(-1).astype(jnp.int32)
    assigned = TOKENS * TOP_K
    flat_token = (jnp.arange(assigned, dtype=jnp.int32) // TOP_K).astype(jnp.int32)
    flat_weight = weights.reshape(-1)
    sorted_ids = jnp.argsort(flat_expert, stable=True).astype(jnp.int32)
    counts = jnp.bincount(flat_expert, length=EXPERTS).astype(jnp.int32)
    starts = (jnp.cumsum(counts) - counts).astype(jnp.int32)
    slot_room = TOKENS // TOK_DEV * CAP
    order_pad = jnp.concatenate([sorted_ids, jnp.full((slot_room,), assigned, jnp.int32)])
    token_pad = jnp.concatenate([flat_token, jnp.full((1,), TOKENS, jnp.int32)])
    weight_pad = jnp.concatenate([flat_weight, jnp.zeros((1,), jnp.float32)])
    normed_pad = jnp.concatenate([normed, jnp.zeros((1, D), jnp.bfloat16)], axis=0)

    def one_expert(summed, expert_id):
        picked = lax.dynamic_slice_in_dim(order_pad, starts[expert_id], slot_room)
        live_slot = jnp.arange(slot_room, dtype=jnp.int32) < counts[expert_id]
        picked = jnp.where(live_slot, picked, assigned).astype(jnp.int32)
        tokens = token_pad[picked]
        picked_rows = normed_pad[tokens]
        result = expert_block(picked_rows, routed_gate_weight[expert_id], routed_up_weight[expert_id], routed_down_weight[expert_id]).astype(jnp.bfloat16)
        return (summed.at[tokens].add(weight_pad[picked][:, None] * result.astype(jnp.float32)), None)
    routed, _ = lax.scan(one_expert, jnp.zeros((TOKENS + 1, D), jnp.float32), jnp.arange(EXPERTS, dtype=jnp.int32))
    shared = expert_block(normed, common_gate_weight, common_up_weight, common_down_weight)
    return (middle_wide + routed[:TOKENS] + shared).astype(jnp.bfloat16)
```

```python
import jax
import jax.numpy as jnp
from jax import lax
from jax.experimental import pallas as pl
from jax.experimental.pallas import tpu as pltpu
from jax.sharding import PartitionSpec as P

KEY_CHANNELS = 64
BLOCK = 64
TOP_K = 4
MSG_PAD = 16

eps_norm = 1e-06
decay_running = 16.0
routed_scale = 2.5


def lane_head(shape):
    return lax.broadcasted_iota(jnp.int32, shape, 1) // KEY_CHANNELS


def state_kernel(k_ref, v_ref, c_ref, o_ref, within_ref, starts_ref, msg_ref):
    rows, width = k_ref.shape
    heads = o_ref.shape[1]
    vdim = v_ref.shape[1] // heads
    x = c_ref[...].astype(jnp.float32)
    decay = (jnp.minimum(x, 0.0) - jnp.log1p(jnp.exp(-jnp.abs(x)))) / decay_running
    head_of = lane_head((rows, width))
    spike = jnp.zeros((rows, width), jnp.float32)
    for h in range(heads):
        spike = jnp.where(head_of == h, o_ref[:, h : h + 1], spike)
    decay = decay + spike
    lower = lax.broadcasted_iota(jnp.int32, (BLOCK, BLOCK), 0) >= lax.broadcasted_iota(
        jnp.int32, (BLOCK, BLOCK), 1
    )
    lower = lower.astype(jnp.float32)
    state_head = lane_head((vdim, width))
    state = jnp.zeros((vdim, width), jnp.float32)
    total = jnp.zeros((1, width), jnp.float32)
    for n in range(rows // BLOCK):
        at = slice(n * BLOCK, (n + 1) * BLOCK)
        within = jnp.dot(
            lower,
            decay[at],
            precision=lax.Precision.HIGHEST,
            preferred_element_type=jnp.float32,
        )
        within_ref[at, :] = within
        starts_ref[n] = state
        last = within[BLOCK - 1 : BLOCK]
        tail = (k_ref[at, :].astype(jnp.float32) * jnp.exp(last - within)).astype(jnp.bfloat16)
        added = jnp.zeros((vdim, width), jnp.float32)
        for h in range(heads):
            one = lax.dot_general(
                v_ref[at, h * vdim : (h + 1) * vdim],
                tail,
                (((0,), (0,)), ((), ())),
                preferred_element_type=jnp.float32,
            )
            added = jnp.where(state_head == h, one, added)
        state = state * jnp.exp(last) + added
        total = total + last
    factor = jnp.exp(total)
    high = factor.astype(jnp.bfloat16).astype(jnp.float32)
    low = factor - high
    row = lax.broadcasted_iota(jnp.int32, (MSG_PAD, width), 0)
    tail_rows = jnp.where(row == 0, high, jnp.where(row == 1, low, 0.0)).astype(jnp.bfloat16)
    state = state.astype(jnp.bfloat16)
    for j in range(msg_ref.shape[0]):
        msg_ref[j, :vdim, :] = state
        msg_ref[j, vdim:, :] = tail_rows


def mixer_kernel(
    place_ref, q_ref, k_ref, v_ref, within_ref, starts_ref, msg_ref, gate_ref, gain_ref, out_ref
):
    rows, width = k_ref.shape
    heads = width // KEY_CHANNELS
    vdim = v_ref.shape[1] // heads

    def hop(j, carried):
        message = msg_ref[j].astype(jnp.float32)
        factor = message[vdim : vdim + 1] + message[vdim + 1 : vdim + 2]
        return carried * factor + message[:vdim]

    carried = lax.fori_loop(0, place_ref[0], hop, jnp.zeros((vdim, width), jnp.float32))
    head_of = lane_head((BLOCK, width))
    causal = lax.broadcasted_iota(jnp.int32, (heads * BLOCK, BLOCK), 0) % BLOCK >= (
        lax.broadcasted_iota(jnp.int32, (heads * BLOCK, BLOCK), 1)
    )
    gain = gain_ref[...]
    before = jnp.zeros((1, width), jnp.float32)
    for n in range(rows // BLOCK):
        at = slice(n * BLOCK, (n + 1) * BLOCK)
        within = within_ref[at, :]
        queries = q_ref[at, :].astype(jnp.float32) * (KEY_CHANNELS**-0.5) * jnp.exp(within)
        grown = (k_ref[at, :].astype(jnp.float32) * jnp.exp(-within)).astype(jnp.bfloat16)
        split = jnp.concatenate(
            [jnp.where(head_of == h, queries, 0.0) for h in range(heads)], axis=0
        ).astype(jnp.bfloat16)
        scores = lax.dot_general(
            split, grown, (((1,), (1,)), ((), ())), preferred_element_type=jnp.float32
        )
        scores = jnp.where(causal, scores, 0.0).astype(jnp.bfloat16)
        entering = (starts_ref[n] + jnp.exp(before) * carried).astype(jnp.bfloat16)
        crossed = lax.dot_general(
            split, entering, (((1,), (1,)), ((), ())), preferred_element_type=jnp.float32
        )
        for h in range(heads):
            cols = slice(h * vdim, (h + 1) * vdim)
            own = slice(h * BLOCK, (h + 1) * BLOCK)
            output = crossed[own] + jnp.dot(
                scores[own], v_ref[at, cols], preferred_element_type=jnp.float32
            )
            scale = lax.rsqrt(jnp.mean(output * output, axis=-1, keepdims=True) + eps_norm)
            gate = gate_ref[at, cols].astype(jnp.float32)
            out_ref[at, cols] = (
                output * scale * gain * (gate / (1.0 + jnp.exp(-gate)))
            ).astype(jnp.bfloat16)
        before = before + within[BLOCK - 1 : BLOCK]


def mixer(queries, keys, values, channel_decay_input, head_decay_offset, gates, gain):
    rows, width = keys.shape
    vdim = gain.shape[0]
    seq = lax.axis_size("sp")
    within, starts, message = pl.pallas_call(
        state_kernel,
        out_shape=(
            jax.ShapeDtypeStruct((rows, width), jnp.float32),
            jax.ShapeDtypeStruct((rows // BLOCK, vdim, width), jnp.float32),
            jax.ShapeDtypeStruct((seq, vdim + MSG_PAD, width), jnp.bfloat16),
        ),
        name="mixer_state",
    )(keys, values, channel_decay_input, head_decay_offset)
    arrived = lax.all_to_all(message, "sp", split_axis=0, concat_axis=0, tiled=True)
    vmem = pl.BlockSpec(memory_space=pltpu.VMEM)
    return pl.pallas_call(
        mixer_kernel,
        in_specs=[pl.BlockSpec(memory_space=pltpu.SMEM)] + [vmem] * 8,
        out_specs=vmem,
        out_shape=jax.ShapeDtypeStruct(values.shape, jnp.bfloat16),
        name="mixer_output",
    )(
        lax.axis_index("sp").astype(jnp.int32).reshape(1),
        queries,
        keys,
        values,
        within,
        starts,
        arrived,
        gates,
        gain.reshape(1, vdim),
    )


def shared_block(rows, gate_weight, up_weight, down_weight):
    gate_pre = jnp.dot(rows, gate_weight, preferred_element_type=jnp.float32)
    up_pre = jnp.dot(rows, up_weight, preferred_element_type=jnp.float32)
    hidden = (jax.nn.silu(gate_pre) * up_pre).astype(jnp.bfloat16)
    return jnp.dot(hidden, down_weight, preferred_element_type=jnp.float32)


def apply_experts(arrived, routed_gate_weight, routed_up_weight, routed_down_weight):
    gate_pre = jnp.einsum(
        "sech,ehf->secf", arrived, routed_gate_weight, preferred_element_type=jnp.float32
    )
    up_pre = jnp.einsum(
        "sech,ehf->secf", arrived, routed_up_weight, preferred_element_type=jnp.float32
    )
    hidden = (jax.nn.silu(gate_pre) * up_pre).astype(jnp.bfloat16)
    return jnp.einsum(
        "secf,efh->sech", hidden, routed_down_weight, preferred_element_type=jnp.float32
    ).astype(jnp.bfloat16)


def slot_tables(chosen, weights, first_expert, slots, cap):
    tokens = chosen.shape[0]
    slot = lax.broadcasted_iota(jnp.int32, (tokens, slots), 1)
    expert = (first_expert + slot // cap).astype(jnp.float32)
    named = jnp.zeros((tokens, slots), jnp.float32)
    weight = jnp.zeros((tokens, slots), jnp.float32)
    for k in range(TOP_K):
        hit = chosen[:, k : k + 1] == expert
        named = jnp.where(hit, 1.0, named)
        weight = jnp.where(hit, weights[:, k : k + 1], weight)
    earlier = jnp.tril(jnp.ones((tokens, tokens), jnp.bfloat16), -1)
    rank = jnp.dot(earlier, named.astype(jnp.bfloat16), preferred_element_type=jnp.float32)
    held = (named > 0) & (rank == (slot % cap).astype(jnp.float32))
    weight = jnp.where(held, weight, 0.0)
    high = weight.astype(jnp.bfloat16)
    low = (weight - high.astype(jnp.float32)).astype(jnp.bfloat16)
    return held.astype(jnp.bfloat16), high, low


def pack(held, rows):
    return lax.dot_general(
        held, rows, (((0,), (0,)), ((), ())), preferred_element_type=jnp.float32
    ).astype(jnp.bfloat16)


def weigh(high, low, results):
    return jnp.dot(high, results, preferred_element_type=jnp.float32) + jnp.dot(
        low, results, preferred_element_type=jnp.float32
    )


def on_device(
    queries,
    key_matrix,
    value_matrix,
    channel_decay_input,
    head_decay_offset,
    output_gate_input,
    head_norm_gain,
    residual,
    mixer_output_weight,
    expert_norm_gain,
    routes,
    chosen_router_scores,
    routed_gate_weight,
    routed_up_weight,
    routed_down_weight,
    common_gate_weight,
    common_up_weight,
    common_down_weight,
):
    seq, heads_axis = lax.axis_size("sp"), lax.axis_size("tp")
    axes = ("sp", "tp")
    devices = seq * heads_axis
    half = devices // 2
    halves = [list(range(half)), list(range(half, devices))]
    swap = [(i, (i + seq // 2) % seq) for i in range(seq)]
    tok_count, width = residual.shape
    exp_dev = routed_gate_weight.shape[0]
    cap = 2 * TOP_K * tok_count // (exp_dev * devices)
    slots = exp_dev * half * cap
    first_expert = (lax.axis_index("sp") // (seq // 2)) * (exp_dev * half)

    weights = (
        routed_scale * chosen_router_scores / jnp.sum(chosen_router_scores, axis=-1, keepdims=True)
    )
    chosen = jnp.concatenate([routes.astype(jnp.float32), weights], axis=1)
    chosen_far = lax.ppermute(chosen, "sp", swap)
    held_near, high_near, low_near = slot_tables(
        chosen[:, :TOP_K], chosen[:, TOP_K:], first_expert, slots, cap
    )
    held_far, high_far, low_far = slot_tables(
        chosen_far[:, :TOP_K], chosen_far[:, TOP_K:], first_expert, slots, cap
    )

    gated = mixer(
        queries,
        key_matrix,
        value_matrix,
        channel_decay_input,
        head_decay_offset,
        output_gate_input,
        head_norm_gain,
    )
    stacked = gated.reshape(heads_axis, tok_count, gated.shape[1])
    projected = jnp.dot(
        lax.all_to_all(stacked, "tp", split_axis=0, concat_axis=2, tiled=True)[0],
        mixer_output_weight,
        preferred_element_type=jnp.float32,
    )
    middle = (residual.astype(jnp.float32) + projected).astype(jnp.bfloat16)
    middle_wide = middle.astype(jnp.float32)
    norm_scale = lax.rsqrt(jnp.mean(middle_wide * middle_wide, axis=-1, keepdims=True) + eps_norm)
    normed = (middle_wide * norm_scale * expert_norm_gain).astype(jnp.bfloat16)

    def spread(rows):
        return lax.all_to_all(
            rows.reshape(half, exp_dev * cap, width),
            axes,
            split_axis=0,
            concat_axis=0,
            axis_index_groups=halves,
            tiled=True,
        )

    def experts(arrived):
        return apply_experts(
            arrived.reshape(half, exp_dev, cap, width),
            routed_gate_weight,
            routed_up_weight,
            routed_down_weight,
        ).reshape(slots, width)

    normed_far = lax.ppermute(normed, "sp", swap)
    arrived_near = spread(pack(held_near, normed))
    arrived_far = spread(pack(held_far, normed_far))
    shared = shared_block(normed, common_gate_weight, common_up_weight, common_down_weight)
    done_near = experts(arrived_near)
    done_far = experts(arrived_far)
    back_far = spread(done_far).reshape(slots, width)
    far = weigh(high_far, low_far, back_far).astype(jnp.bfloat16)
    from_far = lax.ppermute(far, "sp", swap)
    back_near = spread(done_near).reshape(slots, width)
    routed = weigh(high_near, low_near, back_near) + from_far.astype(jnp.float32)
    return (middle_wide + routed + shared).astype(jnp.bfloat16)


def solution(mesh):
    placed = (
        P("sp", "tp"),
        P("sp", "tp"),
        P("sp", "tp"),
        P("sp", "tp"),
        P("sp", "tp"),
        P("sp", "tp"),
        P(),
        P(("sp", "tp"), None),
        P(),
        P(),
        P(("sp", "tp"), None),
        P(("sp", "tp"), None),
        P(("sp", "tp"), None, None),
        P(("sp", "tp"), None, None),
        P(("sp", "tp"), None, None),
        P(),
        P(),
        P(),
    )
    return jax.shard_map(
        on_device, mesh=mesh, in_specs=placed, out_specs=P(("sp", "tp"), None), check_vma=False
    )
```

```python
import functools

import jax
import jax.numpy as jnp
from jax import lax
from jax.experimental import pallas as pl
from jax.experimental.pallas import tpu as pltpu
from jax.sharding import PartitionSpec as P

KEY_CHANNELS = 64
BLOCK = 64
TOP_K = 4
MSG_PAD = 16

eps_norm = 1e-06
decay_running = 16.0
routed_scale = 2.5


def lane_head(shape):
    return lax.broadcasted_iota(jnp.int32, shape, 1) // KEY_CHANNELS


def state_kernel(k_ref, v_ref, c_ref, o_ref, within_ref, starts_ref, msg_ref):
    rows, width = k_ref.shape
    heads = o_ref.shape[0]
    vdim = v_ref.shape[1] // heads
    x = c_ref[...].astype(jnp.float32)
    decay = (jnp.minimum(x, 0.0) - jnp.log1p(jnp.exp(-jnp.abs(x)))) / decay_running
    columns_of = (
        lax.broadcasted_iota(jnp.int32, (heads, width), 0) == lane_head((heads, width))
    ).astype(jnp.float32)
    decay = decay + lax.dot_general(
        o_ref[...],
        columns_of,
        (((0,), (0,)), ((), ())),
        precision=lax.Precision.HIGHEST,
        preferred_element_type=jnp.float32,
    )
    lower = lax.broadcasted_iota(jnp.int32, (BLOCK, BLOCK), 0) >= lax.broadcasted_iota(
        jnp.int32, (BLOCK, BLOCK), 1
    )
    lower = lower.astype(jnp.float32)
    state_head = lane_head((vdim, width))
    state = jnp.zeros((vdim, width), jnp.float32)
    total = jnp.zeros((1, width), jnp.float32)
    for n in range(rows // BLOCK):
        at = slice(n * BLOCK, (n + 1) * BLOCK)
        within = jnp.dot(
            lower,
            decay[at],
            precision=lax.Precision.HIGHEST,
            preferred_element_type=jnp.float32,
        )
        within_ref[at, :] = within
        starts_ref[n] = state
        last = within[BLOCK - 1 : BLOCK]
        tail = (k_ref[at, :].astype(jnp.float32) * jnp.exp(last - within)).astype(jnp.bfloat16)
        added = jnp.zeros((vdim, width), jnp.float32)
        for h in range(heads):
            one = lax.dot_general(
                v_ref[at, h * vdim : (h + 1) * vdim],
                tail,
                (((0,), (0,)), ((), ())),
                preferred_element_type=jnp.float32,
            )
            added = jnp.where(state_head == h, one, added)
        state = state * jnp.exp(last) + added
        total = total + last
    factor = jnp.exp(total)
    high = factor.astype(jnp.bfloat16).astype(jnp.float32)
    low = factor - high
    row = lax.broadcasted_iota(jnp.int32, (MSG_PAD, width), 0)
    tail_rows = jnp.where(row == 0, high, jnp.where(row == 1, low, 0.0)).astype(jnp.bfloat16)
    state = state.astype(jnp.bfloat16)
    for j in range(msg_ref.shape[0]):
        msg_ref[j, :vdim, :] = state
        msg_ref[j, vdim:, :] = tail_rows


def mixer_kernel(
    place_ref, q_ref, k_ref, v_ref, within_ref, starts_ref, msg_ref, gate_ref, gain_ref, out_ref
):
    rows, width = k_ref.shape
    heads = width // KEY_CHANNELS
    vdim = v_ref.shape[1] // heads

    def hop(j, carried):
        message = msg_ref[j].astype(jnp.float32)
        factor = message[vdim : vdim + 1] + message[vdim + 1 : vdim + 2]
        return carried * factor + message[:vdim]

    carried = lax.fori_loop(0, place_ref[0], hop, jnp.zeros((vdim, width), jnp.float32))
    head_of = lane_head((BLOCK, width))
    causal = lax.broadcasted_iota(jnp.int32, (heads * BLOCK, BLOCK), 0) % BLOCK >= (
        lax.broadcasted_iota(jnp.int32, (heads * BLOCK, BLOCK), 1)
    )
    gain = gain_ref[...]
    before = jnp.zeros((1, width), jnp.float32)
    for n in range(rows // BLOCK):
        at = slice(n * BLOCK, (n + 1) * BLOCK)
        within = within_ref[at, :]
        queries = q_ref[at, :].astype(jnp.float32) * (KEY_CHANNELS**-0.5) * jnp.exp(within)
        grown = (k_ref[at, :].astype(jnp.float32) * jnp.exp(-within)).astype(jnp.bfloat16)
        split = jnp.concatenate(
            [jnp.where(head_of == h, queries, 0.0) for h in range(heads)], axis=0
        ).astype(jnp.bfloat16)
        scores = lax.dot_general(
            split, grown, (((1,), (1,)), ((), ())), preferred_element_type=jnp.float32
        )
        scores = jnp.where(causal, scores, 0.0).astype(jnp.bfloat16)
        entering = (starts_ref[n] + jnp.exp(before) * carried).astype(jnp.bfloat16)
        crossed = lax.dot_general(
            split, entering, (((1,), (1,)), ((), ())), preferred_element_type=jnp.float32
        )
        for h in range(heads):
            cols = slice(h * vdim, (h + 1) * vdim)
            own = slice(h * BLOCK, (h + 1) * BLOCK)
            output = crossed[own] + jnp.dot(
                scores[own], v_ref[at, cols], preferred_element_type=jnp.float32
            )
            scale = lax.rsqrt(jnp.mean(output * output, axis=-1, keepdims=True) + eps_norm)
            gate = gate_ref[at, cols].astype(jnp.float32)
            out_ref[at, cols] = (
                output * scale * gain * (gate / (1.0 + jnp.exp(-gate)))
            ).astype(jnp.bfloat16)
        before = before + within[BLOCK - 1 : BLOCK]


def mixer(queries, keys, values, channel_decay_input, head_decay_offset, gates, gain):
    rows, width = keys.shape
    vdim = gain.shape[0]
    seq = lax.axis_size("sp")
    within, starts, message = pl.pallas_call(
        state_kernel,
        out_shape=(
            jax.ShapeDtypeStruct((rows, width), jnp.float32),
            jax.ShapeDtypeStruct((rows // BLOCK, vdim, width), jnp.float32),
            jax.ShapeDtypeStruct((seq, vdim + MSG_PAD, width), jnp.bfloat16),
        ),
        name="mixer_state",
    )(keys, values, channel_decay_input, head_decay_offset.T)
    arrived = lax.all_to_all(message, "sp", split_axis=0, concat_axis=0, tiled=True)
    vmem = pl.BlockSpec(memory_space=pltpu.VMEM)
    return pl.pallas_call(
        mixer_kernel,
        in_specs=[pl.BlockSpec(memory_space=pltpu.SMEM)] + [vmem] * 8,
        out_specs=vmem,
        out_shape=jax.ShapeDtypeStruct(values.shape, jnp.bfloat16),
        name="mixer_output",
    )(
        lax.axis_index("sp").astype(jnp.int32).reshape(1),
        queries,
        keys,
        values,
        within,
        starts,
        arrived,
        gates,
        gain.reshape(1, vdim),
    )


def ffn_kernel(x_ref, gate_ref, up_ref, down_ref, *rest):
    add_ref, out_ref, acc_ref = rest if len(rest) == 3 else (None,) + rest
    step = pl.program_id(1)
    rows = x_ref.shape[0] * x_ref.shape[1]
    x = x_ref[...].reshape(rows, x_ref.shape[2])
    gate_pre = jnp.dot(x, gate_ref[0], preferred_element_type=jnp.float32)
    up_pre = jnp.dot(x, up_ref[0], preferred_element_type=jnp.float32)
    hidden = (gate_pre / (1.0 + jnp.exp(-gate_pre)) * up_pre).astype(jnp.bfloat16)
    part = jnp.dot(hidden, down_ref[0], preferred_element_type=jnp.float32)

    @pl.when(step == 0)
    def _():
        acc_ref[...] = part

    @pl.when(step != 0)
    def _():
        acc_ref[...] += part

    @pl.when(step == pl.num_programs(1) - 1)
    def _():
        whole = acc_ref[...]
        if add_ref is not None:
            whole = whole + add_ref[...].astype(jnp.float32)
        out_ref[...] = whole.astype(out_ref.dtype).reshape(out_ref.shape)


def ffn(rows, gate_weight, up_weight, down_weight, cap, add=None):
    sources, _, width = rows.shape
    count, _, hidden = gate_weight.shape
    steps = 2 if hidden % 256 == 0 else 1
    piece = hidden // steps
    row_spec = pl.BlockSpec((sources, cap, width), lambda e, f: (0, e, 0))
    in_specs = [
        row_spec,
        pl.BlockSpec((1, width, piece), lambda e, f: (e, 0, f)),
        pl.BlockSpec((1, width, piece), lambda e, f: (e, 0, f)),
        pl.BlockSpec((1, piece, width), lambda e, f: (e, f, 0)),
    ]
    args = [rows, gate_weight, up_weight, down_weight]
    dtype = jnp.bfloat16
    if add is not None:
        in_specs.append(pl.BlockSpec((sources * cap, width), lambda e, f: (0, 0)))
        args.append(add)
        dtype = jnp.float32
    return pl.pallas_call(
        ffn_kernel,
        grid=(count, steps),
        in_specs=in_specs,
        out_specs=row_spec,
        out_shape=jax.ShapeDtypeStruct(rows.shape, dtype),
        scratch_shapes=[pltpu.VMEM((sources * cap, width), jnp.float32)],
        compiler_params=pltpu.CompilerParams(vmem_limit_bytes=48 << 20),
        cost_estimate=pl.CostEstimate(
            flops=6 * rows.shape[0] * rows.shape[1] * width * hidden,
            transcendentals=rows.shape[0] * rows.shape[1] * hidden,
            bytes_accessed=6 * count * width * hidden + 4 * rows.size,
        ),
    )(*args)


def slot_tables(chosen, first_expert, held_ref, weight_ref, cap):
    tokens, slots = held_ref.shape
    slot = lax.broadcasted_iota(jnp.int32, (tokens, slots), 1)
    expert = (first_expert + slot // cap).astype(jnp.float32)
    total = chosen[:, TOP_K : TOP_K + 1]
    for k in range(1, TOP_K):
        total = total + chosen[:, TOP_K + k : TOP_K + k + 1]
    named = jnp.zeros((tokens, slots), jnp.float32)
    weight = jnp.zeros((tokens, slots), jnp.float32)
    for k in range(TOP_K):
        hit = chosen[:, k : k + 1] == expert
        named = jnp.where(hit, 1.0, named)
        weight = jnp.where(
            hit, routed_scale * chosen[:, TOP_K + k : TOP_K + k + 1] / total, weight
        )
    earlier = lax.broadcasted_iota(jnp.int32, (tokens, tokens), 0) > lax.broadcasted_iota(
        jnp.int32, (tokens, tokens), 1
    )
    rank = jnp.dot(
        jnp.where(earlier, 1.0, 0.0).astype(jnp.bfloat16),
        named.astype(jnp.bfloat16),
        preferred_element_type=jnp.float32,
    )
    held = (named > 0) & (rank == (slot % cap).astype(jnp.float32))
    weight = jnp.where(held, weight, 0.0)
    high = weight.astype(jnp.bfloat16)
    held_ref[...] = jnp.where(held, 1.0, 0.0).astype(jnp.bfloat16)
    weight_ref[0] = high
    weight_ref[1] = (weight - high.astype(jnp.float32)).astype(jnp.bfloat16)


def tables_kernel(cap, first_ref, near_ref, far_ref, held_near, near_w, held_far, far_w):
    slot_tables(near_ref[...], first_ref[0], held_near, near_w, cap)
    slot_tables(far_ref[...], first_ref[0], held_far, far_w, cap)


def pick(held, rows):
    return lax.dot_general(
        held, rows, (((0,), (0,)), ((), ())), preferred_element_type=jnp.float32
    ).astype(jnp.bfloat16)


def project_kernel(g_ref, w_ref, res_ref, gain_ref, held_ref, mid_ref, norm_ref, sent_ref):
    count, _, cols = g_ref.shape
    total = res_ref[...].astype(jnp.float32)
    for t in range(count):
        total = total + jnp.dot(
            g_ref[t], w_ref[t * cols : (t + 1) * cols, :], preferred_element_type=jnp.float32
        )
    middle = total.astype(jnp.bfloat16)
    mid_ref[...] = middle
    wide = middle.astype(jnp.float32)
    scale = lax.rsqrt(jnp.mean(wide * wide, axis=-1, keepdims=True) + eps_norm)
    normed = (wide * scale * gain_ref[...]).astype(jnp.bfloat16)
    norm_ref[...] = normed
    sent_ref[...] = pick(held_ref[...], normed)


def pack_kernel(held_ref, rows_ref, sent_ref):
    sent_ref[...] = pick(held_ref[...], rows_ref[...])


def weighed(weight_ref, results_ref):
    results = results_ref[...]
    return jnp.dot(weight_ref[0], results, preferred_element_type=jnp.float32) + jnp.dot(
        weight_ref[1], results, preferred_element_type=jnp.float32
    )


def far_kernel(weight_ref, results_ref, out_ref):
    out_ref[...] = weighed(weight_ref, results_ref).astype(jnp.bfloat16)


def final_kernel(weight_ref, results_ref, base_ref, far_ref, out_ref):
    out_ref[...] = (
        base_ref[...] + weighed(weight_ref, results_ref) + far_ref[...].astype(jnp.float32)
    ).astype(jnp.bfloat16)


def call(kernel, out, *args, scalars=0):
    vmem = pl.BlockSpec(memory_space=pltpu.VMEM)
    in_specs = [pl.BlockSpec(memory_space=pltpu.SMEM)] * scalars + [vmem] * (len(args) - scalars)
    return pl.pallas_call(
        kernel, in_specs=in_specs, out_specs=jax.tree.map(lambda _: vmem, out), out_shape=out
    )(*args)


def on_device(
    queries,
    key_matrix,
    value_matrix,
    channel_decay_input,
    head_decay_offset,
    output_gate_input,
    head_norm_gain,
    residual,
    mixer_output_weight,
    expert_norm_gain,
    routes,
    chosen_router_scores,
    routed_gate_weight,
    routed_up_weight,
    routed_down_weight,
    common_gate_weight,
    common_up_weight,
    common_down_weight,
):
    seq, heads_axis = lax.axis_size("sp"), lax.axis_size("tp")
    axes = ("sp", "tp")
    devices = seq * heads_axis
    half = devices // 2
    halves = [list(range(half)), list(range(half, devices))]
    swap = [(i, (i + seq // 2) % seq) for i in range(seq)]
    tok_count, width = residual.shape
    exp_dev = routed_gate_weight.shape[0]
    cap = 2 * TOP_K * tok_count // (exp_dev * devices)
    slots = exp_dev * half * cap
    first_expert = lax.div(lax.axis_index("sp"), jnp.int32(seq // 2)) * (exp_dev * half)

    def like(shape, dtype=jnp.bfloat16):
        return jax.ShapeDtypeStruct(shape, dtype)

    def spread(rows):
        return lax.all_to_all(
            rows.reshape(half, exp_dev * cap, width),
            axes,
            split_axis=0,
            concat_axis=0,
            axis_index_groups=halves,
            tiled=True,
        ).reshape(slots, width)

    def experts(rows):
        weights = (routed_gate_weight, routed_up_weight, routed_down_weight)
        if cap % 16 == 0:
            rows = rows.reshape(half, exp_dev * cap, width)
            return ffn(rows, *weights, cap).reshape(slots, width)
        order = (half, exp_dev, cap, width)
        rows = rows.reshape(order).transpose(1, 0, 2, 3).reshape(1, slots, width)
        done = ffn(rows, *weights, half * cap)
        return done.reshape(exp_dev, half, cap, width).transpose(1, 0, 2, 3).reshape(slots, width)

    packed = like((slots, width))
    chosen = jnp.concatenate([routes.astype(jnp.float32), chosen_router_scores], axis=1)
    chosen_far = lax.ppermute(chosen, "sp", swap)
    held = like((tok_count, slots))
    slot_weights = like((2, tok_count, slots))
    held_near, weights_near, held_far, weights_far = call(
        functools.partial(tables_kernel, cap),
        (held, slot_weights, held, slot_weights),
        first_expert.astype(jnp.int32).reshape(1),
        chosen,
        chosen_far,
        scalars=1,
    )
    gated = mixer(
        queries,
        key_matrix,
        value_matrix,
        channel_decay_input,
        head_decay_offset,
        output_gate_input,
        head_norm_gain,
    )
    stacked = gated.reshape(heads_axis, tok_count, gated.shape[1])
    stacked = lax.all_to_all(stacked, "tp", split_axis=0, concat_axis=0, tiled=True)
    rows = like((tok_count, width))
    middle, normed, sent_near = call(
        project_kernel,
        (rows, rows, packed),
        stacked,
        mixer_output_weight,
        residual,
        expert_norm_gain.reshape(1, width),
        held_near,
    )
    arrived_near = spread(sent_near)
    normed_far = lax.ppermute(normed, "sp", swap)
    base = ffn(
        normed[None],
        common_gate_weight[None],
        common_up_weight[None],
        common_down_weight[None],
        tok_count,
        add=middle,
    )[0]
    sent_far = call(pack_kernel, packed, held_far, normed_far)
    arrived_far = spread(sent_far)
    done_near = experts(arrived_near)
    done_far = experts(arrived_far)
    back_far = spread(done_far)
    back_near = spread(done_near)
    far = call(far_kernel, rows, weights_far, back_far)
    from_far = lax.ppermute(far, "sp", swap)
    return call(final_kernel, rows, weights_near, back_near, base, from_far)


def solution(mesh):
    placed = (
        P("sp", "tp"),
        P("sp", "tp"),
        P("sp", "tp"),
        P("sp", "tp"),
        P("sp", "tp"),
        P("sp", "tp"),
        P(),
        P(("sp", "tp"), None),
        P(),
        P(),
        P(("sp", "tp"), None),
        P(("sp", "tp"), None),
        P(("sp", "tp"), None, None),
        P(("sp", "tp"), None, None),
        P(("sp", "tp"), None, None),
        P(),
        P(),
        P(),
    )
    return jax.shard_map(
        on_device, mesh=mesh, in_specs=placed, out_specs=P(("sp", "tp"), None), check_vma=False
    )
```

```python
import functools

import jax
import jax.numpy as jnp
from jax import lax
from jax.experimental import pallas as pl
from jax.experimental.pallas import tpu as pltpu
from jax.sharding import PartitionSpec as P

KEY_CHANNELS = 64
BLOCK = 64
TOP_K = 4
MSG_PAD = 16

eps_norm = 1e-06
decay_running = 16.0
routed_scale = 2.5


def lane_head(shape):
    return lax.broadcasted_iota(jnp.int32, shape, 1) // KEY_CHANNELS


def two_pieces(value):
    high = value.astype(jnp.bfloat16).astype(jnp.float32)
    return high, value - high


def state_kernel(
    k_ref, v_ref, c_ref, o_ref, routes_ref, scores_ref, within_ref, starts_ref, msg_ref
):
    rows, width = k_ref.shape
    heads = o_ref.shape[0]
    vdim = v_ref.shape[1] // heads
    x = c_ref[...].astype(jnp.float32)
    decay = (jnp.minimum(x, 0.0) - jnp.log1p(jnp.exp(-jnp.abs(x)))) / decay_running
    columns_of = (
        lax.broadcasted_iota(jnp.int32, (heads, width), 0) == lane_head((heads, width))
    ).astype(jnp.float32)
    decay = decay + lax.dot_general(
        o_ref[...],
        columns_of,
        (((0,), (0,)), ((), ())),
        precision=lax.Precision.HIGHEST,
        preferred_element_type=jnp.float32,
    )
    lower = lax.broadcasted_iota(jnp.int32, (BLOCK, BLOCK), 0) >= lax.broadcasted_iota(
        jnp.int32, (BLOCK, BLOCK), 1
    )
    lower = lower.astype(jnp.float32)
    state_head = lane_head((vdim, width))
    state = jnp.zeros((vdim, width), jnp.float32)
    total = jnp.zeros((1, width), jnp.float32)
    for n in range(rows // BLOCK):
        at = slice(n * BLOCK, (n + 1) * BLOCK)
        within = jnp.dot(
            lower,
            decay[at],
            precision=lax.Precision.HIGHEST,
            preferred_element_type=jnp.float32,
        )
        within_ref[at, :] = within
        starts_ref[n] = state
        last = within[BLOCK - 1 : BLOCK]
        tail = (k_ref[at, :].astype(jnp.float32) * jnp.exp(last - within)).astype(jnp.bfloat16)
        added = jnp.zeros((vdim, width), jnp.float32)
        for h in range(heads):
            one = lax.dot_general(
                v_ref[at, h * vdim : (h + 1) * vdim],
                tail,
                (((0,), (0,)), ((), ())),
                preferred_element_type=jnp.float32,
            )
            added = jnp.where(state_head == h, one, added)
        state = state * jnp.exp(last) + added
        total = total + last
    factor = jnp.exp(total)
    tail_rows = jnp.zeros((MSG_PAD, width), jnp.float32)
    row = lax.broadcasted_iota(jnp.int32, (MSG_PAD, width), 0)
    scores = scores_ref[...]
    place = 0
    for value in two_pieces(factor) + (routes_ref[...].astype(jnp.float32),) + two_pieces(scores):
        for r in range(value.shape[0]):
            tail_rows = jnp.where(row == place, value[r : r + 1], tail_rows)
            place += 1
    tail_rows = tail_rows.astype(jnp.bfloat16)
    state = state.astype(jnp.bfloat16)
    for j in range(msg_ref.shape[0]):
        msg_ref[j, :vdim, :] = state
        msg_ref[j, vdim:, :] = tail_rows


def mixer_kernel(
    place_ref, q_ref, k_ref, v_ref, within_ref, starts_ref, msg_ref, gate_ref, gain_ref, out_ref
):
    rows, width = k_ref.shape
    heads = width // KEY_CHANNELS
    vdim = v_ref.shape[1] // heads

    def hop(j, carried):
        message = msg_ref[j].astype(jnp.float32)
        factor = message[vdim : vdim + 1] + message[vdim + 1 : vdim + 2]
        return carried * factor + message[:vdim]

    carried = lax.fori_loop(0, place_ref[0], hop, jnp.zeros((vdim, width), jnp.float32))
    head_of = lane_head((BLOCK, width))
    causal = lax.broadcasted_iota(jnp.int32, (heads * BLOCK, BLOCK), 0) % BLOCK >= (
        lax.broadcasted_iota(jnp.int32, (heads * BLOCK, BLOCK), 1)
    )
    gain = gain_ref[...]
    before = jnp.zeros((1, width), jnp.float32)
    for n in range(rows // BLOCK):
        at = slice(n * BLOCK, (n + 1) * BLOCK)
        within = within_ref[at, :]
        queries = q_ref[at, :].astype(jnp.float32) * (KEY_CHANNELS**-0.5) * jnp.exp(within)
        grown = (k_ref[at, :].astype(jnp.float32) * jnp.exp(-within)).astype(jnp.bfloat16)
        split = jnp.concatenate(
            [jnp.where(head_of == h, queries, 0.0) for h in range(heads)], axis=0
        ).astype(jnp.bfloat16)
        scores = lax.dot_general(
            split, grown, (((1,), (1,)), ((), ())), preferred_element_type=jnp.float32
        )
        scores = jnp.where(causal, scores, 0.0).astype(jnp.bfloat16)
        entering = (starts_ref[n] + jnp.exp(before) * carried).astype(jnp.bfloat16)
        crossed = lax.dot_general(
            split, entering, (((1,), (1,)), ((), ())), preferred_element_type=jnp.float32
        )
        for h in range(heads):
            cols = slice(h * vdim, (h + 1) * vdim)
            own = slice(h * BLOCK, (h + 1) * BLOCK)
            output = crossed[own] + jnp.dot(
                scores[own], v_ref[at, cols], preferred_element_type=jnp.float32
            )
            scale = lax.rsqrt(jnp.mean(output * output, axis=-1, keepdims=True) + eps_norm)
            gate = gate_ref[at, cols].astype(jnp.float32)
            out_ref[at, cols] = (
                output * scale * gain * (gate / (1.0 + jnp.exp(-gate)))
            ).astype(jnp.bfloat16)
        before = before + within[BLOCK - 1 : BLOCK]


def call(kernel, out, *args, scalars=0):
    def whole(x):
        return pl.BlockSpec(x.shape, lambda i, rank=len(x.shape): (0,) * rank)

    in_specs = [pl.BlockSpec(memory_space=pltpu.SMEM)] * scalars + [
        whole(x) for x in args[scalars:]
    ]
    return pl.pallas_call(
        kernel,
        grid=(1,),
        in_specs=in_specs,
        out_specs=jax.tree.map(whole, out),
        out_shape=out,
        compiler_params=pltpu.CompilerParams(vmem_limit_bytes=48 << 20),
    )(*args)


def ffn_kernel(x_ref, gate_ref, up_ref, down_ref, *rest):
    add_ref, out_ref, acc_ref = rest if len(rest) == 3 else (None,) + rest
    step = pl.program_id(1)
    rows = x_ref.shape[0] * x_ref.shape[1]
    x = x_ref[...].reshape(rows, x_ref.shape[2])
    gate_pre = jnp.dot(x, gate_ref[0], preferred_element_type=jnp.float32)
    up_pre = jnp.dot(x, up_ref[0], preferred_element_type=jnp.float32)
    hidden = (gate_pre / (1.0 + jnp.exp(-gate_pre)) * up_pre).astype(jnp.bfloat16)
    part = jnp.dot(hidden, down_ref[0], preferred_element_type=jnp.float32)

    @pl.when(step == 0)
    def _():
        acc_ref[...] = part

    @pl.when(step != 0)
    def _():
        acc_ref[...] += part

    @pl.when(step == pl.num_programs(1) - 1)
    def _():
        whole = acc_ref[...]
        if add_ref is not None:
            whole = whole + add_ref[...].astype(jnp.float32)
        out_ref[...] = whole.astype(out_ref.dtype).reshape(out_ref.shape)


def ffn(rows, gate_weight, up_weight, down_weight, cap, add=None):
    sources, _, width = rows.shape
    count, _, hidden = gate_weight.shape
    steps = 2 if hidden % 256 == 0 else 1
    piece = hidden // steps
    row_spec = pl.BlockSpec((sources, cap, width), lambda e, f: (0, e, 0))
    in_specs = [
        row_spec,
        pl.BlockSpec((1, width, piece), lambda e, f: (e, 0, f)),
        pl.BlockSpec((1, width, piece), lambda e, f: (e, 0, f)),
        pl.BlockSpec((1, piece, width), lambda e, f: (e, f, 0)),
    ]
    args = [rows, gate_weight, up_weight, down_weight]
    dtype = jnp.bfloat16
    if add is not None:
        in_specs.append(pl.BlockSpec((sources * cap, width), lambda e, f: (0, 0)))
        args.append(add)
        dtype = jnp.float32
    return pl.pallas_call(
        ffn_kernel,
        grid=(count, steps),
        in_specs=in_specs,
        out_specs=row_spec,
        out_shape=jax.ShapeDtypeStruct(rows.shape, dtype),
        scratch_shapes=[pltpu.VMEM((sources * cap, width), jnp.float32)],
        compiler_params=pltpu.CompilerParams(vmem_limit_bytes=48 << 20),
        cost_estimate=pl.CostEstimate(
            flops=6 * rows.shape[0] * rows.shape[1] * width * hidden,
            transcendentals=rows.shape[0] * rows.shape[1] * hidden,
            bytes_accessed=6 * count * width * hidden + 4 * rows.size,
        ),
    )(*args)


def slot_tables(routes, scores, first_expert, held_ref, weight_ref, cap):
    slots, tokens = held_ref.shape
    slot = lax.broadcasted_iota(jnp.int32, (slots, tokens), 0)
    expert = (first_expert + lax.div(slot, jnp.int32(cap))).astype(jnp.float32)
    weights = routed_scale * scores / jnp.sum(scores, axis=0, keepdims=True)
    named = jnp.zeros((slots, tokens), jnp.float32)
    weight = jnp.zeros((slots, tokens), jnp.float32)
    for k in range(TOP_K):
        hit = routes[k : k + 1] == expert
        named = jnp.where(hit, 1.0, named)
        weight = jnp.where(hit, weights[k : k + 1], weight)
    earlier = lax.broadcasted_iota(jnp.int32, (tokens, tokens), 0) < lax.broadcasted_iota(
        jnp.int32, (tokens, tokens), 1
    )
    rank = jnp.dot(
        named.astype(jnp.bfloat16),
        jnp.where(earlier, 1.0, 0.0).astype(jnp.bfloat16),
        preferred_element_type=jnp.float32,
    )
    held = (named > 0) & (rank == lax.rem(slot, jnp.int32(cap)).astype(jnp.float32))
    held_ref[...] = jnp.where(held, 1.0, 0.0).astype(jnp.bfloat16)
    high, low = two_pieces(jnp.where(held, weight, 0.0).T)
    weight_ref[0] = high.astype(jnp.bfloat16)
    weight_ref[1] = low.astype(jnp.bfloat16)


def tables_kernel(
    cap, place_ref, routes_ref, scores_ref, far_ref, held_near, near_w, held_far, far_w
):
    slot_tables(
        routes_ref[...].astype(jnp.float32), scores_ref[...], place_ref[0], held_near, near_w, cap
    )
    far = far_ref[0].astype(jnp.float32)
    at = [far[2 + k * TOP_K : 2 + (k + 1) * TOP_K] for k in range(3)]
    slot_tables(at[0], at[1] + at[2], place_ref[0], held_far, far_w, cap)


def tables(places, routes, scores, arrived, slots, cap):
    tokens = routes.shape[1]
    vdim = arrived.shape[1] - MSG_PAD
    held = jax.ShapeDtypeStruct((slots, tokens), jnp.bfloat16)
    weights = jax.ShapeDtypeStruct((2, tokens, slots), jnp.bfloat16)

    def whole(x):
        return pl.BlockSpec(x.shape, lambda i, p, rank=len(x.shape): (0,) * rank)

    out = (held, weights, held, weights)
    return pl.pallas_call(
        functools.partial(tables_kernel, cap),
        grid_spec=pltpu.PrefetchScalarGridSpec(
            num_scalar_prefetch=1,
            grid=(1,),
            in_specs=[
                whole(routes),
                whole(scores),
                pl.BlockSpec(
                    (1, MSG_PAD, arrived.shape[2]), lambda i, p: (p[1], vdim // MSG_PAD, 0)
                ),
            ],
            out_specs=jax.tree.map(whole, out),
        ),
        out_shape=out,
        name="tables",
    )(places, routes, scores, arrived)


def pick(held, rows):
    return jnp.dot(held, rows, preferred_element_type=jnp.float32).astype(jnp.bfloat16)


def project_kernel(g_ref, w_ref, res_ref, gain_ref, held_ref, sent_ref, *rest):
    acc_ref = rest[-1]
    step = pl.program_id(0)
    part = jnp.dot(g_ref[0], w_ref[...], preferred_element_type=jnp.float32)

    @pl.when(step == 0)
    def _():
        acc_ref[...] = res_ref[...].astype(jnp.float32) + part

    @pl.when(step != 0)
    def _():
        acc_ref[...] += part

    @pl.when(step == pl.num_programs(0) - 1)
    def _():
        middle = acc_ref[...].astype(jnp.bfloat16)
        wide = middle.astype(jnp.float32)
        scale = lax.rsqrt(jnp.mean(wide * wide, axis=-1, keepdims=True) + eps_norm)
        normed = (wide * scale * gain_ref[...]).astype(jnp.bfloat16)
        sent_ref[...] = pick(held_ref[...], normed)
        if len(rest) == 3:
            rest[0][...] = middle
            rest[1][...] = normed


def project(stacked, weight, residual, gain, held, keep_rows):
    count, tokens, cols = stacked.shape
    width = residual.shape[1]
    slots = held.shape[0]
    out = [jax.ShapeDtypeStruct((slots, width), jnp.bfloat16)]
    if keep_rows:
        out += [jax.ShapeDtypeStruct((tokens, width), jnp.bfloat16)] * 2

    def whole(x):
        return pl.BlockSpec(x.shape, lambda t, rank=len(x.shape): (0,) * rank)

    return pl.pallas_call(
        project_kernel,
        grid=(count,),
        in_specs=[
            pl.BlockSpec((1, tokens, cols), lambda t: (t, 0, 0)),
            pl.BlockSpec((cols, width), lambda t: (t, 0)),
            whole(residual),
            whole(gain),
            whole(held),
        ],
        out_specs=[whole(x) for x in out],
        out_shape=out,
        scratch_shapes=[pltpu.VMEM((tokens, width), jnp.float32)],
        compiler_params=pltpu.CompilerParams(vmem_limit_bytes=48 << 20),
    )(stacked, weight, residual, gain, held)


def weighed(weight_ref, results_ref):
    return jnp.dot(weight_ref[0], results_ref[...], preferred_element_type=jnp.float32) + jnp.dot(
        weight_ref[1], results_ref[...], preferred_element_type=jnp.float32
    )


def far_kernel(weight_ref, results_ref, out_ref):
    out_ref[...] = weighed(weight_ref, results_ref).astype(jnp.bfloat16)


def final_kernel(weight_ref, results_ref, base_ref, far_ref, out_ref):
    out_ref[...] = (
        base_ref[...] + weighed(weight_ref, results_ref) + far_ref[...].astype(jnp.float32)
    ).astype(jnp.bfloat16)


def by_columns(kernel, out, weights, *args):
    steps = 4 if out.shape[1] % 512 == 0 else 1
    piece = out.shape[1] // steps

    def part(x):
        return pl.BlockSpec((x.shape[0], piece), lambda c: (0, c))

    return pl.pallas_call(
        kernel,
        grid=(steps,),
        in_specs=[pl.BlockSpec(weights.shape, lambda c: (0, 0, 0))] + [part(x) for x in args],
        out_specs=part(out),
        out_shape=out,
    )(weights, *args)


def on_device(
    queries,
    key_matrix,
    value_matrix,
    channel_decay_input,
    head_decay_offset,
    output_gate_input,
    head_norm_gain,
    residual,
    mixer_output_weight,
    expert_norm_gain,
    routes,
    chosen_router_scores,
    routed_gate_weight,
    routed_up_weight,
    routed_down_weight,
    common_gate_weight,
    common_up_weight,
    common_down_weight,
):
    seq, heads_axis = lax.axis_size("sp"), lax.axis_size("tp")
    axes = ("sp", "tp")
    devices = seq * heads_axis
    half = devices // 2
    halves = [list(range(half)), list(range(half, devices))]
    swap = [(i, (i + seq // 2) % seq) for i in range(seq)]
    tok_count, width = residual.shape
    exp_dev = routed_gate_weight.shape[0]
    cap = 2 * TOP_K * tok_count // (exp_dev * devices)
    slots = exp_dev * half * cap
    place = lax.axis_index("sp").astype(jnp.int32)
    first_expert = lax.div(place, jnp.int32(seq // 2)) * (exp_dev * half)
    far_place = lax.rem(place + seq // 2, jnp.int32(seq))

    def like(shape, dtype=jnp.bfloat16):
        return jax.ShapeDtypeStruct(shape, dtype)

    def spread(rows):
        return lax.all_to_all(
            rows.reshape(half, exp_dev * cap, width),
            axes,
            split_axis=0,
            concat_axis=0,
            axis_index_groups=halves,
            tiled=True,
        ).reshape(slots, width)

    def experts(rows):
        weights = (routed_gate_weight, routed_up_weight, routed_down_weight)
        if cap % 16 == 0:
            rows = rows.reshape(half, exp_dev * cap, width)
            return ffn(rows, *weights, cap).reshape(slots, width)
        order = (half, exp_dev, cap, width)
        rows = rows.reshape(order).transpose(1, 0, 2, 3).reshape(1, slots, width)
        done = ffn(rows, *weights, half * cap)
        return done.reshape(exp_dev, half, cap, width).transpose(1, 0, 2, 3).reshape(slots, width)

    key_rows, key_cols = key_matrix.shape
    vdim = head_norm_gain.shape[0]
    routes_t, scores_t = routes.T, chosen_router_scores.T
    within, starts, message = call(
        state_kernel,
        (
            like((key_rows, key_cols), jnp.float32),
            like((key_rows // BLOCK, vdim, key_cols), jnp.float32),
            like((seq, vdim + MSG_PAD, key_cols)),
        ),
        key_matrix,
        value_matrix,
        channel_decay_input,
        head_decay_offset.T,
        routes_t,
        scores_t,
    )
    arrived = lax.all_to_all(message, "sp", split_axis=0, concat_axis=0, tiled=True)
    residual_far = lax.ppermute(residual, "sp", swap)
    gated = call(
        mixer_kernel,
        like(value_matrix.shape),
        place.reshape(1),
        queries,
        key_matrix,
        value_matrix,
        within,
        starts,
        arrived,
        output_gate_input,
        head_norm_gain.reshape(1, vdim),
        scalars=1,
    )
    stacked = gated.reshape(heads_axis, tok_count, gated.shape[1])
    stacked = lax.all_to_all(stacked, "tp", split_axis=0, concat_axis=0, tiled=True)
    held_near, weights_near, held_far, weights_far = tables(
        jnp.stack([first_expert, far_place]), routes_t, scores_t, arrived, slots, cap
    )
    stacked_far = lax.ppermute(stacked, "sp", swap)
    gain = expert_norm_gain.reshape(1, width)
    sent_near, middle, normed = project(
        stacked, mixer_output_weight, residual, gain, held_near, True
    )
    arrived_near = spread(sent_near)
    base = ffn(
        normed[None],
        common_gate_weight[None],
        common_up_weight[None],
        common_down_weight[None],
        tok_count,
        add=middle,
    )[0]
    (sent_far,) = project(stacked_far, mixer_output_weight, residual_far, gain, held_far, False)
    arrived_far = spread(sent_far)
    done_near = experts(arrived_near)
    done_far = experts(arrived_far)
    back_far = spread(done_far)
    back_near = spread(done_near)
    rows = like((tok_count, width))
    far = by_columns(far_kernel, rows, weights_far, back_far)
    from_far = lax.ppermute(far, "sp", swap)
    return by_columns(final_kernel, rows, weights_near, back_near, base, from_far)


def solution(mesh):
    placed = (
        P("sp", "tp"),
        P("sp", "tp"),
        P("sp", "tp"),
        P("sp", "tp"),
        P("sp", "tp"),
        P("sp", "tp"),
        P(),
        P(("sp", "tp"), None),
        P(),
        P(),
        P(("sp", "tp"), None),
        P(("sp", "tp"), None),
        P(("sp", "tp"), None, None),
        P(("sp", "tp"), None, None),
        P(("sp", "tp"), None, None),
        P(),
        P(),
        P(),
    )
    return jax.shard_map(
        on_device, mesh=mesh, in_specs=placed, out_specs=P(("sp", "tp"), None), check_vma=False
    )
```

```python
import functools

import jax
import jax.numpy as jnp
from jax import lax
from jax.experimental import pallas as pl
from jax.experimental.pallas import tpu as pltpu
from jax.sharding import PartitionSpec as P

KEY_CHANNELS = 64
BLOCK = 64
TOP_K = 4
MSG_PAD = 16
ROOM = 40 << 20

eps_norm = 1e-06
decay_running = 16.0
routed_scale = 2.5


def lane_head(shape):
    return lax.broadcasted_iota(jnp.int32, shape, 1) // KEY_CHANNELS


def two_pieces(value):
    high = value.astype(jnp.bfloat16).astype(jnp.float32)
    return high, value - high


def state_kernel(
    k_ref, v_ref, c_ref, o_ref, routes_ref, scores_ref, within_ref, starts_ref, msg_ref
):
    rows, width = k_ref.shape
    heads = o_ref.shape[0]
    vdim = v_ref.shape[1] // heads
    x = c_ref[...].astype(jnp.float32)
    decay = (jnp.minimum(x, 0.0) - jnp.log1p(jnp.exp(-jnp.abs(x)))) / decay_running
    columns_of = (
        lax.broadcasted_iota(jnp.int32, (heads, width), 0) == lane_head((heads, width))
    ).astype(jnp.float32)
    decay = decay + lax.dot_general(
        o_ref[...],
        columns_of,
        (((0,), (0,)), ((), ())),
        precision=lax.Precision.HIGHEST,
        preferred_element_type=jnp.float32,
    )
    lower = lax.broadcasted_iota(jnp.int32, (BLOCK, BLOCK), 0) >= lax.broadcasted_iota(
        jnp.int32, (BLOCK, BLOCK), 1
    )
    lower = lower.astype(jnp.float32)
    state_head = lane_head((vdim, width))
    state = jnp.zeros((vdim, width), jnp.float32)
    total = jnp.zeros((1, width), jnp.float32)
    for n in range(rows // BLOCK):
        at = slice(n * BLOCK, (n + 1) * BLOCK)
        within = jnp.dot(
            lower,
            decay[at],
            precision=lax.Precision.HIGHEST,
            preferred_element_type=jnp.float32,
        )
        within_ref[at, :] = within
        starts_ref[n] = state
        last = within[BLOCK - 1 : BLOCK]
        tail = (k_ref[at, :].astype(jnp.float32) * jnp.exp(last - within)).astype(jnp.bfloat16)
        added = jnp.zeros((vdim, width), jnp.float32)
        for h in range(heads):
            one = lax.dot_general(
                v_ref[at, h * vdim : (h + 1) * vdim],
                tail,
                (((0,), (0,)), ((), ())),
                preferred_element_type=jnp.float32,
            )
            added = jnp.where(state_head == h, one, added)
        state = state * jnp.exp(last) + added
        total = total + last
    factor = jnp.exp(total)
    tail_rows = jnp.zeros((MSG_PAD, width), jnp.float32)
    row = lax.broadcasted_iota(jnp.int32, (MSG_PAD, width), 0)
    scores = scores_ref[...]
    place = 0
    for value in two_pieces(factor) + (routes_ref[...].astype(jnp.float32),) + two_pieces(scores):
        for r in range(value.shape[0]):
            tail_rows = jnp.where(row == place, value[r : r + 1], tail_rows)
            place += 1
    tail_rows = tail_rows.astype(jnp.bfloat16)
    state = state.astype(jnp.bfloat16)
    for j in range(msg_ref.shape[0]):
        msg_ref[j, :vdim, :] = state
        msg_ref[j, vdim:, :] = tail_rows


def mixer_kernel(
    place_ref, q_ref, k_ref, v_ref, within_ref, starts_ref, msg_ref, gate_ref, gain_ref, out_ref
):
    rows, width = k_ref.shape
    heads = width // KEY_CHANNELS
    vdim = v_ref.shape[1] // heads

    def hop(j, carried):
        message = msg_ref[j].astype(jnp.float32)
        factor = message[vdim : vdim + 1] + message[vdim + 1 : vdim + 2]
        return carried * factor + message[:vdim]

    carried = lax.fori_loop(0, place_ref[0], hop, jnp.zeros((vdim, width), jnp.float32))
    head_of = lane_head((BLOCK, width))
    causal = lax.broadcasted_iota(jnp.int32, (heads * BLOCK, BLOCK), 0) % BLOCK >= (
        lax.broadcasted_iota(jnp.int32, (heads * BLOCK, BLOCK), 1)
    )
    gain = gain_ref[...]
    before = jnp.zeros((1, width), jnp.float32)
    for n in range(rows // BLOCK):
        at = slice(n * BLOCK, (n + 1) * BLOCK)
        within = within_ref[at, :]
        queries = q_ref[at, :].astype(jnp.float32) * (KEY_CHANNELS**-0.5) * jnp.exp(within)
        grown = (k_ref[at, :].astype(jnp.float32) * jnp.exp(-within)).astype(jnp.bfloat16)
        split = jnp.concatenate(
            [jnp.where(head_of == h, queries, 0.0) for h in range(heads)], axis=0
        ).astype(jnp.bfloat16)
        scores = lax.dot_general(
            split, grown, (((1,), (1,)), ((), ())), preferred_element_type=jnp.float32
        )
        scores = jnp.where(causal, scores, 0.0).astype(jnp.bfloat16)
        entering = (starts_ref[n] + jnp.exp(before) * carried).astype(jnp.bfloat16)
        crossed = lax.dot_general(
            split, entering, (((1,), (1,)), ((), ())), preferred_element_type=jnp.float32
        )
        for h in range(heads):
            cols = slice(h * vdim, (h + 1) * vdim)
            own = slice(h * BLOCK, (h + 1) * BLOCK)
            output = crossed[own] + jnp.dot(
                scores[own], v_ref[at, cols], preferred_element_type=jnp.float32
            )
            scale = lax.rsqrt(jnp.mean(output * output, axis=-1, keepdims=True) + eps_norm)
            gate = gate_ref[at, cols].astype(jnp.float32)
            out_ref[at, cols] = (
                output * scale * gain * (gate / (1.0 + jnp.exp(-gate)))
            ).astype(jnp.bfloat16)
        before = before + within[BLOCK - 1 : BLOCK]


def whole(x, loose=False):
    return pl.BlockSpec(
        x.shape,
        lambda *_, rank=len(x.shape): (0,) * rank,
        memory_space=None if loose else pltpu.VMEM,
    )


def call(kernel, out, *args, scalars=0, loose=()):
    in_specs = [pl.BlockSpec(memory_space=pltpu.SMEM)] * scalars + [
        whole(x, i in loose) for i, x in enumerate(args[scalars:])
    ]
    return pl.pallas_call(
        kernel, grid=(1,), in_specs=in_specs, out_specs=jax.tree.map(whole, out), out_shape=out
    )(*args)


def ffn_kernel(x_ref, gate_ref, up_ref, down_ref, *rest):
    add_ref, out_ref, acc_ref = rest if len(rest) == 3 else (None,) + rest
    step = pl.program_id(1)
    rows = x_ref.shape[0] * x_ref.shape[1]
    x = x_ref[...].reshape(rows, x_ref.shape[2])
    gate_pre = jnp.dot(x, gate_ref[0], preferred_element_type=jnp.float32)
    up_pre = jnp.dot(x, up_ref[0], preferred_element_type=jnp.float32)
    hidden = (gate_pre / (1.0 + jnp.exp(-gate_pre)) * up_pre).astype(jnp.bfloat16)
    part = jnp.dot(hidden, down_ref[0], preferred_element_type=jnp.float32)

    @pl.when(step == 0)
    def _():
        acc_ref[...] = part

    @pl.when(step != 0)
    def _():
        acc_ref[...] += part

    @pl.when(step == pl.num_programs(1) - 1)
    def _():
        whole = acc_ref[...]
        if add_ref is not None:
            whole = whole + add_ref[...].astype(jnp.float32)
        out_ref[...] = whole.astype(out_ref.dtype).reshape(out_ref.shape)


def ffn(rows, gate_weight, up_weight, down_weight, cap, add=None):
    sources, _, width = rows.shape
    count, _, hidden = gate_weight.shape
    steps = 2 if hidden % 256 == 0 else 1
    piece = hidden // steps
    row_spec = pl.BlockSpec(
        (sources, cap, width), lambda e, f: (0, e, 0), memory_space=pltpu.VMEM
    )
    in_specs = [
        pl.BlockSpec((sources, cap, width), lambda e, f: (0, e, 0)),
        pl.BlockSpec((1, width, piece), lambda e, f: (e, 0, f), memory_space=pltpu.VMEM),
        pl.BlockSpec((1, width, piece), lambda e, f: (e, 0, f), memory_space=pltpu.VMEM),
        pl.BlockSpec((1, piece, width), lambda e, f: (e, f, 0), memory_space=pltpu.VMEM),
    ]
    args = [rows, gate_weight, up_weight, down_weight]
    dtype = jnp.bfloat16
    if add is not None:
        in_specs.append(whole(add))
        args.append(add)
        dtype = jnp.float32
    return pl.pallas_call(
        ffn_kernel,
        grid=(count, steps),
        in_specs=in_specs,
        out_specs=row_spec,
        out_shape=jax.ShapeDtypeStruct(rows.shape, dtype),
        scratch_shapes=[pltpu.VMEM((sources * cap, width), jnp.float32)],
        compiler_params=pltpu.CompilerParams(vmem_limit_bytes=None if add is not None else ROOM),
        cost_estimate=pl.CostEstimate(
            flops=6 * rows.shape[0] * rows.shape[1] * width * hidden,
            transcendentals=rows.shape[0] * rows.shape[1] * hidden,
            bytes_accessed=6 * count * width * hidden + 4 * rows.size,
        ),
    )(*args)


def slot_tables(routes, scores, first_expert, held_ref, weight_ref, cap):
    slots, tokens = held_ref.shape
    slot = lax.broadcasted_iota(jnp.int32, (slots, tokens), 0)
    expert = (first_expert + lax.div(slot, jnp.int32(cap))).astype(jnp.float32)
    weights = routed_scale * scores / jnp.sum(scores, axis=0, keepdims=True)
    named = jnp.zeros((slots, tokens), jnp.float32)
    weight = jnp.zeros((slots, tokens), jnp.float32)
    for k in range(TOP_K):
        hit = routes[k : k + 1] == expert
        named = jnp.where(hit, 1.0, named)
        weight = jnp.where(hit, weights[k : k + 1], weight)
    earlier = lax.broadcasted_iota(jnp.int32, (tokens, tokens), 0) < lax.broadcasted_iota(
        jnp.int32, (tokens, tokens), 1
    )
    rank = jnp.dot(
        named.astype(jnp.bfloat16),
        jnp.where(earlier, 1.0, 0.0).astype(jnp.bfloat16),
        preferred_element_type=jnp.float32,
    )
    held = (named > 0) & (rank == lax.rem(slot, jnp.int32(cap)).astype(jnp.float32))
    held_ref[...] = jnp.where(held, 1.0, 0.0).astype(jnp.bfloat16)
    high, low = two_pieces(jnp.where(held, weight, 0.0).T)
    weight_ref[:tokens] = high.astype(jnp.bfloat16)
    weight_ref[tokens:] = low.astype(jnp.bfloat16)


def tables_kernel(
    cap, place_ref, routes_ref, scores_ref, far_ref, held_near, near_w, held_far, far_w
):
    slot_tables(
        routes_ref[...].astype(jnp.float32), scores_ref[...], place_ref[0], held_near, near_w, cap
    )
    far = far_ref[0].astype(jnp.float32)
    at = [far[2 + k * TOP_K : 2 + (k + 1) * TOP_K] for k in range(3)]
    slot_tables(at[0], at[1] + at[2], place_ref[0], held_far, far_w, cap)


def tables(places, routes, scores, arrived, slots, cap):
    tokens = routes.shape[1]
    vdim = arrived.shape[1] - MSG_PAD
    held = jax.ShapeDtypeStruct((slots, tokens), jnp.bfloat16)
    weights = jax.ShapeDtypeStruct((2 * tokens, slots), jnp.bfloat16)

    out = (held, weights, held, weights)
    return pl.pallas_call(
        functools.partial(tables_kernel, cap),
        grid_spec=pltpu.PrefetchScalarGridSpec(
            num_scalar_prefetch=1,
            grid=(1,),
            in_specs=[
                whole(routes),
                whole(scores),
                pl.BlockSpec(
                    (1, MSG_PAD, arrived.shape[2]), lambda i, p: (p[1], vdim // MSG_PAD, 0)
                ),
            ],
            out_specs=jax.tree.map(whole, out),
        ),
        out_shape=out,
        name="tables",
    )(places, routes, scores, arrived)


def pick(held, rows):
    return jnp.dot(held, rows, preferred_element_type=jnp.float32).astype(jnp.bfloat16)


def project_kernel(g_ref, w_ref, res_ref, gain_ref, held_ref, sent_ref, *rest):
    acc_ref = rest[-1]
    step = pl.program_id(0)
    part = jnp.dot(g_ref[0], w_ref[...], preferred_element_type=jnp.float32)

    @pl.when(step == 0)
    def _():
        acc_ref[...] = res_ref[...].astype(jnp.float32) + part

    @pl.when(step != 0)
    def _():
        acc_ref[...] += part

    @pl.when(step == pl.num_programs(0) - 1)
    def _():
        middle = acc_ref[...].astype(jnp.bfloat16)
        wide = middle.astype(jnp.float32)
        scale = lax.rsqrt(jnp.mean(wide * wide, axis=-1, keepdims=True) + eps_norm)
        normed = (wide * scale * gain_ref[...]).astype(jnp.bfloat16)
        sent_ref[...] = pick(held_ref[...], normed)
        if len(rest) == 3:
            rest[0][...] = middle
            rest[1][...] = normed


def project(stacked, weight, residual, gain, held, keep_rows):
    count, tokens, cols = stacked.shape
    width = residual.shape[1]
    slots = held.shape[0]
    out = [jax.ShapeDtypeStruct((slots, width), jnp.bfloat16)]
    if keep_rows:
        out += [jax.ShapeDtypeStruct((tokens, width), jnp.bfloat16)] * 2

    return pl.pallas_call(
        project_kernel,
        grid=(count,),
        in_specs=[
            pl.BlockSpec((1, tokens, cols), lambda t: (t, 0, 0)),
            pl.BlockSpec((cols, width), lambda t: (t, 0), memory_space=pltpu.VMEM),
            whole(residual, not keep_rows),
            whole(gain),
            whole(held),
        ],
        out_specs=[whole(x) for x in out],
        out_shape=out,
        scratch_shapes=[pltpu.VMEM((tokens, width), jnp.float32)],
    )(stacked, weight, residual, gain, held)


def weigh_kernel(weight_ref, results_ref, *rest):
    out_ref, acc_ref = rest[-2:]
    step = pl.program_id(0)
    tokens = out_ref.shape[0]
    both = jnp.dot(weight_ref[...], results_ref[...], preferred_element_type=jnp.float32)
    part = both[:tokens] + both[tokens:]

    @pl.when(step == 0)
    def _():
        acc_ref[...] = part

    @pl.when(step == pl.num_programs(0) - 1)
    def _():
        total = acc_ref[...] + part
        if len(rest) == 4:
            total = total + rest[0][...] + rest[1][...].astype(jnp.float32)
        out_ref[...] = total.astype(jnp.bfloat16)


def weigh(out, weights, results, *more):
    slots, width = results.shape
    piece = slots // 2
    in_specs = [
        pl.BlockSpec((weights.shape[0], piece), lambda k: (0, k), memory_space=pltpu.VMEM),
        pl.BlockSpec((piece, width), lambda k: (k, 0)),
    ]
    if more:
        in_specs += [whole(more[0]), whole(more[1], True)]
    return pl.pallas_call(
        weigh_kernel,
        grid=(2,),
        in_specs=in_specs,
        out_specs=whole(out),
        out_shape=out,
        scratch_shapes=[pltpu.VMEM(out.shape, jnp.float32)],
        compiler_params=pltpu.CompilerParams(vmem_limit_bytes=ROOM if more else None),
    )(weights, results, *more)


def on_device(
    queries,
    key_matrix,
    value_matrix,
    channel_decay_input,
    head_decay_offset,
    output_gate_input,
    head_norm_gain,
    residual,
    mixer_output_weight,
    expert_norm_gain,
    routes,
    chosen_router_scores,
    routed_gate_weight,
    routed_up_weight,
    routed_down_weight,
    common_gate_weight,
    common_up_weight,
    common_down_weight,
):
    seq, heads_axis = lax.axis_size("sp"), lax.axis_size("tp")
    axes = ("sp", "tp")
    devices = seq * heads_axis
    half = devices // 2
    halves = [list(range(half)), list(range(half, devices))]
    swap = [(i, (i + seq // 2) % seq) for i in range(seq)]
    tok_count, width = residual.shape
    exp_dev = routed_gate_weight.shape[0]
    cap = 2 * TOP_K * tok_count // (exp_dev * devices)
    slots = exp_dev * half * cap
    place = lax.axis_index("sp").astype(jnp.int32)
    first_expert = lax.div(place, jnp.int32(seq // 2)) * (exp_dev * half)
    far_place = lax.rem(place + seq // 2, jnp.int32(seq))

    def like(shape, dtype=jnp.bfloat16):
        return jax.ShapeDtypeStruct(shape, dtype)

    def spread(rows):
        return lax.all_to_all(
            rows.reshape(half, exp_dev * cap, width),
            axes,
            split_axis=0,
            concat_axis=0,
            axis_index_groups=halves,
            tiled=True,
        ).reshape(slots, width)

    def experts(rows):
        weights = (routed_gate_weight, routed_up_weight, routed_down_weight)
        if cap % 16 == 0:
            rows = rows.reshape(half, exp_dev * cap, width)
            return ffn(rows, *weights, cap).reshape(slots, width)
        order = (half, exp_dev, cap, width)
        rows = rows.reshape(order).transpose(1, 0, 2, 3).reshape(1, slots, width)
        done = ffn(rows, *weights, half * cap)
        return done.reshape(exp_dev, half, cap, width).transpose(1, 0, 2, 3).reshape(slots, width)

    key_rows, key_cols = key_matrix.shape
    vdim = head_norm_gain.shape[0]
    routes_t, scores_t = routes.T, chosen_router_scores.T
    within, starts, message = call(
        state_kernel,
        (
            like((key_rows, key_cols), jnp.float32),
            like((key_rows // BLOCK, vdim, key_cols), jnp.float32),
            like((seq, vdim + MSG_PAD, key_cols)),
        ),
        key_matrix,
        value_matrix,
        channel_decay_input,
        head_decay_offset.T,
        routes_t,
        scores_t,
    )
    arrived = lax.all_to_all(message, "sp", split_axis=0, concat_axis=0, tiled=True)
    residual_far = lax.ppermute(residual, "sp", swap)
    gated = call(
        mixer_kernel,
        like(value_matrix.shape),
        place.reshape(1),
        queries,
        key_matrix,
        value_matrix,
        within,
        starts,
        arrived,
        output_gate_input,
        head_norm_gain.reshape(1, vdim),
        scalars=1,
        loose=(5,),
    )
    stacked = gated.reshape(heads_axis, tok_count, gated.shape[1])
    stacked = lax.all_to_all(stacked, "tp", split_axis=0, concat_axis=0, tiled=True)
    held_near, weights_near, held_far, weights_far = tables(
        jnp.stack([first_expert, far_place]), routes_t, scores_t, arrived, slots, cap
    )
    stacked_far = lax.ppermute(stacked, "sp", swap)
    gain = expert_norm_gain.reshape(1, width)
    sent_near, middle, normed = project(
        stacked, mixer_output_weight, residual, gain, held_near, True
    )
    arrived_near = spread(sent_near)
    base = ffn(
        normed[None],
        common_gate_weight[None],
        common_up_weight[None],
        common_down_weight[None],
        tok_count,
        add=middle,
    )[0]
    (sent_far,) = project(stacked_far, mixer_output_weight, residual_far, gain, held_far, False)
    arrived_far = spread(sent_far)
    done_near = experts(arrived_near)
    done_far = experts(arrived_far)
    back_far = spread(done_far)
    back_near = spread(done_near)
    rows = like((tok_count, width))
    far = weigh(rows, weights_far, back_far)
    from_far = lax.ppermute(far, "sp", swap)
    return weigh(rows, weights_near, back_near, base, from_far)


def solution(mesh):
    placed = (
        P("sp", "tp"),
        P("sp", "tp"),
        P("sp", "tp"),
        P("sp", "tp"),
        P("sp", "tp"),
        P("sp", "tp"),
        P(),
        P(("sp", "tp"), None),
        P(),
        P(),
        P(("sp", "tp"), None),
        P(("sp", "tp"), None),
        P(("sp", "tp"), None, None),
        P(("sp", "tp"), None, None),
        P(("sp", "tp"), None, None),
        P(),
        P(),
        P(),
    )
    return jax.shard_map(
        on_device, mesh=mesh, in_specs=placed, out_specs=P(("sp", "tp"), None), check_vma=False
    )
```

```python
import functools

import jax
import jax.numpy as jnp
from jax import lax
from jax.experimental import pallas as pl
from jax.experimental.pallas import tpu as pltpu
from jax.sharding import PartitionSpec as P

KEY_CHANNELS = 64
BLOCK = 64
TOP_K = 4
MSG_PAD = 16
ROOM = 48 << 20

eps_norm = 1e-06
decay_running = 16.0
routed_scale = 2.5


def lane_head(shape):
    return lax.broadcasted_iota(jnp.int32, shape, 1) // KEY_CHANNELS


def two_pieces(value):
    high = value.astype(jnp.bfloat16).astype(jnp.float32)
    return high, value - high


def state_kernel(
    k_ref, v_ref, c_ref, o_ref, routes_ref, scores_ref, within_ref, starts_ref, msg_ref
):
    rows, width = k_ref.shape
    heads = o_ref.shape[0]
    vdim = v_ref.shape[1] // heads
    x = c_ref[...].astype(jnp.float32)
    decay = (jnp.minimum(x, 0.0) - jnp.log1p(jnp.exp(-jnp.abs(x)))) / decay_running
    columns_of = (
        lax.broadcasted_iota(jnp.int32, (heads, width), 0) == lane_head((heads, width))
    ).astype(jnp.float32)
    decay = decay + lax.dot_general(
        o_ref[...],
        columns_of,
        (((0,), (0,)), ((), ())),
        precision=lax.Precision.HIGHEST,
        preferred_element_type=jnp.float32,
    )
    lower = lax.broadcasted_iota(jnp.int32, (BLOCK, BLOCK), 0) >= lax.broadcasted_iota(
        jnp.int32, (BLOCK, BLOCK), 1
    )
    lower = lower.astype(jnp.float32)
    state_head = lane_head((vdim, width))
    state = jnp.zeros((vdim, width), jnp.float32)
    total = jnp.zeros((1, width), jnp.float32)
    for n in range(rows // BLOCK):
        at = slice(n * BLOCK, (n + 1) * BLOCK)
        within = jnp.dot(
            lower,
            decay[at],
            precision=lax.Precision.HIGHEST,
            preferred_element_type=jnp.float32,
        )
        within_ref[at, :] = within
        starts_ref[n] = state
        last = within[BLOCK - 1 : BLOCK]
        tail = (k_ref[at, :].astype(jnp.float32) * jnp.exp(last - within)).astype(jnp.bfloat16)
        added = jnp.zeros((vdim, width), jnp.float32)
        for h in range(heads):
            one = lax.dot_general(
                v_ref[at, h * vdim : (h + 1) * vdim],
                tail,
                (((0,), (0,)), ((), ())),
                preferred_element_type=jnp.float32,
            )
            added = jnp.where(state_head == h, one, added)
        state = state * jnp.exp(last) + added
        total = total + last
    factor = jnp.exp(total)
    tail_rows = jnp.zeros((MSG_PAD, width), jnp.float32)
    row = lax.broadcasted_iota(jnp.int32, (MSG_PAD, width), 0)
    scores = scores_ref[...]
    place = 0
    for value in two_pieces(factor) + (routes_ref[...].astype(jnp.float32),) + two_pieces(scores):
        for r in range(value.shape[0]):
            tail_rows = jnp.where(row == place, value[r : r + 1], tail_rows)
            place += 1
    tail_rows = tail_rows.astype(jnp.bfloat16)
    state = state.astype(jnp.bfloat16)
    for j in range(msg_ref.shape[0]):
        msg_ref[j, :vdim, :] = state
        msg_ref[j, vdim:, :] = tail_rows


def mixer_kernel(
    place_ref, q_ref, k_ref, v_ref, within_ref, starts_ref, msg_ref, gate_ref, gain_ref, out_ref
):
    rows, width = k_ref.shape
    heads = width // KEY_CHANNELS
    vdim = v_ref.shape[1] // heads

    def hop(j, carried):
        message = msg_ref[j].astype(jnp.float32)
        factor = message[vdim : vdim + 1] + message[vdim + 1 : vdim + 2]
        return carried * factor + message[:vdim]

    carried = lax.fori_loop(0, place_ref[0], hop, jnp.zeros((vdim, width), jnp.float32))
    head_of = lane_head((BLOCK, width))
    causal = lax.broadcasted_iota(jnp.int32, (heads * BLOCK, BLOCK), 0) % BLOCK >= (
        lax.broadcasted_iota(jnp.int32, (heads * BLOCK, BLOCK), 1)
    )
    gain = gain_ref[...]
    before = jnp.zeros((1, width), jnp.float32)
    for n in range(rows // BLOCK):
        at = slice(n * BLOCK, (n + 1) * BLOCK)
        within = within_ref[at, :]
        queries = q_ref[at, :].astype(jnp.float32) * (KEY_CHANNELS**-0.5) * jnp.exp(within)
        grown = (k_ref[at, :].astype(jnp.float32) * jnp.exp(-within)).astype(jnp.bfloat16)
        split = jnp.concatenate(
            [jnp.where(head_of == h, queries, 0.0) for h in range(heads)], axis=0
        ).astype(jnp.bfloat16)
        scores = lax.dot_general(
            split, grown, (((1,), (1,)), ((), ())), preferred_element_type=jnp.float32
        )
        scores = jnp.where(causal, scores, 0.0).astype(jnp.bfloat16)
        entering = (starts_ref[n] + jnp.exp(before) * carried).astype(jnp.bfloat16)
        crossed = lax.dot_general(
            split, entering, (((1,), (1,)), ((), ())), preferred_element_type=jnp.float32
        )
        for h in range(heads):
            cols = slice(h * vdim, (h + 1) * vdim)
            own = slice(h * BLOCK, (h + 1) * BLOCK)
            output = crossed[own] + jnp.dot(
                scores[own], v_ref[at, cols], preferred_element_type=jnp.float32
            )
            scale = lax.rsqrt(jnp.mean(output * output, axis=-1, keepdims=True) + eps_norm)
            gate = gate_ref[at, cols].astype(jnp.float32)
            out_ref[at, cols] = (
                output * scale * gain * (gate / (1.0 + jnp.exp(-gate)))
            ).astype(jnp.bfloat16)
        before = before + within[BLOCK - 1 : BLOCK]


def whole(x, loose=False):
    return pl.BlockSpec(
        x.shape,
        lambda *_, rank=len(x.shape): (0,) * rank,
        memory_space=None if loose else pltpu.VMEM,
    )


def call(kernel, out, *args, scalars=0, loose=(), room=None):
    in_specs = [pl.BlockSpec(memory_space=pltpu.SMEM)] * scalars + [
        whole(x, i in loose) for i, x in enumerate(args[scalars:])
    ]
    return pl.pallas_call(
        kernel,
        grid=(1,),
        in_specs=in_specs,
        out_specs=jax.tree.map(whole, out),
        out_shape=out,
        compiler_params=pltpu.CompilerParams(vmem_limit_bytes=room),
    )(*args)


def ffn_kernel(x_ref, gate_ref, up_ref, down_ref, *rest):
    add_ref, out_ref, acc_ref = rest if len(rest) == 3 else (None,) + rest
    step = pl.program_id(1)
    rows = x_ref.shape[0] * x_ref.shape[1]
    x = x_ref[...].reshape(rows, x_ref.shape[2])
    gate_pre = jnp.dot(x, gate_ref[0], preferred_element_type=jnp.float32)
    up_pre = jnp.dot(x, up_ref[0], preferred_element_type=jnp.float32)
    hidden = (gate_pre / (1.0 + jnp.exp(-gate_pre)) * up_pre).astype(jnp.bfloat16)
    part = jnp.dot(hidden, down_ref[0], preferred_element_type=jnp.float32)

    @pl.when(step == 0)
    def _():
        acc_ref[...] = part

    @pl.when(step != 0)
    def _():
        acc_ref[...] += part

    @pl.when(step == pl.num_programs(1) - 1)
    def _():
        whole = acc_ref[...]
        if add_ref is not None:
            whole = whole + add_ref[...].astype(jnp.float32)
        out_ref[...] = whole.astype(out_ref.dtype).reshape(out_ref.shape)


def ffn(rows, gate_weight, up_weight, down_weight, cap, add=None):
    sources, _, width = rows.shape
    count, _, hidden = gate_weight.shape
    steps = 2 if hidden % 256 == 0 else 1
    piece = hidden // steps
    row_spec = pl.BlockSpec(
        (sources, cap, width), lambda e, f: (0, e, 0), memory_space=pltpu.VMEM
    )
    in_specs = [
        pl.BlockSpec((sources, cap, width), lambda e, f: (0, e, 0)),
        pl.BlockSpec((1, width, piece), lambda e, f: (e, 0, f)),
        pl.BlockSpec((1, width, piece), lambda e, f: (e, 0, f)),
        pl.BlockSpec((1, piece, width), lambda e, f: (e, f, 0)),
    ]
    args = [rows, gate_weight, up_weight, down_weight]
    dtype = jnp.bfloat16
    if add is not None:
        in_specs.append(whole(add))
        args.append(add)
        dtype = jnp.float32
    return pl.pallas_call(
        ffn_kernel,
        grid=(count, steps),
        in_specs=in_specs,
        out_specs=row_spec,
        out_shape=jax.ShapeDtypeStruct(rows.shape, dtype),
        scratch_shapes=[pltpu.VMEM((sources * cap, width), jnp.float32)],
        compiler_params=pltpu.CompilerParams(vmem_limit_bytes=None if add is not None else ROOM),
        cost_estimate=pl.CostEstimate(
            flops=6 * rows.shape[0] * rows.shape[1] * width * hidden,
            transcendentals=rows.shape[0] * rows.shape[1] * hidden,
            bytes_accessed=6 * count * width * hidden + 4 * rows.size,
        ),
    )(*args)


def slot_tables(routes, scores, first_expert, held_ref, weight_ref, cap):
    slots, tokens = held_ref.shape
    slot = lax.broadcasted_iota(jnp.int32, (slots, tokens), 0)
    expert = (first_expert + lax.div(slot, jnp.int32(cap))).astype(jnp.float32)
    weights = routed_scale * scores / jnp.sum(scores, axis=0, keepdims=True)
    named = jnp.zeros((slots, tokens), jnp.float32)
    weight = jnp.zeros((slots, tokens), jnp.float32)
    for k in range(TOP_K):
        hit = routes[k : k + 1] == expert
        named = jnp.where(hit, 1.0, named)
        weight = jnp.where(hit, weights[k : k + 1], weight)
    earlier = lax.broadcasted_iota(jnp.int32, (tokens, tokens), 0) < lax.broadcasted_iota(
        jnp.int32, (tokens, tokens), 1
    )
    rank = jnp.dot(
        named.astype(jnp.bfloat16),
        jnp.where(earlier, 1.0, 0.0).astype(jnp.bfloat16),
        preferred_element_type=jnp.float32,
    )
    held = (named > 0) & (rank == lax.rem(slot, jnp.int32(cap)).astype(jnp.float32))
    held_ref[...] = jnp.where(held, 1.0, 0.0).astype(jnp.bfloat16)
    high, low = two_pieces(jnp.where(held, weight, 0.0).T)
    weight_ref[:tokens] = high.astype(jnp.bfloat16)
    weight_ref[tokens:] = low.astype(jnp.bfloat16)


def tables_kernel(
    cap, place_ref, routes_ref, scores_ref, far_ref, held_near, near_w, held_far, far_w
):
    slot_tables(
        routes_ref[...].astype(jnp.float32), scores_ref[...], place_ref[0], held_near, near_w, cap
    )
    far = far_ref[0].astype(jnp.float32)
    at = [far[2 + k * TOP_K : 2 + (k + 1) * TOP_K] for k in range(3)]
    slot_tables(at[0], at[1] + at[2], place_ref[0], held_far, far_w, cap)


def tables(places, routes, scores, arrived, slots, cap):
    tokens = routes.shape[1]
    vdim = arrived.shape[1] - MSG_PAD
    held = jax.ShapeDtypeStruct((slots, tokens), jnp.bfloat16)
    weights = jax.ShapeDtypeStruct((2 * tokens, slots), jnp.bfloat16)

    out = (held, weights, held, weights)
    return pl.pallas_call(
        functools.partial(tables_kernel, cap),
        grid_spec=pltpu.PrefetchScalarGridSpec(
            num_scalar_prefetch=1,
            grid=(1,),
            in_specs=[
                whole(routes),
                whole(scores),
                pl.BlockSpec(
                    (1, MSG_PAD, arrived.shape[2]), lambda i, p: (p[1], vdim // MSG_PAD, 0)
                ),
            ],
            out_specs=jax.tree.map(whole, out),
        ),
        out_shape=out,
        name="tables",
    )(places, routes, scores, arrived)


def pick(held, rows):
    return jnp.dot(held, rows, preferred_element_type=jnp.float32).astype(jnp.bfloat16)


def pack_kernel(held_ref, rows_ref, sent_ref):
    sent_ref[...] = pick(held_ref[...], rows_ref[...])


def project_kernel(
    g_ref, w_ref, res_ref, gain_ref, held_ref, sent_ref, mid_ref, norm_ref, acc_ref
):
    step = pl.program_id(0)
    part = jnp.dot(g_ref[0], w_ref[...], preferred_element_type=jnp.float32)

    @pl.when(step == 0)
    def _():
        acc_ref[...] = res_ref[...].astype(jnp.float32) + part

    @pl.when(step != 0)
    def _():
        acc_ref[...] += part

    @pl.when(step == pl.num_programs(0) - 1)
    def _():
        middle = acc_ref[...].astype(jnp.bfloat16)
        wide = middle.astype(jnp.float32)
        scale = lax.rsqrt(jnp.mean(wide * wide, axis=-1, keepdims=True) + eps_norm)
        normed = (wide * scale * gain_ref[...]).astype(jnp.bfloat16)
        sent_ref[...] = pick(held_ref[...], normed)
        mid_ref[...] = middle
        norm_ref[...] = normed


def project(stacked, weight, residual, gain, held):
    count, tokens, cols = stacked.shape
    width = residual.shape[1]
    slots = held.shape[0]
    rows = jax.ShapeDtypeStruct((tokens, width), jnp.bfloat16)
    out = [jax.ShapeDtypeStruct((slots, width), jnp.bfloat16), rows, rows]

    return pl.pallas_call(
        project_kernel,
        grid=(count,),
        in_specs=[
            pl.BlockSpec((1, tokens, cols), lambda t: (t, 0, 0)),
            pl.BlockSpec((cols, width), lambda t: (t, 0), memory_space=pltpu.VMEM),
            whole(residual),
            whole(gain),
            whole(held),
        ],
        out_specs=[whole(x) for x in out],
        out_shape=out,
        scratch_shapes=[pltpu.VMEM((tokens, width), jnp.float32)],
        name="project",
    )(stacked, weight, residual, gain, held)


def weigh_kernel(weight_ref, results_ref, *rest):
    out_ref, acc_ref = rest[-2:]
    step = pl.program_id(0)
    tokens = out_ref.shape[0]
    both = jnp.dot(weight_ref[...], results_ref[...], preferred_element_type=jnp.float32)
    part = both[:tokens] + both[tokens:]

    @pl.when(step == 0)
    def _():
        acc_ref[...] = part

    @pl.when(step == pl.num_programs(0) - 1)
    def _():
        total = acc_ref[...] + part
        if len(rest) == 4:
            total = total + rest[0][...] + rest[1][...].astype(jnp.float32)
        out_ref[...] = total.astype(jnp.bfloat16)


def weigh(out, weights, results, *more):
    slots, width = results.shape
    piece = slots // 2
    in_specs = [
        pl.BlockSpec((weights.shape[0], piece), lambda k: (0, k), memory_space=pltpu.VMEM),
        pl.BlockSpec((piece, width), lambda k: (k, 0)),
    ]
    if more:
        in_specs += [whole(more[0]), whole(more[1], True)]
    return pl.pallas_call(
        weigh_kernel,
        grid=(2,),
        in_specs=in_specs,
        out_specs=whole(out),
        out_shape=out,
        scratch_shapes=[pltpu.VMEM(out.shape, jnp.float32)],
        compiler_params=pltpu.CompilerParams(vmem_limit_bytes=ROOM if more else None),
    )(weights, results, *more)


def on_device(
    queries,
    key_matrix,
    value_matrix,
    channel_decay_input,
    head_decay_offset,
    output_gate_input,
    head_norm_gain,
    residual,
    mixer_output_weight,
    expert_norm_gain,
    routes,
    chosen_router_scores,
    routed_gate_weight,
    routed_up_weight,
    routed_down_weight,
    common_gate_weight,
    common_up_weight,
    common_down_weight,
):
    seq, heads_axis = lax.axis_size("sp"), lax.axis_size("tp")
    axes = ("sp", "tp")
    devices = seq * heads_axis
    half = devices // 2
    halves = [list(range(half)), list(range(half, devices))]
    swap = [(i, (i + seq // 2) % seq) for i in range(seq)]
    tok_count, width = residual.shape
    exp_dev = routed_gate_weight.shape[0]
    cap = 2 * TOP_K * tok_count // (exp_dev * devices)
    slots = exp_dev * half * cap
    place = lax.axis_index("sp").astype(jnp.int32)
    first_expert = lax.div(place, jnp.int32(seq // 2)) * (exp_dev * half)
    far_place = lax.rem(place + seq // 2, jnp.int32(seq))

    def like(shape, dtype=jnp.bfloat16):
        return jax.ShapeDtypeStruct(shape, dtype)

    def spread(rows):
        return lax.all_to_all(
            rows.reshape(half, exp_dev * cap, width),
            axes,
            split_axis=0,
            concat_axis=0,
            axis_index_groups=halves,
            tiled=True,
        ).reshape(slots, width)

    def experts(rows):
        weights = (routed_gate_weight, routed_up_weight, routed_down_weight)
        if cap % 16 == 0:
            rows = rows.reshape(half, exp_dev * cap, width)
            return ffn(rows, *weights, cap).reshape(slots, width)
        order = (half, exp_dev, cap, width)
        rows = rows.reshape(order).transpose(1, 0, 2, 3).reshape(1, slots, width)
        done = ffn(rows, *weights, half * cap)
        return done.reshape(exp_dev, half, cap, width).transpose(1, 0, 2, 3).reshape(slots, width)

    key_rows, key_cols = key_matrix.shape
    vdim = head_norm_gain.shape[0]
    routes_t, scores_t = routes.T, chosen_router_scores.T
    within, starts, message = call(
        state_kernel,
        (
            like((key_rows, key_cols), jnp.float32),
            like((key_rows // BLOCK, vdim, key_cols), jnp.float32),
            like((seq, vdim + MSG_PAD, key_cols)),
        ),
        key_matrix,
        value_matrix,
        channel_decay_input,
        head_decay_offset.T,
        routes_t,
        scores_t,
    )
    arrived = lax.all_to_all(message, "sp", split_axis=0, concat_axis=0, tiled=True)
    gated = call(
        mixer_kernel,
        like(value_matrix.shape),
        place.reshape(1),
        queries,
        key_matrix,
        value_matrix,
        within,
        starts,
        arrived,
        output_gate_input,
        head_norm_gain.reshape(1, vdim),
        scalars=1,
        loose=(5,),
    )
    stacked = gated.reshape(heads_axis, tok_count, gated.shape[1])
    stacked = lax.all_to_all(stacked, "tp", split_axis=0, concat_axis=0, tiled=True)
    held_near, weights_near, held_far, weights_far = tables(
        jnp.stack([first_expert, far_place]), routes_t, scores_t, arrived, slots, cap
    )
    gain = expert_norm_gain.reshape(1, width)
    sent_near, middle, normed = project(
        stacked, mixer_output_weight, residual, gain, held_near
    )
    arrived_near = spread(sent_near)
    base = ffn(
        normed[None],
        common_gate_weight[None],
        common_up_weight[None],
        common_down_weight[None],
        tok_count,
        add=middle,
    )[0]
    normed_far = lax.ppermute(normed, "sp", swap)
    sent_far = call(pack_kernel, like((slots, width)), held_far, normed_far, room=ROOM)
    arrived_far = spread(sent_far)
    done_near = experts(arrived_near)
    done_far = experts(arrived_far)
    back_far = spread(done_far)
    back_near = spread(done_near)
    rows = like((tok_count, width))
    far = weigh(rows, weights_far, back_far)
    from_far = lax.ppermute(far, "sp", swap)
    return weigh(rows, weights_near, back_near, base, from_far)


def solution(mesh):
    placed = (
        P("sp", "tp"),
        P("sp", "tp"),
        P("sp", "tp"),
        P("sp", "tp"),
        P("sp", "tp"),
        P("sp", "tp"),
        P(),
        P(("sp", "tp"), None),
        P(),
        P(),
        P(("sp", "tp"), None),
        P(("sp", "tp"), None),
        P(("sp", "tp"), None, None),
        P(("sp", "tp"), None, None),
        P(("sp", "tp"), None, None),
        P(),
        P(),
        P(),
    )
    return jax.shard_map(
        on_device, mesh=mesh, in_specs=placed, out_specs=P(("sp", "tp"), None), check_vma=False
    )
```

```python
import functools

import jax
import jax.numpy as jnp
from jax import lax
from jax.experimental import pallas as pl
from jax.experimental.pallas import tpu as pltpu
from jax.sharding import PartitionSpec as P

KEY_CHANNELS = 64
BLOCK = 64
TOP_K = 4
MSG_PAD = 16
ROOM = 48 << 20

eps_norm = 1e-06
decay_running = 16.0
routed_scale = 2.5


def lane_head(shape):
    return lax.broadcasted_iota(jnp.int32, shape, 1) // KEY_CHANNELS


def two_pieces(value):
    high = value.astype(jnp.bfloat16).astype(jnp.float32)
    return high, value - high


def state_kernel(
    k_ref, v_ref, c_ref, o_ref, routes_ref, scores_ref, within_ref, starts_ref, msg_ref
):
    rows, width = k_ref.shape
    heads = o_ref.shape[0]
    vdim = v_ref.shape[1] // heads
    x = c_ref[...].astype(jnp.float32)
    decay = (jnp.minimum(x, 0.0) - jnp.log1p(jnp.exp(-jnp.abs(x)))) / decay_running
    columns_of = (
        lax.broadcasted_iota(jnp.int32, (heads, width), 0) == lane_head((heads, width))
    ).astype(jnp.float32)
    decay = decay + lax.dot_general(
        o_ref[...],
        columns_of,
        (((0,), (0,)), ((), ())),
        precision=lax.Precision.HIGHEST,
        preferred_element_type=jnp.float32,
    )
    lower = lax.broadcasted_iota(jnp.int32, (BLOCK, BLOCK), 0) >= lax.broadcasted_iota(
        jnp.int32, (BLOCK, BLOCK), 1
    )
    lower = lower.astype(jnp.float32)
    state_head = lane_head((vdim, width))
    state = jnp.zeros((vdim, width), jnp.float32)
    total = jnp.zeros((1, width), jnp.float32)
    for n in range(rows // BLOCK):
        at = slice(n * BLOCK, (n + 1) * BLOCK)
        within = jnp.dot(
            lower,
            decay[at],
            precision=lax.Precision.HIGHEST,
            preferred_element_type=jnp.float32,
        )
        within_ref[at, :] = within
        starts_ref[n] = state
        last = within[BLOCK - 1 : BLOCK]
        tail = (k_ref[at, :].astype(jnp.float32) * jnp.exp(last - within)).astype(jnp.bfloat16)
        added = jnp.zeros((vdim, width), jnp.float32)
        for h in range(heads):
            one = lax.dot_general(
                v_ref[at, h * vdim : (h + 1) * vdim],
                tail,
                (((0,), (0,)), ((), ())),
                preferred_element_type=jnp.float32,
            )
            added = jnp.where(state_head == h, one, added)
        state = state * jnp.exp(last) + added
        total = total + last
    factor = jnp.exp(total)
    tail_rows = jnp.zeros((MSG_PAD, width), jnp.float32)
    row = lax.broadcasted_iota(jnp.int32, (MSG_PAD, width), 0)
    scores = scores_ref[...]
    place = 0
    for value in two_pieces(factor) + (routes_ref[...].astype(jnp.float32),) + two_pieces(scores):
        for r in range(value.shape[0]):
            tail_rows = jnp.where(row == place, value[r : r + 1], tail_rows)
            place += 1
    tail_rows = tail_rows.astype(jnp.bfloat16)
    state = state.astype(jnp.bfloat16)
    for j in range(msg_ref.shape[0]):
        msg_ref[j, :vdim, :] = state
        msg_ref[j, vdim:, :] = tail_rows


def mixer_kernel(
    place_ref, q_ref, k_ref, v_ref, within_ref, starts_ref, msg_ref, gate_ref, gain_ref, out_ref
):
    rows, width = k_ref.shape
    heads = width // KEY_CHANNELS
    vdim = v_ref.shape[1] // heads

    def hop(j, carried):
        message = msg_ref[j].astype(jnp.float32)
        factor = message[vdim : vdim + 1] + message[vdim + 1 : vdim + 2]
        return carried * factor + message[:vdim]

    carried = lax.fori_loop(0, place_ref[0], hop, jnp.zeros((vdim, width), jnp.float32))
    head_of = lane_head((BLOCK, width))
    causal = lax.broadcasted_iota(jnp.int32, (heads * BLOCK, BLOCK), 0) % BLOCK >= (
        lax.broadcasted_iota(jnp.int32, (heads * BLOCK, BLOCK), 1)
    )
    gain = gain_ref[...]
    before = jnp.zeros((1, width), jnp.float32)
    for n in range(rows // BLOCK):
        at = slice(n * BLOCK, (n + 1) * BLOCK)
        within = within_ref[at, :]
        queries = q_ref[at, :].astype(jnp.float32) * (KEY_CHANNELS**-0.5) * jnp.exp(within)
        grown = (k_ref[at, :].astype(jnp.float32) * jnp.exp(-within)).astype(jnp.bfloat16)
        split = jnp.concatenate(
            [jnp.where(head_of == h, queries, 0.0) for h in range(heads)], axis=0
        ).astype(jnp.bfloat16)
        scores = lax.dot_general(
            split, grown, (((1,), (1,)), ((), ())), preferred_element_type=jnp.float32
        )
        scores = jnp.where(causal, scores, 0.0).astype(jnp.bfloat16)
        entering = (starts_ref[n] + jnp.exp(before) * carried).astype(jnp.bfloat16)
        crossed = lax.dot_general(
            split, entering, (((1,), (1,)), ((), ())), preferred_element_type=jnp.float32
        )
        for h in range(heads):
            cols = slice(h * vdim, (h + 1) * vdim)
            own = slice(h * BLOCK, (h + 1) * BLOCK)
            output = crossed[own] + jnp.dot(
                scores[own], v_ref[at, cols], preferred_element_type=jnp.float32
            )
            scale = lax.rsqrt(jnp.mean(output * output, axis=-1, keepdims=True) + eps_norm)
            gate = gate_ref[at, cols].astype(jnp.float32)
            out_ref[at, cols] = (
                output * scale * gain * (gate / (1.0 + jnp.exp(-gate)))
            ).astype(jnp.bfloat16)
        before = before + within[BLOCK - 1 : BLOCK]


def whole(x, loose=False):
    return pl.BlockSpec(
        x.shape,
        lambda *_, rank=len(x.shape): (0,) * rank,
        memory_space=None if loose else pltpu.VMEM,
    )


def call(kernel, out, *args, scalars=0, loose=(), room=None):
    in_specs = [pl.BlockSpec(memory_space=pltpu.SMEM)] * scalars + [
        whole(x, i in loose) for i, x in enumerate(args[scalars:])
    ]
    return pl.pallas_call(
        kernel,
        grid=(1,),
        in_specs=in_specs,
        out_specs=jax.tree.map(whole, out),
        out_shape=out,
        compiler_params=pltpu.CompilerParams(vmem_limit_bytes=room),
    )(*args)


def ffn_kernel(x_ref, gate_ref, up_ref, down_ref, *rest):
    add_ref, out_ref, acc_ref = rest if len(rest) == 3 else (None,) + rest
    step = pl.program_id(1)
    rows = x_ref.shape[0] * x_ref.shape[1]
    x = x_ref[...].reshape(rows, x_ref.shape[2])
    gate_pre = jnp.dot(x, gate_ref[0], preferred_element_type=jnp.float32)
    up_pre = jnp.dot(x, up_ref[0], preferred_element_type=jnp.float32)
    hidden = (gate_pre / (1.0 + jnp.exp(-gate_pre)) * up_pre).astype(jnp.bfloat16)
    part = jnp.dot(hidden, down_ref[0], preferred_element_type=jnp.float32)

    @pl.when(step == 0)
    def _():
        acc_ref[...] = part

    @pl.when(step != 0)
    def _():
        acc_ref[...] += part

    @pl.when(step == pl.num_programs(1) - 1)
    def _():
        whole = acc_ref[...]
        if add_ref is not None:
            whole = whole + add_ref[...].astype(jnp.float32)
        out_ref[...] = whole.astype(out_ref.dtype).reshape(out_ref.shape)


def ffn(rows, gate_weight, up_weight, down_weight, cap, add=None):
    sources, _, width = rows.shape
    count, _, hidden = gate_weight.shape
    steps = 2 if hidden % 256 == 0 else 1
    piece = hidden // steps
    row_spec = pl.BlockSpec(
        (sources, cap, width), lambda e, f: (0, e, 0), memory_space=pltpu.VMEM
    )
    in_specs = [
        pl.BlockSpec((sources, cap, width), lambda e, f: (0, e, 0)),
        pl.BlockSpec((1, width, piece), lambda e, f: (e, 0, f)),
        pl.BlockSpec((1, width, piece), lambda e, f: (e, 0, f)),
        pl.BlockSpec((1, piece, width), lambda e, f: (e, f, 0)),
    ]
    args = [rows, gate_weight, up_weight, down_weight]
    dtype = jnp.bfloat16
    if add is not None:
        in_specs.append(whole(add))
        args.append(add)
        dtype = jnp.float32
    return pl.pallas_call(
        ffn_kernel,
        grid=(count, steps),
        in_specs=in_specs,
        out_specs=row_spec,
        out_shape=jax.ShapeDtypeStruct(rows.shape, dtype),
        scratch_shapes=[pltpu.VMEM((sources * cap, width), jnp.float32)],
        compiler_params=pltpu.CompilerParams(vmem_limit_bytes=None if add is not None else ROOM),
        cost_estimate=pl.CostEstimate(
            flops=6 * rows.shape[0] * rows.shape[1] * width * hidden,
            transcendentals=rows.shape[0] * rows.shape[1] * hidden,
            bytes_accessed=6 * count * width * hidden + 4 * rows.size,
        ),
    )(*args)


def slot_tables(routes, scores, first_expert, held_ref, weight_ref, cap):
    slots, tokens = held_ref.shape
    slot = lax.broadcasted_iota(jnp.int32, (slots, tokens), 0)
    expert = (first_expert + lax.div(slot, jnp.int32(cap))).astype(jnp.float32)
    weights = routed_scale * scores / jnp.sum(scores, axis=0, keepdims=True)
    named = jnp.zeros((slots, tokens), jnp.float32)
    weight = jnp.zeros((slots, tokens), jnp.float32)
    for k in range(TOP_K):
        hit = routes[k : k + 1] == expert
        named = jnp.where(hit, 1.0, named)
        weight = jnp.where(hit, weights[k : k + 1], weight)
    earlier = lax.broadcasted_iota(jnp.int32, (tokens, tokens), 0) < lax.broadcasted_iota(
        jnp.int32, (tokens, tokens), 1
    )
    rank = jnp.dot(
        named.astype(jnp.bfloat16),
        jnp.where(earlier, 1.0, 0.0).astype(jnp.bfloat16),
        preferred_element_type=jnp.float32,
    )
    held = (named > 0) & (rank == lax.rem(slot, jnp.int32(cap)).astype(jnp.float32))
    held_ref[...] = jnp.where(held, 1.0, 0.0).astype(jnp.bfloat16)
    high, low = two_pieces(jnp.where(held, weight, 0.0).T)
    weight_ref[:tokens] = high.astype(jnp.bfloat16)
    weight_ref[tokens:] = low.astype(jnp.bfloat16)


def tables_kernel(
    cap, place_ref, routes_ref, scores_ref, far_ref, held_near, near_w, held_far, far_w
):
    slot_tables(
        routes_ref[...].astype(jnp.float32), scores_ref[...], place_ref[0], held_near, near_w, cap
    )
    far = far_ref[0].astype(jnp.float32)
    at = [far[2 + k * TOP_K : 2 + (k + 1) * TOP_K] for k in range(3)]
    slot_tables(at[0], at[1] + at[2], place_ref[0], held_far, far_w, cap)


def tables(places, routes, scores, arrived, slots, cap):
    tokens = routes.shape[1]
    vdim = arrived.shape[1] - MSG_PAD
    held = jax.ShapeDtypeStruct((slots, tokens), jnp.bfloat16)
    weights = jax.ShapeDtypeStruct((2 * tokens, slots), jnp.bfloat16)

    out = (held, weights, held, weights)
    return pl.pallas_call(
        functools.partial(tables_kernel, cap),
        grid_spec=pltpu.PrefetchScalarGridSpec(
            num_scalar_prefetch=1,
            grid=(1,),
            in_specs=[
                whole(routes),
                whole(scores),
                pl.BlockSpec(
                    (1, MSG_PAD, arrived.shape[2]), lambda i, p: (p[1], vdim // MSG_PAD, 0)
                ),
            ],
            out_specs=jax.tree.map(whole, out),
        ),
        out_shape=out,
        name="tables",
    )(places, routes, scores, arrived)


def pick(held, rows):
    return jnp.dot(held, rows, preferred_element_type=jnp.float32).astype(jnp.bfloat16)


def start_all(pairs, sems):
    copies = [pltpu.make_async_copy(src, dst, sems.at[i]) for i, (src, dst) in enumerate(pairs)]
    for copy in copies:
        copy.start()
    return copies


def pieces_of(rows, count):
    return [pl.ds(i * (rows // count), rows // count) for i in range(count)]


def streamed(kernel, out, args, scratch, copies, room=None):
    anywhere = pl.BlockSpec(memory_space=pl.ANY)
    return pl.pallas_call(
        kernel,
        in_specs=[anywhere] * len(args),
        out_specs=jax.tree.map(lambda _: anywhere, out),
        out_shape=out,
        scratch_shapes=[pltpu.VMEM(x.shape, x.dtype) for x in scratch]
        + [pltpu.SemaphoreType.DMA((copies,))],
        compiler_params=pltpu.CompilerParams(vmem_limit_bytes=room),
    )(*args)


PIECES = 4


def store_slots(held, normed, sent, sent_out, sems, first):
    copies = []
    for i, at in enumerate(pieces_of(sent.shape[0], PIECES)):
        sent[at, :] = pick(held[at, :], normed)
        copies.append(
            pltpu.make_async_copy(sent.at[at, :], sent_out.at[at, :], sems.at[first + i])
        )
        copies[-1].start()
    return copies


def pack_kernel(held_in, rows_in, sent_out, held, rows, sent, sems):
    loads = start_all([(held_in, held), (rows_in, rows)], sems)
    for copy in loads:
        copy.wait()
    for copy in store_slots(held, rows[...], sent, sent_out, sems, 2):
        copy.wait()


def pack(held, rows):
    out = jax.ShapeDtypeStruct((held.shape[0], rows.shape[1]), rows.dtype)
    args = (held, rows)
    return streamed(pack_kernel, out, args, args + (out,), 2 + PIECES, ROOM)


def project_kernel(
    g_in, w_in, res_in, gain_in, held_in, sent_out, mid_out, norm_out, *buffers
):
    g, w, res, gain, held, sent, mid, norm, sems = buffers
    count, _, _ = g.shape
    pieces = pieces_of(w.shape[0], count)
    loads = start_all(
        [(g_in, g)]
        + [(w_in.at[at, :], w.at[at, :]) for at in pieces]
        + [(res_in, res), (gain_in, gain), (held_in, held)],
        sems,
    )
    loads[0].wait()
    total = None
    for t, at in enumerate(pieces):
        loads[1 + t].wait()
        part = jnp.dot(g[t], w[at, :], preferred_element_type=jnp.float32)
        total = part if total is None else total + part
    for copy in loads[1 + count :]:
        copy.wait()
    middle = (total + res[...].astype(jnp.float32)).astype(jnp.bfloat16)
    wide = middle.astype(jnp.float32)
    scale = lax.rsqrt(jnp.mean(wide * wide, axis=-1, keepdims=True) + eps_norm)
    normed = (wide * scale * gain[...]).astype(jnp.bfloat16)
    norm[...] = normed
    mid[...] = middle
    first = len(loads)
    stores = [
        pltpu.make_async_copy(norm, norm_out, sems.at[first]),
        pltpu.make_async_copy(mid, mid_out, sems.at[first + 1]),
    ]
    for copy in stores:
        copy.start()
    for copy in stores + store_slots(held, normed, sent, sent_out, sems, first + 2):
        copy.wait()


def project(stacked, weight, residual, gain, held):
    rows = jax.ShapeDtypeStruct(residual.shape, jnp.bfloat16)
    out = (jax.ShapeDtypeStruct((held.shape[0], residual.shape[1]), jnp.bfloat16), rows, rows)
    args = (stacked, weight, residual, gain, held)
    return streamed(project_kernel, out, args, args + out, 6 + stacked.shape[0] + PIECES)


def weigh_kernel(more, weight_in, results_in, *refs):
    extra_in, out_ref = refs[:more], refs[more]
    weight, results = refs[more + 1 : more + 3]
    extra = refs[more + 3 : 2 * more + 3]
    done, sems = refs[2 * more + 3 :]
    tokens = done.shape[0]
    pieces = pieces_of(results.shape[0], PIECES)
    loads = start_all(
        [(weight_in, weight)]
        + [(results_in.at[at, :], results.at[at, :]) for at in pieces]
        + list(zip(extra_in, extra)),
        sems,
    )
    loads[0].wait()
    total = None
    for i, at in enumerate(pieces):
        loads[1 + i].wait()
        part = jnp.dot(weight[:, at], results[at, :], preferred_element_type=jnp.float32)
        total = part if total is None else total + part
    total = total[:tokens] + total[tokens:]
    for copy, ref in zip(loads[1 + PIECES :], extra):
        copy.wait()
        total = total + ref[...].astype(jnp.float32)
    done[...] = total.astype(jnp.bfloat16)
    store = pltpu.make_async_copy(done, out_ref, sems.at[len(loads)])
    store.start()
    store.wait()


def weigh(out, weights, results, *more):
    args = (weights, results) + more
    return streamed(
        functools.partial(weigh_kernel, len(more)),
        out,
        args,
        args + (out,),
        2 + PIECES + len(more),
        ROOM if more else None,
    )


def on_device(
    queries,
    key_matrix,
    value_matrix,
    channel_decay_input,
    head_decay_offset,
    output_gate_input,
    head_norm_gain,
    residual,
    mixer_output_weight,
    expert_norm_gain,
    routes,
    chosen_router_scores,
    routed_gate_weight,
    routed_up_weight,
    routed_down_weight,
    common_gate_weight,
    common_up_weight,
    common_down_weight,
):
    seq, heads_axis = lax.axis_size("sp"), lax.axis_size("tp")
    axes = ("sp", "tp")
    devices = seq * heads_axis
    half = devices // 2
    halves = [list(range(half)), list(range(half, devices))]
    swap = [(i, (i + seq // 2) % seq) for i in range(seq)]
    tok_count, width = residual.shape
    exp_dev = routed_gate_weight.shape[0]
    cap = 2 * TOP_K * tok_count // (exp_dev * devices)
    slots = exp_dev * half * cap
    place = lax.axis_index("sp").astype(jnp.int32)
    first_expert = lax.div(place, jnp.int32(seq // 2)) * (exp_dev * half)
    far_place = lax.rem(place + seq // 2, jnp.int32(seq))

    def like(shape, dtype=jnp.bfloat16):
        return jax.ShapeDtypeStruct(shape, dtype)

    def spread(rows):
        return lax.all_to_all(
            rows.reshape(half, exp_dev * cap, width),
            axes,
            split_axis=0,
            concat_axis=0,
            axis_index_groups=halves,
            tiled=True,
        ).reshape(slots, width)

    def experts(rows):
        weights = (routed_gate_weight, routed_up_weight, routed_down_weight)
        if cap % 16 == 0:
            rows = rows.reshape(half, exp_dev * cap, width)
            return ffn(rows, *weights, cap).reshape(slots, width)
        order = (half, exp_dev, cap, width)
        rows = rows.reshape(order).transpose(1, 0, 2, 3).reshape(1, slots, width)
        done = ffn(rows, *weights, half * cap)
        return done.reshape(exp_dev, half, cap, width).transpose(1, 0, 2, 3).reshape(slots, width)

    key_rows, key_cols = key_matrix.shape
    vdim = head_norm_gain.shape[0]
    routes_t, scores_t = routes.T, chosen_router_scores.T
    within, starts, message = call(
        state_kernel,
        (
            like((key_rows, key_cols), jnp.float32),
            like((key_rows // BLOCK, vdim, key_cols), jnp.float32),
            like((seq, vdim + MSG_PAD, key_cols)),
        ),
        key_matrix,
        value_matrix,
        channel_decay_input,
        head_decay_offset.T,
        routes_t,
        scores_t,
    )
    arrived = lax.all_to_all(message, "sp", split_axis=0, concat_axis=0, tiled=True)
    gated = call(
        mixer_kernel,
        like(value_matrix.shape),
        place.reshape(1),
        queries,
        key_matrix,
        value_matrix,
        within,
        starts,
        arrived,
        output_gate_input,
        head_norm_gain.reshape(1, vdim),
        scalars=1,
        loose=(5,),
    )
    stacked = gated.reshape(heads_axis, tok_count, gated.shape[1])
    stacked = lax.all_to_all(stacked, "tp", split_axis=0, concat_axis=0, tiled=True)
    held_near, weights_near, held_far, weights_far = tables(
        jnp.stack([first_expert, far_place]), routes_t, scores_t, arrived, slots, cap
    )
    gain = expert_norm_gain.reshape(1, width)
    sent_near, middle, normed = project(
        stacked, mixer_output_weight, residual, gain, held_near
    )
    arrived_near = spread(sent_near)
    base = ffn(
        normed[None],
        common_gate_weight[None],
        common_up_weight[None],
        common_down_weight[None],
        tok_count,
        add=middle,
    )[0]
    normed_far = lax.ppermute(normed, "sp", swap)
    sent_far = pack(held_far, normed_far)
    arrived_far = spread(sent_far)
    done_near = experts(arrived_near)
    done_far = experts(arrived_far)
    back_far = spread(done_far)
    back_near = spread(done_near)
    rows = like((tok_count, width))
    far = weigh(rows, weights_far, back_far)
    from_far = lax.ppermute(far, "sp", swap)
    return weigh(rows, weights_near, back_near, base, from_far)


def solution(mesh):
    placed = (
        P("sp", "tp"),
        P("sp", "tp"),
        P("sp", "tp"),
        P("sp", "tp"),
        P("sp", "tp"),
        P("sp", "tp"),
        P(),
        P(("sp", "tp"), None),
        P(),
        P(),
        P(("sp", "tp"), None),
        P(("sp", "tp"), None),
        P(("sp", "tp"), None, None),
        P(("sp", "tp"), None, None),
        P(("sp", "tp"), None, None),
        P(),
        P(),
        P(),
    )
    return jax.shard_map(
        on_device, mesh=mesh, in_specs=placed, out_specs=P(("sp", "tp"), None), check_vma=False
    )
```

```python
import functools

import jax
import jax.numpy as jnp
from jax import lax
from jax.experimental import pallas as pl
from jax.experimental.pallas import tpu as pltpu
from jax.sharding import PartitionSpec as P

KEY_CHANNELS = 64
BLOCK = 64
TOP_K = 4
MSG_PAD = 16
ROOM = 48 << 20

eps_norm = 1e-06
decay_running = 16.0
routed_scale = 2.5


def start_all(pairs, sems):
    copies = [pltpu.make_async_copy(src, dst, sems.at[i]) for i, (src, dst) in enumerate(pairs)]
    for copy in copies:
        copy.start()
    return copies


def pieces_of(rows, count):
    return [pl.ds(i * (rows // count), rows // count) for i in range(count)]


def streamed(kernel, out, args, scratch, copies, scalars=0, room=None):
    anywhere = pl.BlockSpec(memory_space=pl.ANY)
    smem = pl.BlockSpec(memory_space=pltpu.SMEM)
    return pl.pallas_call(
        kernel,
        in_specs=[smem] * scalars + [anywhere] * (len(args) - scalars),
        out_specs=jax.tree.map(lambda _: anywhere, out),
        out_shape=out,
        scratch_shapes=[pltpu.VMEM(x.shape, x.dtype) for x in scratch]
        + [pltpu.SemaphoreType.DMA((copies,))],
        compiler_params=pltpu.CompilerParams(vmem_limit_bytes=room),
    )(*args)


PIECES = 4
DEEP = 2


def lane_head(shape):
    return lax.broadcasted_iota(jnp.int32, shape, 1) // KEY_CHANNELS


def two_pieces(value):
    high = value.astype(jnp.bfloat16).astype(jnp.float32)
    return high, value - high


def state_kernel(
    k_ref, v_ref, c_ref, o_ref, routes_ref, scores_ref, within_ref, starts_ref, msg_ref
):
    rows, width = k_ref.shape
    heads = o_ref.shape[0]
    vdim = v_ref.shape[1] // heads
    x = c_ref[...].astype(jnp.float32)
    decay = (jnp.minimum(x, 0.0) - jnp.log1p(jnp.exp(-jnp.abs(x)))) / decay_running
    columns_of = (
        lax.broadcasted_iota(jnp.int32, (heads, width), 0) == lane_head((heads, width))
    ).astype(jnp.float32)
    decay = decay + lax.dot_general(
        o_ref[...],
        columns_of,
        (((0,), (0,)), ((), ())),
        precision=lax.Precision.HIGHEST,
        preferred_element_type=jnp.float32,
    )
    lower = lax.broadcasted_iota(jnp.int32, (BLOCK, BLOCK), 0) >= lax.broadcasted_iota(
        jnp.int32, (BLOCK, BLOCK), 1
    )
    lower = lower.astype(jnp.float32)
    state_head = lane_head((vdim, width))
    state = jnp.zeros((vdim, width), jnp.float32)
    total = jnp.zeros((1, width), jnp.float32)
    for n in range(rows // BLOCK):
        at = slice(n * BLOCK, (n + 1) * BLOCK)
        within = jnp.dot(
            lower,
            decay[at],
            precision=lax.Precision.HIGHEST,
            preferred_element_type=jnp.float32,
        )
        within_ref[at, :] = within
        starts_ref[n] = state
        last = within[BLOCK - 1 : BLOCK]
        tail = (k_ref[at, :].astype(jnp.float32) * jnp.exp(last - within)).astype(jnp.bfloat16)
        added = jnp.zeros((vdim, width), jnp.float32)
        for h in range(heads):
            one = lax.dot_general(
                v_ref[at, h * vdim : (h + 1) * vdim],
                tail,
                (((0,), (0,)), ((), ())),
                preferred_element_type=jnp.float32,
            )
            added = jnp.where(state_head == h, one, added)
        state = state * jnp.exp(last) + added
        total = total + last
    factor = jnp.exp(total)
    tail_rows = jnp.zeros((MSG_PAD, width), jnp.float32)
    row = lax.broadcasted_iota(jnp.int32, (MSG_PAD, width), 0)
    scores = scores_ref[...]
    place = 0
    for value in two_pieces(factor) + (routes_ref[...].astype(jnp.float32),) + two_pieces(scores):
        for r in range(value.shape[0]):
            tail_rows = jnp.where(row == place, value[r : r + 1], tail_rows)
            place += 1
    tail_rows = tail_rows.astype(jnp.bfloat16)
    state = state.astype(jnp.bfloat16)
    for j in range(msg_ref.shape[0]):
        msg_ref[j, :vdim, :] = state
        msg_ref[j, vdim:, :] = tail_rows


def mixer_kernel(
    place_ref,
    gain_in,
    msg_in,
    q_in,
    k_in,
    v_in,
    within_in,
    gate_in,
    starts_in,
    out_ref,
    gain_ref,
    msg_ref,
    q_ref,
    k_ref,
    v_ref,
    within_ref,
    gate_ref,
    starts_ref,
    done_ref,
    sems,
):
    rows, width = k_ref.shape
    heads = width // KEY_CHANNELS
    vdim = v_ref.shape[1] // heads
    blocks = rows // BLOCK
    each = blocks // PIECES
    by_rows = pieces_of(rows, PIECES)
    pairs = [(msg_in, msg_ref), (gain_in, gain_ref)]
    for p, at in enumerate(by_rows):
        for src, dst in (
            (q_in, q_ref),
            (k_in, k_ref),
            (v_in, v_ref),
            (within_in, within_ref),
            (gate_in, gate_ref),
        ):
            pairs.append((src.at[at, :], dst.at[at, :]))
        part = pl.ds(p * each, each)
        pairs.append((starts_in.at[part], starts_ref.at[part]))
    loads = start_all(pairs, sems)
    per_piece = 6

    def hop(j, carried):
        message = msg_ref[j].astype(jnp.float32)
        factor = message[vdim : vdim + 1] + message[vdim + 1 : vdim + 2]
        return carried * factor + message[:vdim]

    loads[0].wait()
    loads[1].wait()
    carried = lax.fori_loop(0, place_ref[0], hop, jnp.zeros((vdim, width), jnp.float32))
    head_of = lane_head((BLOCK, width))
    causal = lax.broadcasted_iota(jnp.int32, (heads * BLOCK, BLOCK), 0) % BLOCK >= (
        lax.broadcasted_iota(jnp.int32, (heads * BLOCK, BLOCK), 1)
    )
    gain = gain_ref[...]
    before = jnp.zeros((1, width), jnp.float32)
    stores = []
    for n in range(blocks):
        if n % each == 0:
            first = 2 + n // each * per_piece
            for copy in loads[first : first + per_piece]:
                copy.wait()
        at = slice(n * BLOCK, (n + 1) * BLOCK)
        within = within_ref[at, :]
        queries = q_ref[at, :].astype(jnp.float32) * (KEY_CHANNELS**-0.5) * jnp.exp(within)
        grown = (k_ref[at, :].astype(jnp.float32) * jnp.exp(-within)).astype(jnp.bfloat16)
        split = jnp.concatenate(
            [jnp.where(head_of == h, queries, 0.0) for h in range(heads)], axis=0
        ).astype(jnp.bfloat16)
        scores = lax.dot_general(
            split, grown, (((1,), (1,)), ((), ())), preferred_element_type=jnp.float32
        )
        scores = jnp.where(causal, scores, 0.0).astype(jnp.bfloat16)
        entering = (starts_ref[n] + jnp.exp(before) * carried).astype(jnp.bfloat16)
        crossed = lax.dot_general(
            split, entering, (((1,), (1,)), ((), ())), preferred_element_type=jnp.float32
        )
        for h in range(heads):
            cols = slice(h * vdim, (h + 1) * vdim)
            own = slice(h * BLOCK, (h + 1) * BLOCK)
            output = crossed[own] + jnp.dot(
                scores[own], v_ref[at, cols], preferred_element_type=jnp.float32
            )
            scale = lax.rsqrt(jnp.mean(output * output, axis=-1, keepdims=True) + eps_norm)
            gate = gate_ref[at, cols].astype(jnp.float32)
            done_ref[at, cols] = (
                output * scale * gain * (gate / (1.0 + jnp.exp(-gate)))
            ).astype(jnp.bfloat16)
        before = before + within[BLOCK - 1 : BLOCK]
        if (n + 1) % each == 0:
            p = n // each
            stores.append(
                pltpu.make_async_copy(
                    done_ref.at[by_rows[p], :],
                    out_ref.at[by_rows[p], :],
                    sems.at[len(loads) + p],
                )
            )
            stores[-1].start()
    for copy in stores:
        copy.wait()


def whole(x, loose=False):
    return pl.BlockSpec(
        x.shape,
        lambda *_, rank=len(x.shape): (0,) * rank,
        memory_space=None if loose else pltpu.VMEM,
    )


def call(kernel, out, *args, scalars=0, loose=(), room=None):
    in_specs = [pl.BlockSpec(memory_space=pltpu.SMEM)] * scalars + [
        whole(x, i in loose) for i, x in enumerate(args[scalars:])
    ]
    return pl.pallas_call(
        kernel,
        grid=(1,),
        in_specs=in_specs,
        out_specs=jax.tree.map(whole, out),
        out_shape=out,
        compiler_params=pltpu.CompilerParams(vmem_limit_bytes=room),
    )(*args)


def ffn_kernel(x_ref, gate_ref, up_ref, down_ref, *rest):
    add_ref, out_ref, acc_ref = rest if len(rest) == 3 else (None,) + rest
    step = pl.program_id(1)
    rows = x_ref.shape[0] * x_ref.shape[1]
    x = x_ref[...].reshape(rows, x_ref.shape[2])
    gate_pre = jnp.dot(x, gate_ref[0], preferred_element_type=jnp.float32)
    up_pre = jnp.dot(x, up_ref[0], preferred_element_type=jnp.float32)
    hidden = (gate_pre / (1.0 + jnp.exp(-gate_pre)) * up_pre).astype(jnp.bfloat16)
    part = jnp.dot(hidden, down_ref[0], preferred_element_type=jnp.float32)

    @pl.when(step == 0)
    def _():
        acc_ref[...] = part

    @pl.when(step != 0)
    def _():
        acc_ref[...] += part

    @pl.when(step == pl.num_programs(1) - 1)
    def _():
        whole = acc_ref[...]
        if add_ref is not None:
            whole = whole + add_ref[...].astype(jnp.float32)
        out_ref[...] = whole.astype(out_ref.dtype).reshape(out_ref.shape)


def ffn(rows, gate_weight, up_weight, down_weight, cap, add=None):
    sources, _, width = rows.shape
    count, _, hidden = gate_weight.shape
    steps = 2 if hidden % 256 == 0 else 1
    piece = hidden // steps
    row_spec = pl.BlockSpec(
        (sources, cap, width), lambda e, f: (0, e, 0), memory_space=pltpu.VMEM
    )
    in_specs = [
        pl.BlockSpec((sources, cap, width), lambda e, f: (0, e, 0)),
        pl.BlockSpec((1, width, piece), lambda e, f: (e, 0, f)),
        pl.BlockSpec((1, width, piece), lambda e, f: (e, 0, f)),
        pl.BlockSpec((1, piece, width), lambda e, f: (e, f, 0)),
    ]
    args = [rows, gate_weight, up_weight, down_weight]
    dtype = jnp.bfloat16
    if add is not None:
        in_specs.append(whole(add))
        args.append(add)
        dtype = jnp.float32
    return pl.pallas_call(
        ffn_kernel,
        grid=(count, steps),
        in_specs=in_specs,
        out_specs=row_spec,
        out_shape=jax.ShapeDtypeStruct(rows.shape, dtype),
        scratch_shapes=[pltpu.VMEM((sources * cap, width), jnp.float32)],
        compiler_params=pltpu.CompilerParams(vmem_limit_bytes=None if add is not None else ROOM),
        cost_estimate=pl.CostEstimate(
            flops=6 * rows.shape[0] * rows.shape[1] * width * hidden,
            transcendentals=rows.shape[0] * rows.shape[1] * hidden,
            bytes_accessed=6 * count * width * hidden + 4 * rows.size,
        ),
    )(*args)


def slot_tables(routes, scores, first_expert, held_ref, weight_ref, cap):
    slots, tokens = held_ref.shape
    slot = lax.broadcasted_iota(jnp.int32, (slots, tokens), 0)
    expert = (first_expert + lax.div(slot, jnp.int32(cap))).astype(jnp.float32)
    weights = routed_scale * scores / jnp.sum(scores, axis=0, keepdims=True)
    named = jnp.zeros((slots, tokens), jnp.float32)
    weight = jnp.zeros((slots, tokens), jnp.float32)
    for k in range(TOP_K):
        hit = routes[k : k + 1] == expert
        named = jnp.where(hit, 1.0, named)
        weight = jnp.where(hit, weights[k : k + 1], weight)
    earlier = lax.broadcasted_iota(jnp.int32, (tokens, tokens), 0) < lax.broadcasted_iota(
        jnp.int32, (tokens, tokens), 1
    )
    rank = jnp.dot(
        named.astype(jnp.bfloat16),
        jnp.where(earlier, 1.0, 0.0).astype(jnp.bfloat16),
        preferred_element_type=jnp.float32,
    )
    held = (named > 0) & (rank == lax.rem(slot, jnp.int32(cap)).astype(jnp.float32))
    held_ref[...] = jnp.where(held, 1.0, 0.0).astype(jnp.bfloat16)
    high, low = two_pieces(jnp.where(held, weight, 0.0).T)
    weight_ref[:tokens] = high.astype(jnp.bfloat16)
    weight_ref[tokens:] = low.astype(jnp.bfloat16)


def tables_kernel(
    cap, place_ref, routes_ref, scores_ref, far_ref, held_near, near_w, held_far, far_w
):
    slot_tables(
        routes_ref[...].astype(jnp.float32), scores_ref[...], place_ref[0], held_near, near_w, cap
    )
    far = far_ref[0].astype(jnp.float32)
    at = [far[2 + k * TOP_K : 2 + (k + 1) * TOP_K] for k in range(3)]
    slot_tables(at[0], at[1] + at[2], place_ref[0], held_far, far_w, cap)


def tables(places, routes, scores, arrived, slots, cap):
    tokens = routes.shape[1]
    vdim = arrived.shape[1] - MSG_PAD
    held = jax.ShapeDtypeStruct((slots, tokens), jnp.bfloat16)
    weights = jax.ShapeDtypeStruct((2 * tokens, slots), jnp.bfloat16)

    out = (held, weights, held, weights)
    return pl.pallas_call(
        functools.partial(tables_kernel, cap),
        grid_spec=pltpu.PrefetchScalarGridSpec(
            num_scalar_prefetch=1,
            grid=(1,),
            in_specs=[
                whole(routes),
                whole(scores),
                pl.BlockSpec(
                    (1, MSG_PAD, arrived.shape[2]), lambda i, p: (p[1], vdim // MSG_PAD, 0)
                ),
            ],
            out_specs=jax.tree.map(whole, out),
        ),
        out_shape=out,
        name="tables",
    )(places, routes, scores, arrived)


def pick(held, rows):
    return jnp.dot(held, rows, preferred_element_type=jnp.float32).astype(jnp.bfloat16)


def store_slots(held, normed, sent, sent_out, sems, first):
    copies = []
    for i, at in enumerate(pieces_of(sent.shape[0], PIECES)):
        sent[at, :] = pick(held[at, :], normed)
        copies.append(
            pltpu.make_async_copy(sent.at[at, :], sent_out.at[at, :], sems.at[first + i])
        )
        copies[-1].start()
    return copies


def pack_kernel(held_in, rows_in, sent_out, held, rows, sent, sems):
    loads = start_all([(held_in, held), (rows_in, rows)], sems)
    for copy in loads:
        copy.wait()
    for copy in store_slots(held, rows[...], sent, sent_out, sems, 2):
        copy.wait()


def pack(held, rows):
    out = jax.ShapeDtypeStruct((held.shape[0], rows.shape[1]), rows.dtype)
    args = (held, rows)
    return streamed(pack_kernel, out, args, args + (out,), 2 + PIECES, room=ROOM)


def project_kernel(
    g_in, w_in, res_in, gain_in, held_in, sent_out, mid_out, norm_out, *buffers
):
    g, w, res, gain, held, sent, mid, norm, sems = buffers
    count, _, _ = g.shape
    pieces = pieces_of(w.shape[0], count)
    loads = start_all(
        [(g_in, g)]
        + [(w_in.at[at, :], w.at[at, :]) for at in pieces]
        + [(res_in, res), (gain_in, gain), (held_in, held)],
        sems,
    )
    loads[0].wait()
    total = None
    for t, at in enumerate(pieces):
        loads[1 + t].wait()
        part = jnp.dot(g[t], w[at, :], preferred_element_type=jnp.float32)
        total = part if total is None else total + part
    for copy in loads[1 + count :]:
        copy.wait()
    middle = (total + res[...].astype(jnp.float32)).astype(jnp.bfloat16)
    wide = middle.astype(jnp.float32)
    scale = lax.rsqrt(jnp.mean(wide * wide, axis=-1, keepdims=True) + eps_norm)
    normed = (wide * scale * gain[...]).astype(jnp.bfloat16)
    norm[...] = normed
    mid[...] = middle
    first = len(loads)
    stores = [
        pltpu.make_async_copy(norm, norm_out, sems.at[first]),
        pltpu.make_async_copy(mid, mid_out, sems.at[first + 1]),
    ]
    for copy in stores:
        copy.start()
    for copy in stores + store_slots(held, normed, sent, sent_out, sems, first + 2):
        copy.wait()


def project(stacked, weight, residual, gain, held):
    rows = jax.ShapeDtypeStruct(residual.shape, jnp.bfloat16)
    out = (jax.ShapeDtypeStruct((held.shape[0], residual.shape[1]), jnp.bfloat16), rows, rows)
    args = (stacked, weight, residual, gain, held)
    return streamed(project_kernel, out, args, args + out, 6 + stacked.shape[0] + PIECES)


def weigh_kernel(more, weight_in, results_in, *refs):
    extra_in, out_ref = refs[:more], refs[more]
    weight, results = refs[more + 1 : more + 3]
    extra = refs[more + 3 : 2 * more + 3]
    done, sems = refs[2 * more + 3 :]
    tokens = done.shape[0]
    pieces = pieces_of(results.shape[0], DEEP)
    loads = start_all(
        [(weight_in, weight)]
        + [(results_in.at[at, :], results.at[at, :]) for at in pieces]
        + list(zip(extra_in, extra)),
        sems,
    )
    loads[0].wait()
    total = None
    for i, at in enumerate(pieces):
        loads[1 + i].wait()
        part = jnp.dot(weight[:, at], results[at, :], preferred_element_type=jnp.float32)
        total = part if total is None else total + part
    total = total[:tokens] + total[tokens:]
    for copy, ref in zip(loads[1 + DEEP :], extra):
        copy.wait()
        total = total + ref[...].astype(jnp.float32)
    done[...] = total.astype(jnp.bfloat16)
    store = pltpu.make_async_copy(done, out_ref, sems.at[len(loads)])
    store.start()
    store.wait()


def weigh(out, weights, results, *more):
    args = (weights, results) + more
    return streamed(
        functools.partial(weigh_kernel, len(more)),
        out,
        args,
        args + (out,),
        2 + DEEP + len(more),
        room=ROOM if more else None,
    )


def on_device(
    queries,
    key_matrix,
    value_matrix,
    channel_decay_input,
    head_decay_offset,
    output_gate_input,
    head_norm_gain,
    residual,
    mixer_output_weight,
    expert_norm_gain,
    routes,
    chosen_router_scores,
    routed_gate_weight,
    routed_up_weight,
    routed_down_weight,
    common_gate_weight,
    common_up_weight,
    common_down_weight,
):
    seq, heads_axis = lax.axis_size("sp"), lax.axis_size("tp")
    axes = ("sp", "tp")
    devices = seq * heads_axis
    half = devices // 2
    halves = [list(range(half)), list(range(half, devices))]
    swap = [(i, (i + seq // 2) % seq) for i in range(seq)]
    tok_count, width = residual.shape
    exp_dev = routed_gate_weight.shape[0]
    cap = 2 * TOP_K * tok_count // (exp_dev * devices)
    slots = exp_dev * half * cap
    place = lax.axis_index("sp").astype(jnp.int32)
    first_expert = lax.div(place, jnp.int32(seq // 2)) * (exp_dev * half)
    far_place = lax.rem(place + seq // 2, jnp.int32(seq))

    def like(shape, dtype=jnp.bfloat16):
        return jax.ShapeDtypeStruct(shape, dtype)

    def spread(rows):
        return lax.all_to_all(
            rows.reshape(half, exp_dev * cap, width),
            axes,
            split_axis=0,
            concat_axis=0,
            axis_index_groups=halves,
            tiled=True,
        ).reshape(slots, width)

    def experts(rows):
        weights = (routed_gate_weight, routed_up_weight, routed_down_weight)
        if cap % 16 == 0:
            rows = rows.reshape(half, exp_dev * cap, width)
            return ffn(rows, *weights, cap).reshape(slots, width)
        order = (half, exp_dev, cap, width)
        rows = rows.reshape(order).transpose(1, 0, 2, 3).reshape(1, slots, width)
        done = ffn(rows, *weights, half * cap)
        return done.reshape(exp_dev, half, cap, width).transpose(1, 0, 2, 3).reshape(slots, width)

    key_rows, key_cols = key_matrix.shape
    vdim = head_norm_gain.shape[0]
    routes_t, scores_t = routes.T, chosen_router_scores.T
    within, starts, message = call(
        state_kernel,
        (
            like((key_rows, key_cols), jnp.float32),
            like((key_rows // BLOCK, vdim, key_cols), jnp.float32),
            like((seq, vdim + MSG_PAD, key_cols)),
        ),
        key_matrix,
        value_matrix,
        channel_decay_input,
        head_decay_offset.T,
        routes_t,
        scores_t,
    )
    arrived = lax.all_to_all(message, "sp", split_axis=0, concat_axis=0, tiled=True)
    gated_args = (
        place.reshape(1),
        head_norm_gain.reshape(1, vdim),
        arrived,
        queries,
        key_matrix,
        value_matrix,
        within,
        output_gate_input,
        starts,
    )
    gated_like = like(value_matrix.shape)
    gated = streamed(
        mixer_kernel,
        gated_like,
        gated_args,
        gated_args[1:] + (gated_like,),
        2 + 7 * PIECES,
        scalars=1,
    )
    stacked = gated.reshape(heads_axis, tok_count, gated.shape[1])
    stacked = lax.all_to_all(stacked, "tp", split_axis=0, concat_axis=0, tiled=True)
    held_near, weights_near, held_far, weights_far = tables(
        jnp.stack([first_expert, far_place]), routes_t, scores_t, arrived, slots, cap
    )
    gain = expert_norm_gain.reshape(1, width)
    sent_near, middle, normed = project(
        stacked, mixer_output_weight, residual, gain, held_near
    )
    arrived_near = spread(sent_near)
    base = ffn(
        normed[None],
        common_gate_weight[None],
        common_up_weight[None],
        common_down_weight[None],
        tok_count,
        add=middle,
    )[0]
    normed_far = lax.ppermute(normed, "sp", swap)
    sent_far = pack(held_far, normed_far)
    arrived_far = spread(sent_far)
    done_near = experts(arrived_near)
    done_far = experts(arrived_far)
    back_far = spread(done_far)
    back_near = spread(done_near)
    rows = like((tok_count, width))
    far = weigh(rows, weights_far, back_far)
    from_far = lax.ppermute(far, "sp", swap)
    return weigh(rows, weights_near, back_near, base, from_far)


def solution(mesh):
    placed = (
        P("sp", "tp"),
        P("sp", "tp"),
        P("sp", "tp"),
        P("sp", "tp"),
        P("sp", "tp"),
        P("sp", "tp"),
        P(),
        P(("sp", "tp"), None),
        P(),
        P(),
        P(("sp", "tp"), None),
        P(("sp", "tp"), None),
        P(("sp", "tp"), None, None),
        P(("sp", "tp"), None, None),
        P(("sp", "tp"), None, None),
        P(),
        P(),
        P(),
    )
    return jax.shard_map(
        on_device, mesh=mesh, in_specs=placed, out_specs=P(("sp", "tp"), None), check_vma=False
    )
```

```python
import functools

import jax
import jax.numpy as jnp
from jax import lax
from jax.experimental import pallas as pl
from jax.experimental.pallas import tpu as pltpu
from jax.sharding import PartitionSpec as P

KEY_CHANNELS = 64
BLOCK = 64
TOP_K = 4
MSG_PAD = 16
ROOM = 48 << 20

eps_norm = 1e-06
decay_running = 16.0
routed_scale = 2.5


def start_all(pairs, sems):
    copies = [pltpu.make_async_copy(src, dst, sems.at[i]) for i, (src, dst) in enumerate(pairs)]
    for copy in copies:
        copy.start()
    return copies


def pieces_of(rows, count):
    return [pl.ds(i * (rows // count), rows // count) for i in range(count)]


def streamed(kernel, out, args, scratch, copies, scalars=0, room=None):
    anywhere = pl.BlockSpec(memory_space=pl.ANY)
    smem = pl.BlockSpec(memory_space=pltpu.SMEM)
    return pl.pallas_call(
        kernel,
        in_specs=[smem] * scalars + [anywhere] * (len(args) - scalars),
        out_specs=jax.tree.map(lambda _: anywhere, out),
        out_shape=out,
        scratch_shapes=[pltpu.VMEM(x.shape, x.dtype) for x in scratch]
        + [pltpu.SemaphoreType.DMA((copies,))],
        compiler_params=pltpu.CompilerParams(vmem_limit_bytes=room),
    )(*args)


PIECES = 4
DEEP = 2


def lane_head(shape):
    return lax.broadcasted_iota(jnp.int32, shape, 1) // KEY_CHANNELS


def two_pieces(value):
    high = value.astype(jnp.bfloat16).astype(jnp.float32)
    return high, value - high


def state_kernel(
    k_ref, v_ref, c_ref, o_ref, routes_ref, scores_ref, within_ref, starts_ref, msg_ref
):
    rows, width = k_ref.shape
    heads = o_ref.shape[0]
    vdim = v_ref.shape[1] // heads
    x = c_ref[...].astype(jnp.float32)
    decay = (jnp.minimum(x, 0.0) - jnp.log1p(jnp.exp(-jnp.abs(x)))) / decay_running
    columns_of = (
        lax.broadcasted_iota(jnp.int32, (heads, width), 0) == lane_head((heads, width))
    ).astype(jnp.float32)
    decay = decay + lax.dot_general(
        o_ref[...],
        columns_of,
        (((0,), (0,)), ((), ())),
        precision=lax.Precision.HIGHEST,
        preferred_element_type=jnp.float32,
    )
    lower = lax.broadcasted_iota(jnp.int32, (BLOCK, BLOCK), 0) >= lax.broadcasted_iota(
        jnp.int32, (BLOCK, BLOCK), 1
    )
    lower = lower.astype(jnp.float32)
    state_head = lane_head((vdim, width))
    state = jnp.zeros((vdim, width), jnp.float32)
    total = jnp.zeros((1, width), jnp.float32)
    for n in range(rows // BLOCK):
        at = slice(n * BLOCK, (n + 1) * BLOCK)
        within = jnp.dot(
            lower,
            decay[at],
            precision=lax.Precision.HIGHEST,
            preferred_element_type=jnp.float32,
        )
        within_ref[at, :] = within
        starts_ref[n] = state
        last = within[BLOCK - 1 : BLOCK]
        tail = (k_ref[at, :].astype(jnp.float32) * jnp.exp(last - within)).astype(jnp.bfloat16)
        added = jnp.zeros((vdim, width), jnp.float32)
        for h in range(heads):
            one = lax.dot_general(
                v_ref[at, h * vdim : (h + 1) * vdim],
                tail,
                (((0,), (0,)), ((), ())),
                preferred_element_type=jnp.float32,
            )
            added = jnp.where(state_head == h, one, added)
        state = state * jnp.exp(last) + added
        total = total + last
    factor = jnp.exp(total)
    tail_rows = jnp.zeros((MSG_PAD, width), jnp.float32)
    row = lax.broadcasted_iota(jnp.int32, (MSG_PAD, width), 0)
    scores = scores_ref[...]
    place = 0
    for value in two_pieces(factor) + (routes_ref[...].astype(jnp.float32),) + two_pieces(scores):
        for r in range(value.shape[0]):
            tail_rows = jnp.where(row == place, value[r : r + 1], tail_rows)
            place += 1
    tail_rows = tail_rows.astype(jnp.bfloat16)
    state = state.astype(jnp.bfloat16)
    for j in range(msg_ref.shape[0]):
        msg_ref[j, :vdim, :] = state
        msg_ref[j, vdim:, :] = tail_rows


def mixer_kernel(
    place_ref, q_ref, k_ref, v_ref, within_ref, starts_ref, msg_ref, gate_ref, gain_ref, out_ref
):
    rows, width = k_ref.shape
    heads = width // KEY_CHANNELS
    vdim = v_ref.shape[1] // heads

    def hop(j, carried):
        message = msg_ref[j].astype(jnp.float32)
        factor = message[vdim : vdim + 1] + message[vdim + 1 : vdim + 2]
        return carried * factor + message[:vdim]

    carried = lax.fori_loop(0, place_ref[0], hop, jnp.zeros((vdim, width), jnp.float32))
    head_of = lane_head((BLOCK, width))
    causal = lax.broadcasted_iota(jnp.int32, (heads * BLOCK, BLOCK), 0) % BLOCK >= (
        lax.broadcasted_iota(jnp.int32, (heads * BLOCK, BLOCK), 1)
    )
    gain = gain_ref[...]
    before = jnp.zeros((1, width), jnp.float32)
    for n in range(rows // BLOCK):
        at = slice(n * BLOCK, (n + 1) * BLOCK)
        within = within_ref[at, :]
        queries = q_ref[at, :].astype(jnp.float32) * (KEY_CHANNELS**-0.5) * jnp.exp(within)
        grown = (k_ref[at, :].astype(jnp.float32) * jnp.exp(-within)).astype(jnp.bfloat16)
        split = jnp.concatenate(
            [jnp.where(head_of == h, queries, 0.0) for h in range(heads)], axis=0
        ).astype(jnp.bfloat16)
        scores = lax.dot_general(
            split, grown, (((1,), (1,)), ((), ())), preferred_element_type=jnp.float32
        )
        scores = jnp.where(causal, scores, 0.0).astype(jnp.bfloat16)
        entering = (starts_ref[n] + jnp.exp(before) * carried).astype(jnp.bfloat16)
        crossed = lax.dot_general(
            split, entering, (((1,), (1,)), ((), ())), preferred_element_type=jnp.float32
        )
        for h in range(heads):
            cols = slice(h * vdim, (h + 1) * vdim)
            own = slice(h * BLOCK, (h + 1) * BLOCK)
            output = crossed[own] + jnp.dot(
                scores[own], v_ref[at, cols], preferred_element_type=jnp.float32
            )
            scale = lax.rsqrt(jnp.mean(output * output, axis=-1, keepdims=True) + eps_norm)
            gate = gate_ref[at, cols].astype(jnp.float32)
            out_ref[at, cols] = (
                output * scale * gain * (gate / (1.0 + jnp.exp(-gate)))
            ).astype(jnp.bfloat16)
        before = before + within[BLOCK - 1 : BLOCK]


def whole(x, loose=False):
    return pl.BlockSpec(
        x.shape,
        lambda *_, rank=len(x.shape): (0,) * rank,
        memory_space=None if loose else pltpu.VMEM,
    )


def call(kernel, out, *args, scalars=0, loose=(), room=None):
    in_specs = [pl.BlockSpec(memory_space=pltpu.SMEM)] * scalars + [
        whole(x, i in loose) for i, x in enumerate(args[scalars:])
    ]
    return pl.pallas_call(
        kernel,
        grid=(1,),
        in_specs=in_specs,
        out_specs=jax.tree.map(whole, out),
        out_shape=out,
        compiler_params=pltpu.CompilerParams(vmem_limit_bytes=room),
    )(*args)


def ffn_kernel(x_ref, gate_ref, up_ref, down_ref, *rest):
    add_ref, out_ref, acc_ref = rest if len(rest) == 3 else (None,) + rest
    step = pl.program_id(1)
    rows = x_ref.shape[0] * x_ref.shape[1]
    x = x_ref[...].reshape(rows, x_ref.shape[2])
    gate_pre = jnp.dot(x, gate_ref[0], preferred_element_type=jnp.float32)
    up_pre = jnp.dot(x, up_ref[0], preferred_element_type=jnp.float32)
    hidden = (gate_pre / (1.0 + jnp.exp(-gate_pre)) * up_pre).astype(jnp.bfloat16)
    part = jnp.dot(hidden, down_ref[0], preferred_element_type=jnp.float32)

    @pl.when(step == 0)
    def _():
        acc_ref[...] = part

    @pl.when(step != 0)
    def _():
        acc_ref[...] += part

    @pl.when(step == pl.num_programs(1) - 1)
    def _():
        whole = acc_ref[...]
        if add_ref is not None:
            whole = whole + add_ref[...].astype(jnp.float32)
        out_ref[...] = whole.astype(out_ref.dtype).reshape(out_ref.shape)


def ffn(rows, gate_weight, up_weight, down_weight, cap, add=None):
    sources, _, width = rows.shape
    count, _, hidden = gate_weight.shape
    steps = 2 if hidden % 256 == 0 else 1
    piece = hidden // steps
    row_spec = pl.BlockSpec(
        (sources, cap, width), lambda e, f: (0, e, 0), memory_space=pltpu.VMEM
    )
    in_specs = [
        pl.BlockSpec((sources, cap, width), lambda e, f: (0, e, 0)),
        pl.BlockSpec((1, width, piece), lambda e, f: (e, 0, f)),
        pl.BlockSpec((1, width, piece), lambda e, f: (e, 0, f)),
        pl.BlockSpec((1, piece, width), lambda e, f: (e, f, 0)),
    ]
    args = [rows, gate_weight, up_weight, down_weight]
    dtype = jnp.bfloat16
    if add is not None:
        in_specs.append(whole(add))
        args.append(add)
        dtype = jnp.float32
    return pl.pallas_call(
        ffn_kernel,
        grid=(count, steps),
        in_specs=in_specs,
        out_specs=row_spec,
        out_shape=jax.ShapeDtypeStruct(rows.shape, dtype),
        scratch_shapes=[pltpu.VMEM((sources * cap, width), jnp.float32)],
        compiler_params=pltpu.CompilerParams(vmem_limit_bytes=None if add is not None else ROOM),
        cost_estimate=pl.CostEstimate(
            flops=6 * rows.shape[0] * rows.shape[1] * width * hidden,
            transcendentals=rows.shape[0] * rows.shape[1] * hidden,
            bytes_accessed=6 * count * width * hidden + 4 * rows.size,
        ),
    )(*args)


def slot_tables(routes, scores, first_expert, held_ref, weight_ref, cap):
    slots, tokens = held_ref.shape
    slot = lax.broadcasted_iota(jnp.int32, (slots, tokens), 0)
    expert = (first_expert + lax.div(slot, jnp.int32(cap))).astype(jnp.float32)
    weights = routed_scale * scores / jnp.sum(scores, axis=0, keepdims=True)
    named = jnp.zeros((slots, tokens), jnp.float32)
    weight = jnp.zeros((slots, tokens), jnp.float32)
    for k in range(TOP_K):
        hit = routes[k : k + 1] == expert
        named = jnp.where(hit, 1.0, named)
        weight = jnp.where(hit, weights[k : k + 1], weight)
    earlier = lax.broadcasted_iota(jnp.int32, (tokens, tokens), 0) < lax.broadcasted_iota(
        jnp.int32, (tokens, tokens), 1
    )
    rank = jnp.dot(
        named.astype(jnp.bfloat16),
        jnp.where(earlier, 1.0, 0.0).astype(jnp.bfloat16),
        preferred_element_type=jnp.float32,
    )
    held = (named > 0) & (rank == lax.rem(slot, jnp.int32(cap)).astype(jnp.float32))
    held_ref[...] = jnp.where(held, 1.0, 0.0).astype(jnp.bfloat16)
    high, low = two_pieces(jnp.where(held, weight, 0.0).T)
    weight_ref[:tokens] = high.astype(jnp.bfloat16)
    weight_ref[tokens:] = low.astype(jnp.bfloat16)


def tables_kernel(
    cap, place_ref, routes_ref, scores_ref, far_ref, held_near, near_w, held_far, far_w
):
    slot_tables(
        routes_ref[...].astype(jnp.float32), scores_ref[...], place_ref[0], held_near, near_w, cap
    )
    far = far_ref[0].astype(jnp.float32)
    at = [far[2 + k * TOP_K : 2 + (k + 1) * TOP_K] for k in range(3)]
    slot_tables(at[0], at[1] + at[2], place_ref[0], held_far, far_w, cap)


def tables(places, routes, scores, arrived, slots, cap):
    tokens = routes.shape[1]
    vdim = arrived.shape[1] - MSG_PAD
    held = jax.ShapeDtypeStruct((slots, tokens), jnp.bfloat16)
    weights = jax.ShapeDtypeStruct((2 * tokens, slots), jnp.bfloat16)

    out = (held, weights, held, weights)
    return pl.pallas_call(
        functools.partial(tables_kernel, cap),
        grid_spec=pltpu.PrefetchScalarGridSpec(
            num_scalar_prefetch=1,
            grid=(1,),
            in_specs=[
                whole(routes),
                whole(scores),
                pl.BlockSpec(
                    (1, MSG_PAD, arrived.shape[2]), lambda i, p: (p[1], vdim // MSG_PAD, 0)
                ),
            ],
            out_specs=jax.tree.map(whole, out),
        ),
        out_shape=out,
        name="tables",
    )(places, routes, scores, arrived)


def pick(held, rows):
    return jnp.dot(held, rows, preferred_element_type=jnp.float32).astype(jnp.bfloat16)


def store_slots(held, normed, sent, sent_out, sems, first):
    copies = []
    for i, at in enumerate(pieces_of(sent.shape[0], PIECES)):
        sent[at, :] = pick(held[at, :], normed)
        copies.append(
            pltpu.make_async_copy(sent.at[at, :], sent_out.at[at, :], sems.at[first + i])
        )
        copies[-1].start()
    return copies


def pack_kernel(held_in, rows_in, sent_out, held, rows, sent, sems):
    loads = start_all([(held_in, held), (rows_in, rows)], sems)
    for copy in loads:
        copy.wait()
    for copy in store_slots(held, rows[...], sent, sent_out, sems, 2):
        copy.wait()


def pack(held, rows):
    out = jax.ShapeDtypeStruct((held.shape[0], rows.shape[1]), rows.dtype)
    args = (held, rows)
    return streamed(pack_kernel, out, args, args + (out,), 2 + PIECES, room=ROOM)


def project_kernel(
    g_in, w_in, res_in, gain_in, held_in, sent_out, mid_out, norm_out, *buffers
):
    g, w, res, gain, held, sent, mid, norm, sems = buffers
    count, _, _ = g.shape
    pieces = pieces_of(w.shape[0], count)
    loads = start_all(
        [(g_in, g)]
        + [(w_in.at[at, :], w.at[at, :]) for at in pieces]
        + [(res_in, res), (gain_in, gain), (held_in, held)],
        sems,
    )
    loads[0].wait()
    total = None
    for t, at in enumerate(pieces):
        loads[1 + t].wait()
        part = jnp.dot(g[t], w[at, :], preferred_element_type=jnp.float32)
        total = part if total is None else total + part
    for copy in loads[1 + count :]:
        copy.wait()
    middle = (total + res[...].astype(jnp.float32)).astype(jnp.bfloat16)
    wide = middle.astype(jnp.float32)
    scale = lax.rsqrt(jnp.mean(wide * wide, axis=-1, keepdims=True) + eps_norm)
    normed = (wide * scale * gain[...]).astype(jnp.bfloat16)
    norm[...] = normed
    mid[...] = middle
    first = len(loads)
    stores = [
        pltpu.make_async_copy(norm, norm_out, sems.at[first]),
        pltpu.make_async_copy(mid, mid_out, sems.at[first + 1]),
    ]
    for copy in stores:
        copy.start()
    for copy in stores + store_slots(held, normed, sent, sent_out, sems, first + 2):
        copy.wait()


def project(stacked, weight, residual, gain, held):
    rows = jax.ShapeDtypeStruct(residual.shape, jnp.bfloat16)
    out = (jax.ShapeDtypeStruct((held.shape[0], residual.shape[1]), jnp.bfloat16), rows, rows)
    args = (stacked, weight, residual, gain, held)
    return streamed(project_kernel, out, args, args + out, 6 + stacked.shape[0] + PIECES)


def weigh_kernel(more, weight_in, results_in, *refs):
    extra_in, out_ref = refs[:more], refs[more]
    weight, results = refs[more + 1 : more + 3]
    extra = refs[more + 3 : 2 * more + 3]
    done, sems = refs[2 * more + 3 :]
    tokens = done.shape[0]
    pieces = pieces_of(results.shape[0], DEEP)
    loads = start_all(
        [(weight_in, weight)]
        + [(results_in.at[at, :], results.at[at, :]) for at in pieces]
        + list(zip(extra_in, extra)),
        sems,
    )
    loads[0].wait()
    total = None
    for i, at in enumerate(pieces):
        loads[1 + i].wait()
        part = jnp.dot(weight[:, at], results[at, :], preferred_element_type=jnp.float32)
        total = part if total is None else total + part
    total = total[:tokens] + total[tokens:]
    for copy, ref in zip(loads[1 + DEEP :], extra):
        copy.wait()
        total = total + ref[...].astype(jnp.float32)
    done[...] = total.astype(jnp.bfloat16)
    store = pltpu.make_async_copy(done, out_ref, sems.at[len(loads)])
    store.start()
    store.wait()


def weigh(out, weights, results, *more):
    args = (weights, results) + more
    return streamed(
        functools.partial(weigh_kernel, len(more)),
        out,
        args,
        args + (out,),
        2 + DEEP + len(more),
        room=ROOM if more else None,
    )


def on_device(
    queries,
    key_matrix,
    value_matrix,
    channel_decay_input,
    head_decay_offset,
    output_gate_input,
    head_norm_gain,
    residual,
    mixer_output_weight,
    expert_norm_gain,
    routes,
    chosen_router_scores,
    routed_gate_weight,
    routed_up_weight,
    routed_down_weight,
    common_gate_weight,
    common_up_weight,
    common_down_weight,
):
    seq, heads_axis = lax.axis_size("sp"), lax.axis_size("tp")
    axes = ("sp", "tp")
    devices = seq * heads_axis
    half = devices // 2
    halves = [list(range(half)), list(range(half, devices))]
    swap = [(i, (i + seq // 2) % seq) for i in range(seq)]
    tok_count, width = residual.shape
    exp_dev = routed_gate_weight.shape[0]
    cap = 2 * TOP_K * tok_count // (exp_dev * devices)
    slots = exp_dev * half * cap
    place = lax.axis_index("sp").astype(jnp.int32)
    first_expert = lax.div(place, jnp.int32(seq // 2)) * (exp_dev * half)
    far_place = lax.rem(place + seq // 2, jnp.int32(seq))

    def like(shape, dtype=jnp.bfloat16):
        return jax.ShapeDtypeStruct(shape, dtype)

    def spread(rows):
        return lax.all_to_all(
            rows.reshape(half, exp_dev * cap, width),
            axes,
            split_axis=0,
            concat_axis=0,
            axis_index_groups=halves,
            tiled=True,
        ).reshape(slots, width)

    def experts(rows):
        weights = (routed_gate_weight, routed_up_weight, routed_down_weight)
        if cap % 16 == 0:
            rows = rows.reshape(half, exp_dev * cap, width)
            return ffn(rows, *weights, cap).reshape(slots, width)
        order = (half, exp_dev, cap, width)
        rows = rows.reshape(order).transpose(1, 0, 2, 3).reshape(1, slots, width)
        done = ffn(rows, *weights, half * cap)
        return done.reshape(exp_dev, half, cap, width).transpose(1, 0, 2, 3).reshape(slots, width)

    key_rows, key_cols = key_matrix.shape
    vdim = head_norm_gain.shape[0]
    routes_t, scores_t = routes.T, chosen_router_scores.T
    within, starts, message = call(
        state_kernel,
        (
            like((key_rows, key_cols), jnp.float32),
            like((key_rows // BLOCK, vdim, key_cols), jnp.float32),
            like((seq, vdim + MSG_PAD, key_cols)),
        ),
        key_matrix,
        value_matrix,
        channel_decay_input,
        head_decay_offset.T,
        routes_t,
        scores_t,
    )
    arrived = lax.all_to_all(message, "sp", split_axis=0, concat_axis=0, tiled=True)
    gated = call(
        mixer_kernel,
        like(value_matrix.shape),
        place.reshape(1),
        queries,
        key_matrix,
        value_matrix,
        within,
        starts,
        arrived,
        output_gate_input,
        head_norm_gain.reshape(1, vdim),
        scalars=1,
        loose=(5,),
    )
    stacked = gated.reshape(heads_axis, tok_count, gated.shape[1])
    stacked = lax.all_to_all(stacked, "tp", split_axis=0, concat_axis=0, tiled=True)
    held_near, weights_near, held_far, weights_far = tables(
        jnp.stack([first_expert, far_place]), routes_t, scores_t, arrived, slots, cap
    )
    gain = expert_norm_gain.reshape(1, width)
    sent_near, middle, normed = project(
        stacked, mixer_output_weight, residual, gain, held_near
    )
    arrived_near = spread(sent_near)
    base = ffn(
        normed[None],
        common_gate_weight[None],
        common_up_weight[None],
        common_down_weight[None],
        tok_count,
        add=middle,
    )[0]
    normed_far = lax.ppermute(normed, "sp", swap)
    sent_far = pack(held_far, normed_far)
    arrived_far = spread(sent_far)
    done_near = experts(arrived_near)
    done_far = experts(arrived_far)
    back_far = spread(done_far)
    back_near = spread(done_near)
    rows = like((tok_count, width))
    far = weigh(rows, weights_far, back_far)
    from_far = lax.ppermute(far, "sp", swap)
    return weigh(rows, weights_near, back_near, base, from_far)


def solution(mesh):
    placed = (
        P("sp", "tp"),
        P("sp", "tp"),
        P("sp", "tp"),
        P("sp", "tp"),
        P("sp", "tp"),
        P("sp", "tp"),
        P(),
        P(("sp", "tp"), None),
        P(),
        P(),
        P(("sp", "tp"), None),
        P(("sp", "tp"), None),
        P(("sp", "tp"), None, None),
        P(("sp", "tp"), None, None),
        P(("sp", "tp"), None, None),
        P(),
        P(),
        P(),
    )
    return jax.shard_map(
        on_device, mesh=mesh, in_specs=placed, out_specs=P(("sp", "tp"), None), check_vma=False
    )
```

```python
import functools

import jax
import jax.numpy as jnp
from jax import lax
from jax.experimental import pallas as pl
from jax.experimental.pallas import tpu as pltpu
from jax.sharding import PartitionSpec as P

KEY_CHANNELS = 64
BLOCK = 64
TOP_K = 4
MSG_PAD = 16
ROOM = 48 << 20

eps_norm = 1e-06
decay_running = 16.0
routed_scale = 2.5


def start_all(pairs, sems):
    copies = [pltpu.make_async_copy(src, dst, sems.at[i]) for i, (src, dst) in enumerate(pairs)]
    for copy in copies:
        copy.start()
    return copies


def pieces_of(rows, count):
    return [pl.ds(i * (rows // count), rows // count) for i in range(count)]


def streamed(kernel, out, args, scratch, copies, scalars=0, room=None):
    anywhere = pl.BlockSpec(memory_space=pl.ANY)
    smem = pl.BlockSpec(memory_space=pltpu.SMEM)
    return pl.pallas_call(
        kernel,
        in_specs=[smem] * scalars + [anywhere] * (len(args) - scalars),
        out_specs=jax.tree.map(lambda _: anywhere, out),
        out_shape=out,
        scratch_shapes=[pltpu.VMEM(x.shape, x.dtype) for x in scratch]
        + [pltpu.SemaphoreType.DMA((copies,))],
        compiler_params=pltpu.CompilerParams(vmem_limit_bytes=room),
    )(*args)


PIECES = 4
DEEP = 2


def lane_head(shape):
    return lax.broadcasted_iota(jnp.int32, shape, 1) // KEY_CHANNELS


def two_pieces(value):
    high = value.astype(jnp.bfloat16).astype(jnp.float32)
    return high, value - high


def state_kernel(
    k_ref, v_ref, c_ref, o_ref, routes_ref, scores_ref, within_ref, starts_ref, msg_ref
):
    rows, width = k_ref.shape
    heads = o_ref.shape[0]
    vdim = v_ref.shape[1] // heads
    x = c_ref[...].astype(jnp.float32)
    decay = (jnp.minimum(x, 0.0) - jnp.log1p(jnp.exp(-jnp.abs(x)))) / decay_running
    columns_of = (
        lax.broadcasted_iota(jnp.int32, (heads, width), 0) == lane_head((heads, width))
    ).astype(jnp.float32)
    decay = decay + lax.dot_general(
        o_ref[...],
        columns_of,
        (((0,), (0,)), ((), ())),
        precision=lax.Precision.HIGHEST,
        preferred_element_type=jnp.float32,
    )
    lower = lax.broadcasted_iota(jnp.int32, (BLOCK, BLOCK), 0) >= lax.broadcasted_iota(
        jnp.int32, (BLOCK, BLOCK), 1
    )
    lower = lower.astype(jnp.float32)
    state_head = lane_head((vdim, width))
    state = jnp.zeros((vdim, width), jnp.float32)
    total = jnp.zeros((1, width), jnp.float32)
    for n in range(rows // BLOCK):
        at = slice(n * BLOCK, (n + 1) * BLOCK)
        within = jnp.dot(
            lower,
            decay[at],
            precision=lax.Precision.HIGHEST,
            preferred_element_type=jnp.float32,
        )
        within_ref[at, :] = within
        starts_ref[n] = state
        last = within[BLOCK - 1 : BLOCK]
        tail = (k_ref[at, :].astype(jnp.float32) * jnp.exp(last - within)).astype(jnp.bfloat16)
        added = jnp.zeros((vdim, width), jnp.float32)
        for h in range(heads):
            one = lax.dot_general(
                v_ref[at, h * vdim : (h + 1) * vdim],
                tail,
                (((0,), (0,)), ((), ())),
                preferred_element_type=jnp.float32,
            )
            added = jnp.where(state_head == h, one, added)
        state = state * jnp.exp(last) + added
        total = total + last
    factor = jnp.exp(total)
    tail_rows = jnp.zeros((MSG_PAD, width), jnp.float32)
    row = lax.broadcasted_iota(jnp.int32, (MSG_PAD, width), 0)
    scores = scores_ref[...]
    place = 0
    for value in two_pieces(factor) + (routes_ref[...].astype(jnp.float32),) + two_pieces(scores):
        for r in range(value.shape[0]):
            tail_rows = jnp.where(row == place, value[r : r + 1], tail_rows)
            place += 1
    tail_rows = tail_rows.astype(jnp.bfloat16)
    state = state.astype(jnp.bfloat16)
    for j in range(msg_ref.shape[0]):
        msg_ref[j, :vdim, :] = state
        msg_ref[j, vdim:, :] = tail_rows


def mixer_kernel(
    place_ref, q_ref, k_ref, v_ref, within_ref, starts_ref, msg_ref, gate_ref, gain_ref, out_ref
):
    rows, width = k_ref.shape
    heads = width // KEY_CHANNELS
    vdim = v_ref.shape[1] // heads

    def hop(j, carried):
        message = msg_ref[j].astype(jnp.float32)
        factor = message[vdim : vdim + 1] + message[vdim + 1 : vdim + 2]
        return carried * factor + message[:vdim]

    carried = lax.fori_loop(0, place_ref[0], hop, jnp.zeros((vdim, width), jnp.float32))
    head_of = lane_head((BLOCK, width))
    causal = lax.broadcasted_iota(jnp.int32, (heads * BLOCK, BLOCK), 0) % BLOCK >= (
        lax.broadcasted_iota(jnp.int32, (heads * BLOCK, BLOCK), 1)
    )
    gain = gain_ref[...]
    before = jnp.zeros((1, width), jnp.float32)
    for n in range(rows // BLOCK):
        at = slice(n * BLOCK, (n + 1) * BLOCK)
        within = within_ref[at, :]
        queries = q_ref[at, :].astype(jnp.float32) * (KEY_CHANNELS**-0.5) * jnp.exp(within)
        grown = (k_ref[at, :].astype(jnp.float32) * jnp.exp(-within)).astype(jnp.bfloat16)
        split = jnp.concatenate(
            [jnp.where(head_of == h, queries, 0.0) for h in range(heads)], axis=0
        ).astype(jnp.bfloat16)
        scores = lax.dot_general(
            split, grown, (((1,), (1,)), ((), ())), preferred_element_type=jnp.float32
        )
        scores = jnp.where(causal, scores, 0.0).astype(jnp.bfloat16)
        entering = (starts_ref[n] + jnp.exp(before) * carried).astype(jnp.bfloat16)
        crossed = lax.dot_general(
            split, entering, (((1,), (1,)), ((), ())), preferred_element_type=jnp.float32
        )
        for h in range(heads):
            cols = slice(h * vdim, (h + 1) * vdim)
            own = slice(h * BLOCK, (h + 1) * BLOCK)
            output = crossed[own] + jnp.dot(
                scores[own], v_ref[at, cols], preferred_element_type=jnp.float32
            )
            scale = lax.rsqrt(jnp.mean(output * output, axis=-1, keepdims=True) + eps_norm)
            gate = gate_ref[at, cols].astype(jnp.float32)
            out_ref[at, cols] = (
                output * scale * gain * (gate / (1.0 + jnp.exp(-gate)))
            ).astype(jnp.bfloat16)
        before = before + within[BLOCK - 1 : BLOCK]


def whole(x, loose=False):
    return pl.BlockSpec(
        x.shape,
        lambda *_, rank=len(x.shape): (0,) * rank,
        memory_space=None if loose else pltpu.VMEM,
    )


def call(kernel, out, *args, scalars=0, loose=(), room=None):
    in_specs = [pl.BlockSpec(memory_space=pltpu.SMEM)] * scalars + [
        whole(x, i in loose) for i, x in enumerate(args[scalars:])
    ]
    return pl.pallas_call(
        kernel,
        grid=(1,),
        in_specs=in_specs,
        out_specs=jax.tree.map(whole, out),
        out_shape=out,
        compiler_params=pltpu.CompilerParams(vmem_limit_bytes=room),
    )(*args)


def ffn_kernel(x_ref, gate_ref, up_ref, down_ref, *rest):
    add_ref, out_ref, acc_ref = rest if len(rest) == 3 else (None,) + rest
    step = pl.program_id(1)
    rows = x_ref.shape[0] * x_ref.shape[1]
    x = x_ref[...].reshape(rows, x_ref.shape[2])
    gate_pre = jnp.dot(x, gate_ref[0], preferred_element_type=jnp.float32)
    up_pre = jnp.dot(x, up_ref[0], preferred_element_type=jnp.float32)
    hidden = (gate_pre / (1.0 + jnp.exp(-gate_pre)) * up_pre).astype(jnp.bfloat16)
    part = jnp.dot(hidden, down_ref[0], preferred_element_type=jnp.float32)

    @pl.when(step == 0)
    def _():
        acc_ref[...] = part

    @pl.when(step != 0)
    def _():
        acc_ref[...] += part

    @pl.when(step == pl.num_programs(1) - 1)
    def _():
        whole = acc_ref[...]
        if add_ref is not None:
            whole = whole + add_ref[...].astype(jnp.float32)
        out_ref[...] = whole.astype(out_ref.dtype).reshape(out_ref.shape)


def ffn(rows, gate_weight, up_weight, down_weight, cap, add=None):
    sources, _, width = rows.shape
    count, _, hidden = gate_weight.shape
    steps = 2 if hidden % 256 == 0 else 1
    piece = hidden // steps
    row_spec = pl.BlockSpec(
        (sources, cap, width), lambda e, f: (0, e, 0), memory_space=pltpu.VMEM
    )
    in_specs = [
        pl.BlockSpec((sources, cap, width), lambda e, f: (0, e, 0)),
        pl.BlockSpec((1, width, piece), lambda e, f: (e, 0, f)),
        pl.BlockSpec((1, width, piece), lambda e, f: (e, 0, f)),
        pl.BlockSpec((1, piece, width), lambda e, f: (e, f, 0)),
    ]
    args = [rows, gate_weight, up_weight, down_weight]
    dtype = jnp.bfloat16
    if add is not None:
        in_specs.append(whole(add))
        args.append(add)
        dtype = jnp.float32
    return pl.pallas_call(
        ffn_kernel,
        grid=(count, steps),
        in_specs=in_specs,
        out_specs=row_spec,
        out_shape=jax.ShapeDtypeStruct(rows.shape, dtype),
        scratch_shapes=[pltpu.VMEM((sources * cap, width), jnp.float32)],
        compiler_params=pltpu.CompilerParams(vmem_limit_bytes=None if add is not None else ROOM),
        cost_estimate=pl.CostEstimate(
            flops=6 * rows.shape[0] * rows.shape[1] * width * hidden,
            transcendentals=rows.shape[0] * rows.shape[1] * hidden,
            bytes_accessed=6 * count * width * hidden + 4 * rows.size,
        ),
    )(*args)


def slot_tables(routes, scores, first_expert, held_ref, weight_ref, cap):
    slots, tokens = held_ref.shape
    slot = lax.broadcasted_iota(jnp.int32, (slots, tokens), 0)
    expert = (first_expert + lax.div(slot, jnp.int32(cap))).astype(jnp.float32)
    weights = routed_scale * scores / jnp.sum(scores, axis=0, keepdims=True)
    named = jnp.zeros((slots, tokens), jnp.float32)
    weight = jnp.zeros((slots, tokens), jnp.float32)
    for k in range(TOP_K):
        hit = routes[k : k + 1] == expert
        named = jnp.where(hit, 1.0, named)
        weight = jnp.where(hit, weights[k : k + 1], weight)
    earlier = lax.broadcasted_iota(jnp.int32, (tokens, tokens), 0) < lax.broadcasted_iota(
        jnp.int32, (tokens, tokens), 1
    )
    rank = jnp.dot(
        named.astype(jnp.bfloat16),
        jnp.where(earlier, 1.0, 0.0).astype(jnp.bfloat16),
        preferred_element_type=jnp.float32,
    )
    held = (named > 0) & (rank == lax.rem(slot, jnp.int32(cap)).astype(jnp.float32))
    held_ref[...] = jnp.where(held, 1.0, 0.0).astype(jnp.bfloat16)
    high, low = two_pieces(jnp.where(held, weight, 0.0).T)
    weight_ref[:tokens] = high.astype(jnp.bfloat16)
    weight_ref[tokens:] = low.astype(jnp.bfloat16)


def tables_kernel(
    cap, place_ref, routes_ref, scores_ref, far_ref, held_near, near_w, held_far, far_w
):
    slot_tables(
        routes_ref[...].astype(jnp.float32), scores_ref[...], place_ref[0], held_near, near_w, cap
    )
    far = far_ref[0].astype(jnp.float32)
    at = [far[2 + k * TOP_K : 2 + (k + 1) * TOP_K] for k in range(3)]
    slot_tables(at[0], at[1] + at[2], place_ref[0], held_far, far_w, cap)


def tables(places, routes, scores, arrived, slots, cap):
    tokens = routes.shape[1]
    vdim = arrived.shape[1] - MSG_PAD
    held = jax.ShapeDtypeStruct((slots, tokens), jnp.bfloat16)
    weights = jax.ShapeDtypeStruct((2 * tokens, slots), jnp.bfloat16)

    out = (held, weights, held, weights)
    return pl.pallas_call(
        functools.partial(tables_kernel, cap),
        grid_spec=pltpu.PrefetchScalarGridSpec(
            num_scalar_prefetch=1,
            grid=(1,),
            in_specs=[
                whole(routes),
                whole(scores),
                pl.BlockSpec(
                    (1, MSG_PAD, arrived.shape[2]), lambda i, p: (p[1], vdim // MSG_PAD, 0)
                ),
            ],
            out_specs=jax.tree.map(whole, out),
        ),
        out_shape=out,
        name="tables",
    )(places, routes, scores, arrived)


def pick(held, rows):
    return jnp.dot(held, rows, preferred_element_type=jnp.float32).astype(jnp.bfloat16)


def store_slots(held, normed, sent, sent_out, sems, first):
    copies = []
    for i, at in enumerate(pieces_of(sent.shape[0], PIECES)):
        sent[at, :] = pick(held[at, :], normed)
        copies.append(
            pltpu.make_async_copy(sent.at[at, :], sent_out.at[at, :], sems.at[first + i])
        )
        copies[-1].start()
    return copies


def pack_kernel(held_in, outer_in, inner_in, sent_out, held, outer, inner, sent, sems):
    loads = start_all([(held_in, held), (outer_in, outer), (inner_in, inner)], sems)
    for copy in loads:
        copy.wait()
    rows = outer[...] + inner[...]
    for copy in store_slots(held, rows, sent, sent_out, sems, 3):
        copy.wait()


def pack(held, outer, inner):
    out = jax.ShapeDtypeStruct((held.shape[0], outer.shape[1]), outer.dtype)
    args = (held, outer, inner)
    return streamed(pack_kernel, out, args, args + (out,), 3 + PIECES, room=ROOM)


def project_kernel(
    g_in, w_in, res_in, gain_in, held_in, sent_out, mid_out, norm_out, *buffers
):
    g, w, res, gain, held, sent, mid, norm, sems = buffers
    count, _, _ = g.shape
    pieces = pieces_of(w.shape[0], count)
    loads = start_all(
        [(g_in, g)]
        + [(w_in.at[at, :], w.at[at, :]) for at in pieces]
        + [(res_in, res), (gain_in, gain), (held_in, held)],
        sems,
    )
    loads[0].wait()
    total = None
    for t, at in enumerate(pieces):
        loads[1 + t].wait()
        part = jnp.dot(g[t], w[at, :], preferred_element_type=jnp.float32)
        total = part if total is None else total + part
    for copy in loads[1 + count :]:
        copy.wait()
    middle = (total + res[...].astype(jnp.float32)).astype(jnp.bfloat16)
    wide = middle.astype(jnp.float32)
    scale = lax.rsqrt(jnp.mean(wide * wide, axis=-1, keepdims=True) + eps_norm)
    normed = (wide * scale * gain[...]).astype(jnp.bfloat16)
    norm[...] = normed
    mid[...] = middle
    first = len(loads)
    stores = [
        pltpu.make_async_copy(norm, norm_out, sems.at[first]),
        pltpu.make_async_copy(mid, mid_out, sems.at[first + 1]),
    ]
    for copy in stores:
        copy.start()
    for copy in stores + store_slots(held, normed, sent, sent_out, sems, first + 2):
        copy.wait()


def project(stacked, weight, residual, gain, held):
    rows = jax.ShapeDtypeStruct(residual.shape, jnp.bfloat16)
    out = (jax.ShapeDtypeStruct((held.shape[0], residual.shape[1]), jnp.bfloat16), rows, rows)
    args = (stacked, weight, residual, gain, held)
    return streamed(project_kernel, out, args, args + out, 6 + stacked.shape[0] + PIECES)


def weigh_kernel(more, weight_in, results_in, *refs):
    extra_in, out_ref = refs[:more], refs[more]
    weight, results = refs[more + 1 : more + 3]
    extra = refs[more + 3 : 2 * more + 3]
    done, sems = refs[2 * more + 3 :]
    tokens = done.shape[0]
    pieces = pieces_of(results.shape[0], DEEP)
    loads = start_all(
        [(weight_in, weight)]
        + [(results_in.at[at, :], results.at[at, :]) for at in pieces]
        + list(zip(extra_in, extra)),
        sems,
    )
    loads[0].wait()
    total = None
    for i, at in enumerate(pieces):
        loads[1 + i].wait()
        part = jnp.dot(weight[:, at], results[at, :], preferred_element_type=jnp.float32)
        total = part if total is None else total + part
    total = total[:tokens] + total[tokens:]
    for copy, ref in zip(loads[1 + DEEP :], extra):
        copy.wait()
        total = total + ref[...].astype(jnp.float32)
    done[...] = total.astype(jnp.bfloat16)
    store = pltpu.make_async_copy(done, out_ref, sems.at[len(loads)])
    store.start()
    store.wait()


def weigh(out, weights, results, *more):
    args = (weights, results) + more
    return streamed(
        functools.partial(weigh_kernel, len(more)),
        out,
        args,
        args + (out,),
        2 + DEEP + len(more),
        room=ROOM if more else None,
    )


def on_device(
    queries,
    key_matrix,
    value_matrix,
    channel_decay_input,
    head_decay_offset,
    output_gate_input,
    head_norm_gain,
    residual,
    mixer_output_weight,
    expert_norm_gain,
    routes,
    chosen_router_scores,
    routed_gate_weight,
    routed_up_weight,
    routed_down_weight,
    common_gate_weight,
    common_up_weight,
    common_down_weight,
):
    seq, heads_axis = lax.axis_size("sp"), lax.axis_size("tp")
    axes = ("sp", "tp")
    devices = seq * heads_axis
    half = devices // 2
    halves = [list(range(half)), list(range(half, devices))]
    swap = [(i, (i + seq // 2) % seq) for i in range(seq)]
    tok_count, width = residual.shape
    exp_dev = routed_gate_weight.shape[0]
    cap = 2 * TOP_K * tok_count // (exp_dev * devices)
    slots = exp_dev * half * cap
    place = lax.axis_index("sp").astype(jnp.int32)
    first_expert = lax.div(place, jnp.int32(seq // 2)) * (exp_dev * half)
    far_place = lax.rem(place + seq // 2, jnp.int32(seq))

    def like(shape, dtype=jnp.bfloat16):
        return jax.ShapeDtypeStruct(shape, dtype)

    def spread(rows):
        return lax.all_to_all(
            rows.reshape(half, exp_dev * cap, width),
            axes,
            split_axis=0,
            concat_axis=0,
            axis_index_groups=halves,
            tiled=True,
        ).reshape(slots, width)

    def experts(rows):
        weights = (routed_gate_weight, routed_up_weight, routed_down_weight)
        if cap % 16 == 0:
            rows = rows.reshape(half, exp_dev * cap, width)
            return ffn(rows, *weights, cap).reshape(slots, width)
        order = (half, exp_dev, cap, width)
        rows = rows.reshape(order).transpose(1, 0, 2, 3).reshape(1, slots, width)
        done = ffn(rows, *weights, half * cap)
        return done.reshape(exp_dev, half, cap, width).transpose(1, 0, 2, 3).reshape(slots, width)

    key_rows, key_cols = key_matrix.shape
    vdim = head_norm_gain.shape[0]
    routes_t, scores_t = routes.T, chosen_router_scores.T
    within, starts, message = call(
        state_kernel,
        (
            like((key_rows, key_cols), jnp.float32),
            like((key_rows // BLOCK, vdim, key_cols), jnp.float32),
            like((seq, vdim + MSG_PAD, key_cols)),
        ),
        key_matrix,
        value_matrix,
        channel_decay_input,
        head_decay_offset.T,
        routes_t,
        scores_t,
    )
    arrived = lax.all_to_all(message, "sp", split_axis=0, concat_axis=0, tiled=True)
    gated = call(
        mixer_kernel,
        like(value_matrix.shape),
        place.reshape(1),
        queries,
        key_matrix,
        value_matrix,
        within,
        starts,
        arrived,
        output_gate_input,
        head_norm_gain.reshape(1, vdim),
        scalars=1,
        loose=(5,),
    )
    stacked = gated.reshape(heads_axis, tok_count, gated.shape[1])
    stacked = lax.all_to_all(stacked, "tp", split_axis=0, concat_axis=0, tiled=True)
    held_near, weights_near, held_far, weights_far = tables(
        jnp.stack([first_expert, far_place]), routes_t, scores_t, arrived, slots, cap
    )
    gain = expert_norm_gain.reshape(1, width)
    sent_near, middle, normed = project(
        stacked, mixer_output_weight, residual, gain, held_near
    )
    arrived_near = spread(sent_near)
    base = ffn(
        normed[None],
        common_gate_weight[None],
        common_up_weight[None],
        common_down_weight[None],
        tok_count,
        add=middle,
    )[0]
    quarter = seq // 4
    outer = [pair for pair in swap if pair[0] < quarter or pair[0] >= seq - quarter]
    inner = [pair for pair in swap if pair not in outer]
    outer_rows = lax.ppermute(normed, "sp", outer)
    inner_rows = lax.ppermute(normed, "sp", inner)
    sent_far = pack(held_far, outer_rows, inner_rows)
    arrived_far = spread(sent_far)
    done_near = experts(arrived_near)
    done_far = experts(arrived_far)
    back_far = spread(done_far)
    back_near = spread(done_near)
    rows = like((tok_count, width))
    far = weigh(rows, weights_far, back_far)
    from_far = lax.ppermute(far, "sp", swap)
    return weigh(rows, weights_near, back_near, base, from_far)


def solution(mesh):
    placed = (
        P("sp", "tp"),
        P("sp", "tp"),
        P("sp", "tp"),
        P("sp", "tp"),
        P("sp", "tp"),
        P("sp", "tp"),
        P(),
        P(("sp", "tp"), None),
        P(),
        P(),
        P(("sp", "tp"), None),
        P(("sp", "tp"), None),
        P(("sp", "tp"), None, None),
        P(("sp", "tp"), None, None),
        P(("sp", "tp"), None, None),
        P(),
        P(),
        P(),
    )
    return jax.shard_map(
        on_device, mesh=mesh, in_specs=placed, out_specs=P(("sp", "tp"), None), check_vma=False
    )
```

```python
import functools

import jax
import jax.numpy as jnp
from jax import lax
from jax.experimental import pallas as pl
from jax.experimental.pallas import tpu as pltpu
from jax.sharding import PartitionSpec as P

KEY_CHANNELS = 64
BLOCK = 64
TOP_K = 4
MSG_PAD = 16
ROOM = 48 << 20

eps_norm = 1e-06
decay_running = 16.0
routed_scale = 2.5


def start_all(pairs, sems):
    copies = [pltpu.make_async_copy(src, dst, sems.at[i]) for i, (src, dst) in enumerate(pairs)]
    for copy in copies:
        copy.start()
    return copies


def pieces_of(rows, count):
    return [pl.ds(i * (rows // count), rows // count) for i in range(count)]


def streamed(kernel, out, args, scratch, copies, scalars=0, room=None):
    anywhere = pl.BlockSpec(memory_space=pl.ANY)
    smem = pl.BlockSpec(memory_space=pltpu.SMEM)
    return pl.pallas_call(
        kernel,
        in_specs=[smem] * scalars + [anywhere] * (len(args) - scalars),
        out_specs=jax.tree.map(lambda _: anywhere, out),
        out_shape=out,
        scratch_shapes=[pltpu.VMEM(x.shape, x.dtype) for x in scratch]
        + [pltpu.SemaphoreType.DMA((copies,))],
        compiler_params=pltpu.CompilerParams(vmem_limit_bytes=room),
    )(*args)


PIECES = 4
DEEP = 2


def lane_head(shape):
    return lax.broadcasted_iota(jnp.int32, shape, 1) // KEY_CHANNELS


def two_pieces(value):
    high = value.astype(jnp.bfloat16).astype(jnp.float32)
    return high, value - high


def state_kernel(
    k_ref, v_ref, c_ref, o_ref, routes_ref, scores_ref, within_ref, starts_ref, msg_ref
):
    rows, width = k_ref.shape
    heads = o_ref.shape[0]
    vdim = v_ref.shape[1] // heads
    x = c_ref[...].astype(jnp.float32)
    decay = (jnp.minimum(x, 0.0) - jnp.log1p(jnp.exp(-jnp.abs(x)))) / decay_running
    columns_of = (
        lax.broadcasted_iota(jnp.int32, (heads, width), 0) == lane_head((heads, width))
    ).astype(jnp.float32)
    decay = decay + lax.dot_general(
        o_ref[...],
        columns_of,
        (((0,), (0,)), ((), ())),
        precision=lax.Precision.HIGHEST,
        preferred_element_type=jnp.float32,
    )
    lower = lax.broadcasted_iota(jnp.int32, (BLOCK, BLOCK), 0) >= lax.broadcasted_iota(
        jnp.int32, (BLOCK, BLOCK), 1
    )
    lower = lower.astype(jnp.float32).astype(jnp.bfloat16)
    blocks = rows // BLOCK
    high, rest = two_pieces(decay)
    middle, low = two_pieces(rest)
    summed = None
    for piece in (high, middle, low):
        piece = piece.astype(jnp.bfloat16)
        wide = jnp.concatenate(
            [piece[n * BLOCK : (n + 1) * BLOCK] for n in range(blocks)], axis=1
        )
        part = jnp.dot(lower, wide, preferred_element_type=jnp.float32)
        summed = part if summed is None else summed + part
    state_head = lane_head((vdim, width))
    state = jnp.zeros((vdim, width), jnp.float32)
    total = jnp.zeros((1, width), jnp.float32)
    for n in range(blocks):
        at = slice(n * BLOCK, (n + 1) * BLOCK)
        within = summed[:, n * width : (n + 1) * width]
        within_ref[at, :] = within
        starts_ref[n] = state.astype(jnp.bfloat16)
        last = within[BLOCK - 1 : BLOCK]
        tail = (k_ref[at, :].astype(jnp.float32) * jnp.exp(last - within)).astype(jnp.bfloat16)
        added = jnp.zeros((vdim, width), jnp.float32)
        for h in range(heads):
            one = lax.dot_general(
                v_ref[at, h * vdim : (h + 1) * vdim],
                tail,
                (((0,), (0,)), ((), ())),
                preferred_element_type=jnp.float32,
            )
            added = jnp.where(state_head == h, one, added)
        state = state * jnp.exp(last) + added
        total = total + last
    factor = jnp.exp(total)
    tail_rows = jnp.zeros((MSG_PAD, width), jnp.float32)
    row = lax.broadcasted_iota(jnp.int32, (MSG_PAD, width), 0)
    scores = scores_ref[...]
    place = 0
    for value in two_pieces(factor) + (routes_ref[...].astype(jnp.float32),) + two_pieces(scores):
        for r in range(value.shape[0]):
            tail_rows = jnp.where(row == place, value[r : r + 1], tail_rows)
            place += 1
    tail_rows = tail_rows.astype(jnp.bfloat16)
    state = state.astype(jnp.bfloat16)
    for j in range(msg_ref.shape[0]):
        msg_ref[j, :vdim, :] = state
        msg_ref[j, vdim:, :] = tail_rows


def mixer_kernel(
    place_ref, q_ref, k_ref, v_ref, within_ref, starts_ref, msg_ref, gate_ref, gain_ref, out_ref
):
    rows, width = k_ref.shape
    heads = width // KEY_CHANNELS
    vdim = v_ref.shape[1] // heads

    def hop(j, carried):
        message = msg_ref[j].astype(jnp.float32)
        factor = message[vdim : vdim + 1] + message[vdim + 1 : vdim + 2]
        return carried * factor + message[:vdim]

    carried = lax.fori_loop(0, place_ref[0], hop, jnp.zeros((vdim, width), jnp.float32))
    head_of = lane_head((BLOCK, width))
    causal = lax.broadcasted_iota(jnp.int32, (heads * BLOCK, BLOCK), 0) % BLOCK >= (
        lax.broadcasted_iota(jnp.int32, (heads * BLOCK, BLOCK), 1)
    )
    gain = gain_ref[...]
    before = jnp.zeros((1, width), jnp.float32)
    for n in range(rows // BLOCK):
        at = slice(n * BLOCK, (n + 1) * BLOCK)
        within = within_ref[at, :]
        queries = q_ref[at, :].astype(jnp.float32) * (KEY_CHANNELS**-0.5) * jnp.exp(within)
        grown = (k_ref[at, :].astype(jnp.float32) * jnp.exp(-within)).astype(jnp.bfloat16)
        split = jnp.concatenate(
            [jnp.where(head_of == h, queries, 0.0) for h in range(heads)], axis=0
        ).astype(jnp.bfloat16)
        scores = lax.dot_general(
            split, grown, (((1,), (1,)), ((), ())), preferred_element_type=jnp.float32
        )
        scores = jnp.where(causal, scores, 0.0).astype(jnp.bfloat16)
        entering = (starts_ref[n].astype(jnp.float32) + jnp.exp(before) * carried).astype(jnp.bfloat16)
        crossed = lax.dot_general(
            split, entering, (((1,), (1,)), ((), ())), preferred_element_type=jnp.float32
        )
        for h in range(heads):
            cols = slice(h * vdim, (h + 1) * vdim)
            own = slice(h * BLOCK, (h + 1) * BLOCK)
            output = crossed[own] + jnp.dot(
                scores[own], v_ref[at, cols], preferred_element_type=jnp.float32
            )
            scale = lax.rsqrt(jnp.mean(output * output, axis=-1, keepdims=True) + eps_norm)
            gate = gate_ref[at, cols].astype(jnp.float32)
            out_ref[at, cols] = (
                output * scale * gain * (gate / (1.0 + jnp.exp(-gate)))
            ).astype(jnp.bfloat16)
        before = before + within[BLOCK - 1 : BLOCK]


def whole(x, loose=False):
    return pl.BlockSpec(
        x.shape,
        lambda *_, rank=len(x.shape): (0,) * rank,
        memory_space=None if loose else pltpu.VMEM,
    )


def call(kernel, out, *args, scalars=0, loose=(), room=None):
    in_specs = [pl.BlockSpec(memory_space=pltpu.SMEM)] * scalars + [
        whole(x, i in loose) for i, x in enumerate(args[scalars:])
    ]
    return pl.pallas_call(
        kernel,
        grid=(1,),
        in_specs=in_specs,
        out_specs=jax.tree.map(whole, out),
        out_shape=out,
        compiler_params=pltpu.CompilerParams(vmem_limit_bytes=room),
    )(*args)


def ffn_kernel(x_ref, gate_ref, up_ref, down_ref, *rest):
    add_ref, out_ref, acc_ref = rest if len(rest) == 3 else (None,) + rest
    step = pl.program_id(1)
    rows = x_ref.shape[0] * x_ref.shape[1]
    x = x_ref[...].reshape(rows, x_ref.shape[2])
    gate_pre = jnp.dot(x, gate_ref[0], preferred_element_type=jnp.float32)
    up_pre = jnp.dot(x, up_ref[0], preferred_element_type=jnp.float32)
    hidden = (gate_pre / (1.0 + jnp.exp(-gate_pre)) * up_pre).astype(jnp.bfloat16)
    part = jnp.dot(hidden, down_ref[0], preferred_element_type=jnp.float32)

    @pl.when(step == 0)
    def _():
        acc_ref[...] = part

    @pl.when(step != 0)
    def _():
        acc_ref[...] += part

    @pl.when(step == pl.num_programs(1) - 1)
    def _():
        whole = acc_ref[...]
        if add_ref is not None:
            whole = whole + add_ref[...].astype(jnp.float32)
        out_ref[...] = whole.astype(out_ref.dtype).reshape(out_ref.shape)


def ffn(rows, gate_weight, up_weight, down_weight, cap, add=None):
    sources, _, width = rows.shape
    count, _, hidden = gate_weight.shape
    steps = 2 if hidden % 256 == 0 else 1
    piece = hidden // steps
    row_spec = pl.BlockSpec(
        (sources, cap, width), lambda e, f: (0, e, 0), memory_space=pltpu.VMEM
    )
    in_specs = [
        pl.BlockSpec((sources, cap, width), lambda e, f: (0, e, 0)),
        pl.BlockSpec((1, width, piece), lambda e, f: (e, 0, f)),
        pl.BlockSpec((1, width, piece), lambda e, f: (e, 0, f)),
        pl.BlockSpec((1, piece, width), lambda e, f: (e, f, 0)),
    ]
    args = [rows, gate_weight, up_weight, down_weight]
    dtype = jnp.bfloat16
    if add is not None:
        in_specs.append(whole(add))
        args.append(add)
        dtype = jnp.float32
    return pl.pallas_call(
        ffn_kernel,
        grid=(count, steps),
        in_specs=in_specs,
        out_specs=row_spec,
        out_shape=jax.ShapeDtypeStruct(rows.shape, dtype),
        scratch_shapes=[pltpu.VMEM((sources * cap, width), jnp.float32)],
        compiler_params=pltpu.CompilerParams(vmem_limit_bytes=None if add is not None else ROOM),
        cost_estimate=pl.CostEstimate(
            flops=6 * rows.shape[0] * rows.shape[1] * width * hidden,
            transcendentals=rows.shape[0] * rows.shape[1] * hidden,
            bytes_accessed=6 * count * width * hidden + 4 * rows.size,
        ),
    )(*args)


def slot_tables(routes, scores, first_expert, held_ref, weight_ref, cap):
    slots, tokens = held_ref.shape
    slot = lax.broadcasted_iota(jnp.int32, (slots, tokens), 0)
    expert = (first_expert + lax.div(slot, jnp.int32(cap))).astype(jnp.float32)
    weights = routed_scale * scores / jnp.sum(scores, axis=0, keepdims=True)
    named = jnp.zeros((slots, tokens), jnp.float32)
    weight = jnp.zeros((slots, tokens), jnp.float32)
    for k in range(TOP_K):
        hit = routes[k : k + 1] == expert
        named = jnp.where(hit, 1.0, named)
        weight = jnp.where(hit, weights[k : k + 1], weight)
    earlier = lax.broadcasted_iota(jnp.int32, (tokens, tokens), 0) < lax.broadcasted_iota(
        jnp.int32, (tokens, tokens), 1
    )
    rank = jnp.dot(
        named.astype(jnp.bfloat16),
        jnp.where(earlier, 1.0, 0.0).astype(jnp.bfloat16),
        preferred_element_type=jnp.float32,
    )
    held = (named > 0) & (rank == lax.rem(slot, jnp.int32(cap)).astype(jnp.float32))
    held_ref[...] = jnp.where(held, 1.0, 0.0).astype(jnp.bfloat16)
    high, low = two_pieces(jnp.where(held, weight, 0.0).T)
    weight_ref[:tokens] = high.astype(jnp.bfloat16)
    weight_ref[tokens:] = low.astype(jnp.bfloat16)


def tables_kernel(
    cap, place_ref, routes_ref, scores_ref, far_ref, held_near, near_w, held_far, far_w
):
    slot_tables(
        routes_ref[...].astype(jnp.float32), scores_ref[...], place_ref[0], held_near, near_w, cap
    )
    far = far_ref[0].astype(jnp.float32)
    at = [far[2 + k * TOP_K : 2 + (k + 1) * TOP_K] for k in range(3)]
    slot_tables(at[0], at[1] + at[2], place_ref[0], held_far, far_w, cap)


def tables(places, routes, scores, arrived, slots, cap):
    tokens = routes.shape[1]
    vdim = arrived.shape[1] - MSG_PAD
    held = jax.ShapeDtypeStruct((slots, tokens), jnp.bfloat16)
    weights = jax.ShapeDtypeStruct((2 * tokens, slots), jnp.bfloat16)

    out = (held, weights, held, weights)
    return pl.pallas_call(
        functools.partial(tables_kernel, cap),
        grid_spec=pltpu.PrefetchScalarGridSpec(
            num_scalar_prefetch=1,
            grid=(1,),
            in_specs=[
                whole(routes),
                whole(scores),
                pl.BlockSpec(
                    (1, MSG_PAD, arrived.shape[2]), lambda i, p: (p[1], vdim // MSG_PAD, 0)
                ),
            ],
            out_specs=jax.tree.map(whole, out),
        ),
        out_shape=out,
        name="tables",
    )(places, routes, scores, arrived)


def pick(held, rows):
    return jnp.dot(held, rows, preferred_element_type=jnp.float32).astype(jnp.bfloat16)


def store_slots(held, normed, sent, sent_out, sems, first):
    copies = []
    for i, at in enumerate(pieces_of(sent.shape[0], PIECES)):
        sent[at, :] = pick(held[at, :], normed)
        copies.append(
            pltpu.make_async_copy(sent.at[at, :], sent_out.at[at, :], sems.at[first + i])
        )
        copies[-1].start()
    return copies


def pack_kernel(held_in, rows_in, sent_out, held, rows, sent, sems):
    loads = start_all([(held_in, held), (rows_in, rows)], sems)
    for copy in loads:
        copy.wait()
    for copy in store_slots(held, rows[...], sent, sent_out, sems, 2):
        copy.wait()


def pack(held, rows):
    out = jax.ShapeDtypeStruct((held.shape[0], rows.shape[1]), rows.dtype)
    args = (held, rows)
    return streamed(pack_kernel, out, args, args + (out,), 2 + PIECES, room=ROOM)


def project_kernel(
    g_in, w_in, res_in, gain_in, held_in, sent_out, mid_out, norm_out, *buffers
):
    g, w, res, gain, held, sent, mid, norm, sems = buffers
    count, _, _ = g.shape
    pieces = pieces_of(w.shape[0], count)
    loads = start_all(
        [(g_in, g)]
        + [(w_in.at[at, :], w.at[at, :]) for at in pieces]
        + [(res_in, res), (gain_in, gain), (held_in, held)],
        sems,
    )
    loads[0].wait()
    total = None
    for t, at in enumerate(pieces):
        loads[1 + t].wait()
        part = jnp.dot(g[t], w[at, :], preferred_element_type=jnp.float32)
        total = part if total is None else total + part
    for copy in loads[1 + count :]:
        copy.wait()
    middle = (total + res[...].astype(jnp.float32)).astype(jnp.bfloat16)
    wide = middle.astype(jnp.float32)
    scale = lax.rsqrt(jnp.mean(wide * wide, axis=-1, keepdims=True) + eps_norm)
    normed = (wide * scale * gain[...]).astype(jnp.bfloat16)
    norm[...] = normed
    mid[...] = middle
    first = len(loads)
    stores = [
        pltpu.make_async_copy(norm, norm_out, sems.at[first]),
        pltpu.make_async_copy(mid, mid_out, sems.at[first + 1]),
    ]
    for copy in stores:
        copy.start()
    for copy in stores + store_slots(held, normed, sent, sent_out, sems, first + 2):
        copy.wait()


def project(stacked, weight, residual, gain, held):
    rows = jax.ShapeDtypeStruct(residual.shape, jnp.bfloat16)
    out = (jax.ShapeDtypeStruct((held.shape[0], residual.shape[1]), jnp.bfloat16), rows, rows)
    args = (stacked, weight, residual, gain, held)
    return streamed(project_kernel, out, args, args + out, 6 + stacked.shape[0] + PIECES)


def weigh_kernel(more, weight_in, results_in, *refs):
    extra_in, out_ref = refs[:more], refs[more]
    weight, results = refs[more + 1 : more + 3]
    extra = refs[more + 3 : 2 * more + 3]
    done, sems = refs[2 * more + 3 :]
    tokens = done.shape[0]
    pieces = pieces_of(results.shape[0], DEEP)
    loads = start_all(
        [(weight_in, weight)]
        + [(results_in.at[at, :], results.at[at, :]) for at in pieces]
        + list(zip(extra_in, extra)),
        sems,
    )
    loads[0].wait()
    total = None
    for i, at in enumerate(pieces):
        loads[1 + i].wait()
        part = jnp.dot(weight[:, at], results[at, :], preferred_element_type=jnp.float32)
        total = part if total is None else total + part
    total = total[:tokens] + total[tokens:]
    for copy, ref in zip(loads[1 + DEEP :], extra):
        copy.wait()
        total = total + ref[...].astype(jnp.float32)
    done[...] = total.astype(jnp.bfloat16)
    store = pltpu.make_async_copy(done, out_ref, sems.at[len(loads)])
    store.start()
    store.wait()


def weigh(out, weights, results, *more):
    args = (weights, results) + more
    return streamed(
        functools.partial(weigh_kernel, len(more)),
        out,
        args,
        args + (out,),
        2 + DEEP + len(more),
        room=ROOM if more else None,
    )


def on_device(
    queries,
    key_matrix,
    value_matrix,
    channel_decay_input,
    head_decay_offset,
    output_gate_input,
    head_norm_gain,
    residual,
    mixer_output_weight,
    expert_norm_gain,
    routes,
    chosen_router_scores,
    routed_gate_weight,
    routed_up_weight,
    routed_down_weight,
    common_gate_weight,
    common_up_weight,
    common_down_weight,
):
    seq, heads_axis = lax.axis_size("sp"), lax.axis_size("tp")
    axes = ("sp", "tp")
    devices = seq * heads_axis
    half = devices // 2
    halves = [list(range(half)), list(range(half, devices))]
    swap = [(i, (i + seq // 2) % seq) for i in range(seq)]
    tok_count, width = residual.shape
    exp_dev = routed_gate_weight.shape[0]
    cap = 2 * TOP_K * tok_count // (exp_dev * devices)
    slots = exp_dev * half * cap
    place = lax.axis_index("sp").astype(jnp.int32)
    first_expert = lax.div(place, jnp.int32(seq // 2)) * (exp_dev * half)
    far_place = lax.rem(place + seq // 2, jnp.int32(seq))

    def like(shape, dtype=jnp.bfloat16):
        return jax.ShapeDtypeStruct(shape, dtype)

    def spread(rows):
        return lax.all_to_all(
            rows.reshape(half, exp_dev * cap, width),
            axes,
            split_axis=0,
            concat_axis=0,
            axis_index_groups=halves,
            tiled=True,
        ).reshape(slots, width)

    def experts(rows):
        weights = (routed_gate_weight, routed_up_weight, routed_down_weight)
        if cap % 16 == 0:
            rows = rows.reshape(half, exp_dev * cap, width)
            return ffn(rows, *weights, cap).reshape(slots, width)
        order = (half, exp_dev, cap, width)
        rows = rows.reshape(order).transpose(1, 0, 2, 3).reshape(1, slots, width)
        done = ffn(rows, *weights, half * cap)
        return done.reshape(exp_dev, half, cap, width).transpose(1, 0, 2, 3).reshape(slots, width)

    key_rows, key_cols = key_matrix.shape
    vdim = head_norm_gain.shape[0]
    routes_t, scores_t = routes.T, chosen_router_scores.T
    within, starts, message = call(
        state_kernel,
        (
            like((key_rows, key_cols), jnp.float32),
            like((key_rows // BLOCK, vdim, key_cols)),
            like((seq, vdim + MSG_PAD, key_cols)),
        ),
        key_matrix,
        value_matrix,
        channel_decay_input,
        head_decay_offset.T,
        routes_t,
        scores_t,
    )
    arrived = lax.all_to_all(message, "sp", split_axis=0, concat_axis=0, tiled=True)
    gated = call(
        mixer_kernel,
        like(value_matrix.shape),
        place.reshape(1),
        queries,
        key_matrix,
        value_matrix,
        within,
        starts,
        arrived,
        output_gate_input,
        head_norm_gain.reshape(1, vdim),
        scalars=1,
        loose=(5,),
    )
    stacked = gated.reshape(heads_axis, tok_count, gated.shape[1])
    stacked = lax.all_to_all(stacked, "tp", split_axis=0, concat_axis=0, tiled=True)
    held_near, weights_near, held_far, weights_far = tables(
        jnp.stack([first_expert, far_place]), routes_t, scores_t, arrived, slots, cap
    )
    gain = expert_norm_gain.reshape(1, width)
    sent_near, middle, normed = project(
        stacked, mixer_output_weight, residual, gain, held_near
    )
    arrived_near = spread(sent_near)
    base = ffn(
        normed[None],
        common_gate_weight[None],
        common_up_weight[None],
        common_down_weight[None],
        tok_count,
        add=middle,
    )[0]
    normed_far = lax.ppermute(normed, "sp", swap)
    sent_far = pack(held_far, normed_far)
    arrived_far = spread(sent_far)
    done_near = experts(arrived_near)
    done_far = experts(arrived_far)
    back_far = spread(done_far)
    back_near = spread(done_near)
    rows = like((tok_count, width))
    far = weigh(rows, weights_far, back_far)
    from_far = lax.ppermute(far, "sp", swap)
    return weigh(rows, weights_near, back_near, base, from_far)


def solution(mesh):
    placed = (
        P("sp", "tp"),
        P("sp", "tp"),
        P("sp", "tp"),
        P("sp", "tp"),
        P("sp", "tp"),
        P("sp", "tp"),
        P(),
        P(("sp", "tp"), None),
        P(),
        P(),
        P(("sp", "tp"), None),
        P(("sp", "tp"), None),
        P(("sp", "tp"), None, None),
        P(("sp", "tp"), None, None),
        P(("sp", "tp"), None, None),
        P(),
        P(),
        P(),
    )
    return jax.shard_map(
        on_device, mesh=mesh, in_specs=placed, out_specs=P(("sp", "tp"), None), check_vma=False
    )
```
